32 devices in a mesh: ep: 8 (over z, y), tp: 4 (over x, core).
Axes of the slice: x: 2, y: 2, z: 4, core: 2. Of those that a mesh axis runs over, the one named last changes fastest.
Arguments:
- queries: bfloat16 [8192, 1024], P('ep', 'tp'), may hold values from -6 to 6
- head_keys: bfloat16 [8192, 256], P('ep', 'tp'), may hold values from -6 to 6
- head_values: bfloat16 [8192, 256], P('ep', 'tp'), may hold values from -6 to 6
- sink_logits: float32 [16], P('tp'), may hold values from -2 to 5
- out_weight: bfloat16 [1024, 2048], P('tp'), may hold values from -1.5 to 1.5
- moe_input: bfloat16 [4096, 2048], P(('ep', 'tp')), may hold values from -6 to 6
- norm_gain: float32 [2048], replicated, may hold values from 0.1 to 1.9
- routes: int32 [4096, 4], P(('ep', 'tp')), may hold values from 0 to 7, all different within a row; in each aligned block of 128 rows (0 to 127, 128 to 255, ...) at most 128 rows name the same one
- route_weight: float32 [4096, 4], P(('ep', 'tp')), may hold values from 0.05 to 1
- gate_weight: bfloat16 [8, 2048, 512], P('ep'), may hold values from -2 to 2
- up_weight: bfloat16 [8, 2048, 512], P('ep'), may hold values from -2 to 2
- down_weight: bfloat16 [8, 512, 2048], P('ep'), may hold values from -0.25 to 0.25
Outputs:
- attention_out: bfloat16 [8192, 2048], P(('ep', 'tp'))
- routed_out: bfloat16 [4096, 2048], P(('ep', 'tp'))
The draws below stay inside these ranges and needn't reach their ends.
Inputs may be any that keep to these rules, and one draw needn't show every extreme that they name: `routes`: within the rows of one device (aligned blocks of 128 rows), each expert is named by at most 128 rows, and in every draw some expert by exactly 128; a row names 4 different experts.
All inputs are finite; a program needn't handle non-finite values.
Results may differ from the reference program's by a relative error of at most 0.0078.
Values may be sent and summed in bfloat16 or wider, within the bound.
A program may use at most 128 MiB of HBM per device.

```python
import math
import jax
import jax.numpy as jnp
import numpy as np
from jax import lax

D = 2048
HEADS = 16
KV_HEADS = 4
HEAD_DIM = 64
WINDOW = 128
SEQS = 1
FF = 512
TOPK = 4
TOK_M = 128
EXPERTS = 8
CAP = 128
TOKENS_A = 8192
TOKENS_M = 4096


def draw_queries(key, part):
    per_group = HEADS // KV_HEADS
    normal = jax.random.normal(jax.random.fold_in(key, 1), (TOKENS_A, KV_HEADS, per_group, HEAD_DIM), jnp.float32)
    normal = jnp.clip(normal, -6.0, 6.0)
    return normal.reshape(TOKENS_A, HEADS * HEAD_DIM).astype(jnp.bfloat16)


def draw_head_keys(key, part):
    normal = jax.random.normal(jax.random.fold_in(key, 2), (TOKENS_A, KV_HEADS, 1, HEAD_DIM), jnp.float32)
    normal = jnp.clip(normal, -6.0, 6.0)
    return normal.reshape(TOKENS_A, KV_HEADS * HEAD_DIM).astype(jnp.bfloat16)


def expert_matrix(key, salt):
    normal = jax.random.normal(jax.random.fold_in(key, salt), (EXPERTS, D, FF), jnp.float32)
    normal = jnp.clip(normal, -6.0, 6.0) * D ** (-0.5)
    return jnp.clip(normal, -2.0, 2.0).astype(jnp.bfloat16)


def draw_gate_weight(key, part):
    return expert_matrix(key, 11)


def draw_up_weight(key, part):
    return expert_matrix(key, 13)


def block_scale(stream_key, shape, pieces, low, top_value):
    factor_of, own = 1.0, jax.random.fold_in(stream_key, 6)
    for position, parts in pieces:
        draws = jnp.exp(jax.random.uniform(jax.random.fold_in(own, position), (parts,), jnp.float32, low / len(pieces), top_value / len(pieces)))
        factor_of = factor_of * jnp.repeat(draws, shape[position] // parts).reshape([-1 if axis == position else 1 for axis in range(len(shape))])
    return factor_of


def deal_out(key, own, number, rows, number_of, top, limit, lean):
    sequence = jax.random.permutation(key, number_of)
    crowded, ordinary = shares(number_of, rows * top, limit, lean, True), shares(number_of, rows * top, limit, lean, False)
    places = jnp.arange(number_of)

    def named(tallies, turn):
        used = int((tallies > 0).sum())
        fixed = max(1, used // 4)
        passed = fixed + (places - fixed + turn * (used - fixed)) % max(1, number_of - fixed)
        return jnp.zeros((number_of,), jnp.int32).at[sequence[jnp.where(places < fixed, places, passed)]].set(jnp.asarray(tallies, jnp.int32))

    tallies = jnp.where(number % 4 == 0, named(crowded, number // 4), named(ordinary, number - number // 4 - 1))
    mixed = jax.random.permutation(jax.random.fold_in(own, 3), number_of)
    giver, sink = mixed[0:number_of // 2 * 2:2], mixed[1:number_of // 2 * 2:2]
    margin = jnp.minimum(tallies[giver] - 1, limit - tallies[sink]) // 2
    margin = jnp.where((giver == sequence[0]) | (sink == sequence[0]) | (tallies[sink] == 0), 0, jnp.maximum(margin, 0))
    passed = jax.random.randint(jax.random.fold_in(own, 4), (number_of // 2,), 0, 1 << 20) % (margin + 1)
    tallies = tallies.at[giver].add(-passed).at[sink].add(passed)
    labels = jnp.searchsorted(jnp.cumsum(tallies), jnp.arange(rows * top), side="right").astype(jnp.int32)
    listing = labels.reshape(top, rows).T
    listing = listing[jax.random.permutation(jax.random.fold_in(own, 1), rows)]
    turn = jax.random.randint(jax.random.fold_in(own, 2), (rows, 1), 0, top)
    return jnp.take_along_axis(listing, (jnp.arange(top)[None, :] + turn) % top, axis=1)


def shares(number_of, total, most, skew, full):
    portions = [(1 << 20) // math.isqrt(standing ** skew) + 1 for standing in range(1, number_of + 1)]
    largest = most if full else min(most, max(-(-total // number_of), total * portions[0] // sum(portions)))
    least = 1 if total - largest >= number_of - 1 else 0
    given, rest = [largest] + [least] * (number_of - 1), total - largest - least * (number_of - 1)
    while rest > 0:
        candidates = [i for i in range(1, number_of) if given[i] < largest] or [i for i in range(1, number_of) if given[i] < most]
        mass, remaining = sum([portions[i] for i in candidates]), rest
        for i in candidates:
            addition = min(most - given[i], max(1, remaining * portions[i] // mass), rest)
            given[i] = given[i] + addition
            rest = rest - addition
    return np.array(given)


def gaussian(key, shape, spread, reach, split=(), kind=jnp.bfloat16):
    drawn = jax.random.normal(key, shape, jnp.float32) * spread
    if len(split) > 0:
        drawn = block_scale(key, shape, split, -0.22, 0.18) * drawn
    return jnp.clip(drawn, min=-reach, max=reach).astype(kind)


def setup_inputs(seed: int = 0) -> dict:
    streams_of = jax.random.split(jax.random.key(seed), 13)
    queries = draw_queries(jax.random.fold_in(streams_of[12], 71), 0)
    head_keys = draw_head_keys(jax.random.fold_in(streams_of[12], 71), 0)
    head_values = gaussian(streams_of[2], (TOKENS_A, KV_HEADS * HEAD_DIM), 1.0, 6.0, ((0, 8), (1, 4)))
    sink_logits = jnp.clip(-2.0 + 7.0 * jax.random.uniform(streams_of[3], (HEADS,), jnp.float32) ** block_scale(streams_of[3], (HEADS,), ((0, 4),), -0.2, 0.2), -2.0, 5.0)
    out_weight = gaussian(streams_of[4], (HEADS * HEAD_DIM, D), 0.25, 1.5, ((0, 4),))
    moe_input = gaussian(streams_of[5], (TOKENS_M, D), 1.0, 6.0, ((0, 32),))
    norm_gain = jnp.clip(1.0 + 0.18 * jax.random.normal(streams_of[6], (D,), jnp.float32), 0.1, 1.9)
    routes_keys = jax.random.split(jax.random.fold_in(streams_of[7], 1), TOKENS_M // TOK_M)
    routes_turns = jax.random.permutation(jax.random.fold_in(streams_of[7], 3), TOKENS_M // TOK_M)
    routes = jax.vmap(lambda own, number: deal_out(jax.random.fold_in(streams_of[7], 2), own, number, TOK_M, EXPERTS, TOPK, CAP, 1))(routes_keys, routes_turns).reshape((TOKENS_M, TOPK))
    route_weight = jnp.clip(jnp.exp(math.log(1.0) - 2.9957323 * jax.random.uniform(streams_of[8], (TOKENS_M, TOPK), jnp.float32) ** block_scale(streams_of[8], (TOKENS_M, TOPK), ((0, 32),), -0.2, 0.2)), 0.05, 1.0)
    gate_weight = draw_gate_weight(jax.random.fold_in(streams_of[12], 71), 0)
    up_weight = draw_up_weight(jax.random.fold_in(streams_of[12], 71), 0)
    down_weight = gaussian(streams_of[11], (EXPERTS, FF, D), FF ** -0.5, 0.25, ((0, 8),))
    return dict(queries=queries, head_keys=head_keys, head_values=head_values, sink_logits=sink_logits, out_weight=out_weight, moe_input=moe_input, norm_gain=norm_gain, routes=routes, route_weight=route_weight, gate_weight=gate_weight, up_weight=up_weight, down_weight=down_weight)


EPSILON = 1e-05
NEGATIVE = -1e+30

def clamped_unit(gate_pre, up_pre):
    gate_cut = jnp.minimum(gate_pre, 7.0)
    up_cut = jnp.clip(up_pre, -7.0, 7.0)
    return gate_cut * jax.nn.sigmoid(1.702 * gate_cut) * (up_cut + 1.0)

def window_attention(queries, head_keys, head_values, sink_logits, out_weight):
    total = queries.shape[0]
    per_group = HEADS // KV_HEADS
    seq_len = TOKENS_A // SEQS
    padding = jnp.zeros((WINDOW, KV_HEADS * HEAD_DIM), head_keys.dtype)
    padded_keys = jnp.concatenate([padding, head_keys], axis=0)
    padded_values = jnp.concatenate([padding, head_values], axis=0)
    sinks = sink_logits.astype(jnp.float32).reshape(KV_HEADS, per_group, 1, 1)

    def one_block(index):
        first = (index * WINDOW).astype(jnp.int32)
        block_q = lax.dynamic_slice_in_dim(queries, first, WINDOW, 0)
        block_q = block_q.reshape(WINDOW, KV_HEADS, per_group, HEAD_DIM).astype(jnp.float32)
        block_k = lax.dynamic_slice_in_dim(padded_keys, first, 2 * WINDOW, 0)
        block_k = block_k.reshape(2 * WINDOW, KV_HEADS, HEAD_DIM).astype(jnp.float32)
        block_v = lax.dynamic_slice_in_dim(padded_values, first, 2 * WINDOW, 0)
        block_v = block_v.reshape(2 * WINDOW, KV_HEADS, HEAD_DIM).astype(jnp.float32)
        scores = jnp.einsum('qkgd,skd->kgqs', block_q, block_k) * HEAD_DIM ** (-0.5)
        query_pos = first + jnp.arange(WINDOW, dtype=jnp.int32)
        key_pos = first - WINDOW + jnp.arange(2 * WINDOW, dtype=jnp.int32)
        distance = query_pos[:, None] - key_pos[None, :]
        starts = query_pos // seq_len * seq_len
        valid = (distance >= 0) & (distance < WINDOW) & (key_pos[None, :] >= starts[:, None])
        scores = jnp.where(valid[None, None], scores, NEGATIVE)
        maxima = jnp.maximum(lax.optimization_barrier(jnp.max(scores, axis=-1, keepdims=True)), sinks)
        powers = jnp.exp(scores - maxima)
        weights = powers / (lax.optimization_barrier(jnp.sum(powers, axis=-1, keepdims=True)) + jnp.exp(sinks - maxima))
        weights = weights.astype(jnp.bfloat16)
        heads = jnp.einsum('kgqs,skd->qkgd', weights.astype(jnp.float32), block_v)
        return heads.astype(jnp.bfloat16).reshape(WINDOW, HEADS * HEAD_DIM)
    heads_out = lax.map(one_block, jnp.arange(total // WINDOW, dtype=jnp.int32))
    heads_out = heads_out.reshape(total, HEADS * HEAD_DIM)
    return jnp.dot(heads_out, out_weight, preferred_element_type=jnp.float32).astype(jnp.bfloat16)

def routed_experts(moe_input, norm_gain, routes, route_weight, gate_weight, up_weight, down_weight):
    token_count = moe_input.shape[0]
    values32 = moe_input.astype(jnp.float32)
    scale = lax.rsqrt(lax.optimization_barrier(jnp.mean(values32 * values32, axis=-1, keepdims=True)) + EPSILON)
    normed = (values32 * scale * norm_gain.astype(jnp.float32)).astype(jnp.bfloat16)
    assigned = token_count * TOPK
    group_rows = 256
    flat_routes = routes.reshape(assigned).astype(jnp.int32)
    token_of = (jnp.arange(assigned, dtype=jnp.int32) // TOPK).astype(jnp.int32)
    order = jnp.argsort(flat_routes, stable=True).astype(jnp.int32)
    sorted_routes = flat_routes[order]
    counts = lax.optimization_barrier(jnp.sum((flat_routes[:, None] == jnp.arange(EXPERTS, dtype=jnp.int32)[None, :]).astype(jnp.int32), axis=0)).astype(jnp.int32)
    padded = ((counts + group_rows - 1) // group_rows * group_rows).astype(jnp.int32)
    end_pad = jnp.cumsum(padded).astype(jnp.int32)
    start_pad = (end_pad - padded).astype(jnp.int32)
    start_raw = (jnp.cumsum(counts) - counts).astype(jnp.int32)
    dest = (start_pad[sorted_routes] + jnp.arange(assigned, dtype=jnp.int32) - start_raw[sorted_routes]).astype(jnp.int32)
    group_count = -(-assigned // group_rows) + EXPERTS
    slot_total = group_count * group_rows
    row_token = jnp.zeros((slot_total,), jnp.int32).at[dest].set(token_of[order])
    row_weight = jnp.zeros((slot_total,), jnp.float32).at[dest].set(route_weight.reshape(assigned).astype(jnp.float32)[order])
    group_expert = jnp.searchsorted(end_pad, jnp.arange(group_count, dtype=jnp.int32) * group_rows, side='right')
    group_expert = jnp.minimum(group_expert, EXPERTS - 1).astype(jnp.int32)

    def add_group(total, inputs):
        expert, tokens, weights = inputs
        rows_in = normed[tokens]
        gate_pre = jnp.dot(rows_in, gate_weight[expert], preferred_element_type=jnp.float32)
        up_pre = jnp.dot(rows_in, up_weight[expert], preferred_element_type=jnp.float32)
        act = clamped_unit(gate_pre, up_pre).astype(jnp.bfloat16)
        result = jnp.dot(act, down_weight[expert], preferred_element_type=jnp.float32).astype(jnp.bfloat16)
        return (total.at[tokens].add(result.astype(jnp.float32) * weights[:, None]), None)
    initial = jnp.zeros((token_count, D), jnp.float32)
    total, _ = lax.scan(add_group, initial, (group_expert, row_token.reshape(group_count, group_rows), row_weight.reshape(group_count, group_rows)))
    return total.astype(jnp.bfloat16)

def reference(queries, head_keys, head_values, sink_logits, out_weight, moe_input, norm_gain, routes, route_weight, gate_weight, up_weight, down_weight):
    attention_out = window_attention(queries, head_keys, head_values, sink_logits, out_weight)
    routed_out = routed_experts(moe_input, norm_gain, routes, route_weight, gate_weight, up_weight, down_weight)
    return (attention_out, routed_out)
```

```python
import functools

import jax
import jax.numpy as jnp
from jax import lax
from jax.experimental import pallas as pl
from jax.experimental.pallas import tpu as pltpu
from jax.sharding import PartitionSpec as P

HEAD_DIM = 64
WINDOW = 128
SEQS = 1


EPSILON = 1e-05
NEGATIVE = -1e30


def passed_along(value, axis, steps):
    count = lax.axis_size(axis)
    first, last = (max(0, -steps), min(count, count - steps))
    return lax.ppermute(value, axis, [(source, source + steps) for source in range(first, last)])


def clamped_unit(gate_pre, up_pre):
    gate_cut = jnp.minimum(gate_pre, 7.0)
    up_cut = jnp.clip(up_pre, -7.0, 7.0)
    return gate_cut * jax.nn.sigmoid(1.702 * gate_cut) * (up_cut + 1.0)


def attend(queries, head_keys, head_values, sink_logits, out_weight):
    tok_rows = queries.shape[0]
    local_heads = sink_logits.shape[0]
    local_kv = head_keys.shape[1] // HEAD_DIM
    per_group = local_heads // local_kv
    block_count = tok_rows // WINDOW
    key_width = local_kv * HEAD_DIM
    kv_rows = jnp.concatenate([head_keys, head_values], axis=1)
    earlier = passed_along(kv_rows[tok_rows - WINDOW :], "ep", 1)
    extended = jnp.concatenate([earlier, kv_rows], axis=0)
    banded = jnp.concatenate(
        [
            extended[:tok_rows].reshape(block_count, WINDOW, 2 * key_width),
            kv_rows.reshape(block_count, WINDOW, 2 * key_width),
        ],
        axis=1,
    )
    band_keys = banded[:, :, :key_width].reshape(block_count, 2 * WINDOW, local_kv, HEAD_DIM)
    band_values = banded[:, :, key_width:].reshape(block_count, 2 * WINDOW, local_kv, HEAD_DIM)
    blocked = queries.reshape(block_count, WINDOW, local_kv, per_group, HEAD_DIM)
    scores = jnp.einsum(
        "nqkgd,nskd->nkgqs", blocked, band_keys, preferred_element_type=jnp.float32
    ) * HEAD_DIM ** (-0.5)
    offset = lax.axis_index("ep") * tok_rows
    seq_len = tok_rows * lax.axis_size("ep") // SEQS
    query_pos = offset + jnp.arange(tok_rows, dtype=jnp.int32).reshape(block_count, WINDOW)
    key_pos = (
        offset
        - WINDOW
        + (jnp.arange(block_count, dtype=jnp.int32) * WINDOW)[:, None]
        + jnp.arange(2 * WINDOW, dtype=jnp.int32)[None, :]
    )
    distance = query_pos[:, :, None] - key_pos[:, None, :]
    starts = query_pos // seq_len * seq_len
    valid = (distance >= 0) & (distance < WINDOW) & (key_pos[:, None, :] >= starts[:, :, None])
    scores = jnp.where(valid[:, None, None], scores, NEGATIVE)
    sinks = sink_logits.reshape(local_kv, per_group, 1, 1)
    maxima = jnp.maximum(jnp.max(scores, axis=-1, keepdims=True), sinks)
    powers = jnp.exp(scores - maxima)
    weights = (powers / (jnp.sum(powers, axis=-1, keepdims=True) + jnp.exp(sinks - maxima))).astype(
        jnp.bfloat16
    )
    heads_out = jnp.einsum(
        "nkgqs,nskd->nqkgd", weights, band_values, preferred_element_type=jnp.float32
    )
    heads_out = heads_out.astype(jnp.bfloat16).reshape(tok_rows, local_heads * HEAD_DIM)
    summed = lax.psum_scatter(
        jnp.dot(heads_out, out_weight, preferred_element_type=jnp.float32),
        "tp",
        scatter_dimension=0,
        tiled=True,
    )
    return summed.astype(jnp.bfloat16)


def experts_part(moe_input, norm_gain, routes, route_weight, gate_weight, up_weight, down_weight):
    tok_rows, model_width = moe_input.shape
    choice_count = routes.shape[1]
    targets = lax.axis_size("ep")
    capacity = 2 * choice_count * tok_rows // targets
    values32 = moe_input.astype(jnp.float32)
    scale = lax.rsqrt(jnp.mean(values32 * values32, axis=-1, keepdims=True) + EPSILON)
    normed = (values32 * scale * norm_gain).astype(jnp.bfloat16)
    if capacity >= tok_rows:
        experts = jnp.arange(targets, dtype=jnp.int32)
        named = routes[:, :, None] == experts[None, None, :]
        shares = jnp.sum(jnp.where(named, route_weight[:, :, None], 0.0), axis=1)
        everyone = lax.all_gather(normed, "ep", axis=0, tiled=True)
        mine = lax.all_to_all(shares.T[:, None], "ep", split_axis=0, concat_axis=0, tiled=True)
        gate_pre = jnp.dot(everyone, gate_weight[0], preferred_element_type=jnp.float32)
        up_pre = jnp.dot(everyone, up_weight[0], preferred_element_type=jnp.float32)
        act = clamped_unit(gate_pre, up_pre).astype(jnp.bfloat16)
        result = jnp.dot(act, down_weight[0], preferred_element_type=jnp.float32)
        part = result.astype(jnp.bfloat16).astype(jnp.float32) * mine.reshape(-1, 1)
        return lax.psum_scatter(
            part.astype(jnp.bfloat16), "ep", scatter_dimension=0, tiled=True
        )
    flat_routes = routes.reshape(-1)
    onehot = (flat_routes[:, None] == jnp.arange(targets, dtype=jnp.int32)[None, :]).astype(
        jnp.int32
    )
    earlier_count = jnp.sum((jnp.cumsum(onehot, axis=0) - onehot) * onehot, axis=1)
    slot_index = flat_routes * capacity + earlier_count
    copies = jnp.repeat(normed, choice_count, axis=0)
    outgoing = jnp.zeros((targets * capacity, model_width), jnp.bfloat16).at[slot_index].set(copies)
    outgoing = outgoing.reshape(targets, capacity, model_width)
    arrived = lax.all_to_all(outgoing, "ep", split_axis=0, concat_axis=0, tiled=True)
    flat_rows = arrived.reshape(-1, model_width)
    gate_pre = jnp.dot(flat_rows, gate_weight[0], preferred_element_type=jnp.float32)
    up_pre = jnp.dot(flat_rows, up_weight[0], preferred_element_type=jnp.float32)
    act = clamped_unit(gate_pre, up_pre).astype(jnp.bfloat16)
    result = jnp.dot(act, down_weight[0], preferred_element_type=jnp.float32).astype(jnp.bfloat16)
    came_back = lax.all_to_all(
        result.reshape(arrived.shape), "ep", split_axis=0, concat_axis=0, tiled=True
    )
    picked = came_back.reshape(targets * capacity, model_width)[slot_index]
    weighted = (
        picked.astype(jnp.float32).reshape(tok_rows, choice_count, model_width)
        * route_weight[:, :, None]
    )
    return jnp.sum(weighted, axis=1).astype(jnp.bfloat16)


ROW = 2
CORES = 2
TP = 4
PIECES = 4
CHUNKS = 4
SLABS = 8
LAG = 2


def fused_kernel(
    lines, width,
    rows_hbm, shares_hbm, gate_hbm, up_hbm, down_hbm, q_hbm, kv_hbm, sinks_hbm, proj_hbm,
    routed_ref, attn_ref,
    gath, shares, wgu, wd, act, onward, from_line,
    qs, ext, sinks, wo, keep, mate_out, mate_in, x_out, x_in,
    local_sem, share_send, share_recv, halo_sem,
    up_send, down_send, tok_recv,
    y_send, y_recv, x_send, x_recv, m_send, m_recv,
    line_send, line_recv, pair_send, pair_recv, cross_send, cross_recv,
):
    ep, tp = lax.axis_index("ep"), lax.axis_index("tp")
    z, y, x, c = ep // ROW, ep % ROW, tp // CORES, tp % CORES
    tok_rows, model_width = routed_ref.shape
    hidden = gate_hbm.shape[1]
    piece = tok_rows // PIECES
    chunk = model_width // CHUNKS
    last = lines - 1

    def at(zz, yy, xx, cc):
        return {"ep": zz * ROW + yy, "tp": xx * CORES + cc}

    def remote(source, target, send, recv, device):
        return pltpu.make_async_remote_copy(
            src_ref=source, dst_ref=target, send_sem=send, recv_sem=recv,
            device_id=device, device_id_type=pl.DeviceIdType.MESH,
        )

    above = at(jnp.minimum(z + 1, last), y, x, c)
    below = at(jnp.maximum(z - 1, 0), y, x, c)
    over_y, over_x, mate = at(z, 1 - y, x, c), at(z, y, 1 - x, c), at(z, y, x, 1 - c)

    own_kv = ext.at[pl.ds(WINDOW, q_hbm.shape[0])]
    loads = [
        pltpu.make_async_copy(source, target, local_sem.at[i])
        for i, (source, target) in enumerate([
            (kv_hbm, own_kv),
            (rows_hbm, gath.at[z]),
            (shares_hbm, shares.at[z]),
            (gate_hbm, wgu.at[0, :, pl.ds(0, hidden)]),
            (up_hbm, wgu.at[0, :, pl.ds(hidden, hidden)]),
            (down_hbm, wd.at[pl.ds(0, hidden)]),
            (q_hbm, qs),
            (sinks_hbm, sinks),
            (proj_hbm, wo),
        ])
    ]
    for load in loads:
        load.start()

    ahead = ep + 1 < lines * ROW
    behind = ep > 0
    skew = jnp.where(y == 1, z < last, z > 0)
    skew_ep = jnp.where(y == 1, jnp.minimum(ep + 1, lines * ROW - 1), jnp.maximum(ep - 1, 0))
    barrier = pltpu.get_barrier_semaphore()

    def greet(device):
        pl.semaphore_signal(barrier, inc=1, device_id=device, device_id_type=pl.DeviceIdType.MESH)

    for step in range(1, lines):
        greet(at(lax.rem(z + step, lines), y, x, c))
    greet(over_y)
    greet(over_x)
    greet(mate)

    @pl.when(skew)
    def _():
        greet({"ep": skew_ep, "tp": tp})

    pl.semaphore_wait(barrier, last + 3 + jnp.where(skew, 1, 0))

    halo = remote(
        ext.at[pl.ds(q_hbm.shape[0], WINDOW)], ext.at[pl.ds(0, WINDOW)], halo_sem.at[0],
        halo_sem.at[1], {"ep": jnp.minimum(ep + 1, lines * ROW - 1), "tp": tp},
    )

    def share_copy(slot, recv_slot, device):
        return remote(
            shares.at[slot], shares.at[slot], share_send.at[recv_slot], share_recv.at[slot], device
        )

    def tok_copy(block, part, sems, device):
        view = gath.at[block, pl.ds(part * piece, piece)]
        return remote(view, view, sems.at[block, part], tok_recv.at[block, part], device)

    quarter = wgu.shape[1] // TP
    slab = quarter // SLABS

    def gu_view(expert, q, p):
        return wgu.at[expert, pl.ds(q * quarter + p * slab, slab)]

    def d_view(expert, q, p):
        return wd.at[
            pl.ds(expert * hidden + q * (hidden // TP), hidden // TP), pl.ds(p * chunk, chunk)
        ]

    def weight_copies(view, base):
        def over_link(p):
            return remote(
                view(0, tp, p), view(1, tp, p), y_send.at[base + p], y_recv.at[base + p], over_y
            )

        def to_plane(p):
            return remote(
                view(1, tp, p), view(1, tp, p), x_send.at[base + p], x_recv.at[base + p], over_x
            )

        def to_mate(p, second):
            q = jnp.where(second == 1, (1 - x) * CORES + c, tp) if second else tp
            return remote(
                view(1, q, p), view(1, q, p), m_send.at[second, base + p],
                m_recv.at[second, base + p], mate,
            )

        return over_link, to_plane, to_mate

    gu_over, gu_plane, gu_mate = weight_copies(gu_view, 0)
    d_over, d_plane, d_mate = weight_copies(d_view, SLABS)

    loads[0].wait()

    @pl.when(ahead)
    def _():
        halo.start()

    loads[1].wait()
    loads[2].wait()
    for step in range(1, lines):
        other = lax.rem(z + step, lines)
        share_copy(z, other, at(other, y, x, c)).start()

    def own_tokens(first, count, upward):
        for part in range(first, first + count):
            if upward:
                tok_copy(z, part, up_send, above).start()
            else:
                tok_copy(z, part, down_send, below).start()

    half = PIECES // 2

    @pl.when(z < last)
    def _():
        own_tokens(0, half, True)

    @pl.when(z == 0)
    def _():
        own_tokens(half, half, True)

    @pl.when(z > 0)
    def _():
        own_tokens(0, half, False)

    @pl.when(z == last)
    def _():
        own_tokens(half, half, False)

    loads[3].wait()
    loads[4].wait()

    def launch_gu(p, carry):
        gu_over(p).start()
        return carry

    lax.fori_loop(0, SLABS, launch_gu, 0)
    loads[5].wait()

    def launch_d(p, carry):
        d_over(p).start()
        return carry

    lax.fori_loop(0, CHUNKS, launch_d, 0)

    @pl.when(z == 0)
    def _():
        from_line[0] = jnp.zeros_like(from_line[0])

    @pl.when(z == last)
    def _():
        from_line[1] = jnp.zeros_like(from_line[1])

    loads[6].wait()
    loads[7].wait()
    loads[8].wait()

    @pl.when(behind)
    def _():
        halo.wait_recv()

    @pl.when(ep == 0)
    def _():
        ext[pl.ds(0, WINDOW)] = jnp.zeros((WINDOW, ext.shape[1]), ext.dtype)

    def arrival(i, reach):
        s = i // half
        far = s < reach
        distance = jnp.where(far, s + 1, 2 * reach - s)
        part = jnp.where(far, 0, half) + i % half
        return distance, part

    def pump_tokens(i):
        for upward in (True, False):
            reach = z if upward else last - z
            distance, part = arrival(i, reach)
            block = jnp.clip(z - distance if upward else z + distance, 0, last)

            @pl.when(i < PIECES * reach)
            def _():
                tok_copy(block, part, up_send, above).wait_recv()

            @pl.when((i < PIECES * reach) & (reach < last))
            def _():
                if upward:
                    tok_copy(block, part, up_send, above).start()
                else:
                    tok_copy(block, part, down_send, below).start()

            @pl.when((i == PIECES * reach - 1) & (reach < last))
            def _():
                own_tokens(half, half, upward)

    per_group = sinks.shape[0]
    band = 2 * WINDOW
    quarter_rows = attn_ref.shape[0]
    blocks_each = quarter_rows // WINDOW
    kv_width = ext.shape[1] // 2

    def pair_copy(owner_x):
        return remote(
            mate_out.at[owner_x], mate_in.at[owner_x], pair_send.at[owner_x],
            pair_recv.at[owner_x], mate,
        )

    def attend_block(n):
        q_rows = qs[pl.ds(n * WINDOW, WINDOW)] * jnp.bfloat16(HEAD_DIM ** (-0.5))
        held = ext[pl.ds(n * WINDOW, band)]
        keys = jnp.concatenate([held[:, :kv_width]] * 2, axis=1)
        values = jnp.concatenate([held[:, kv_width:]] * 2, axis=1)
        q_head = lax.broadcasted_iota(jnp.int32, q_rows.shape, 1) // HEAD_DIM
        stacked = jnp.concatenate(
            [jnp.where(q_head == h, q_rows, jnp.zeros_like(q_rows)) for h in range(per_group)],
            axis=0,
        )
        scores = lax.dot_general(
            stacked, keys, (((1,), (1,)), ((), ())), preferred_element_type=jnp.float32
        )
        begins = lax.rem(ep * (qs.shape[0] // WINDOW) + n, lines * ROW * (qs.shape[0] // WINDOW) // SEQS) == 0
        row = lax.broadcasted_iota(jnp.int32, (WINDOW, band), 0)
        col = lax.broadcasted_iota(jnp.int32, (WINDOW, band), 1)
        valid = (col > row) & (col <= row + WINDOW) & (col >= jnp.where(begins, WINDOW, 0))
        weights = []
        for h in range(per_group):
            score = jnp.where(valid, scores[h * WINDOW : (h + 1) * WINDOW], NEGATIVE)
            sink = sinks[h : h + 1, 0:1]
            top = jnp.maximum(jnp.max(score, axis=1, keepdims=True), sink)
            powers = jnp.exp(score - top)
            total = jnp.sum(powers, axis=1, keepdims=True) + jnp.exp(sink - top)
            weights.append((powers * (1.0 / total)).astype(jnp.bfloat16))
        v_head = lax.broadcasted_iota(jnp.int32, values.shape, 1) // HEAD_DIM
        spread = jnp.concatenate(
            [jnp.where(v_head == h, values, jnp.zeros_like(values)) for h in range(per_group)],
            axis=0,
        )
        heads = jnp.dot(
            jnp.concatenate(weights, axis=1), spread, preferred_element_type=jnp.float32
        ).astype(jnp.bfloat16)
        owner = n // blocks_each
        owner_x, owner_c = owner // CORES, owner % CORES
        place = pl.ds((n % blocks_each) * WINDOW, WINDOW)
        share = jnp.dot(heads, wo[...], preferred_element_type=jnp.float32)

        @pl.when(owner_c == c)
        def _():
            keep[owner_x, place] = share

        @pl.when(owner_c != c)
        def _():
            mate_out[owner_x, place] = share.astype(jnp.bfloat16)

    def slot(i, carry):
        gu_over(i).wait_recv()
        gu_plane(i).start()
        gu_mate(i, 0).start()
        pump_tokens(i)

        @pl.when(i >= LAG)
        def _():
            gu_plane(i - LAG).wait_recv()
            gu_mate(i - LAG, 1).start()

        attend_block(i)
        return carry

    lax.fori_loop(0, SLABS, slot, 0)
    for owner_x in range(TP // CORES):
        pair_copy(owner_x).start()
    for p in range(SLABS - LAG, SLABS):
        gu_plane(p).wait_recv()
        gu_mate(p, 1).start()
    for step in range(1, lines):
        source = lax.rem(z + step, lines)
        share_copy(source, source, at(source, y, x, c)).wait_recv()

    def gather_gu(p, carry):
        gu_mate(p, 0).wait_recv()
        gu_mate(p, 1).wait_recv()
        return carry

    lax.fori_loop(0, SLABS, gather_gu, 0)

    square = (tok_rows, tok_rows)
    eye = lax.broadcasted_iota(jnp.int32, square, 0) == lax.broadcasted_iota(jnp.int32, square, 1)

    def activate(block):
        def one(expert, carry):
            pre = jnp.dot(gath[block], wgu[expert], preferred_element_type=jnp.float32)
            unit = clamped_unit(pre[:, :hidden], pre[:, hidden:])
            named = z * ROW + jnp.where(expert == 1, 1 - y, y)
            column = jnp.sum(
                jnp.where(eye, shares[block, pl.ds(named, 1), :], 0.0), axis=1, keepdims=True
            )
            act[expert] = (unit * column).astype(jnp.bfloat16)
            return carry

        lax.fori_loop(0, ROW, one, 0)

    def partial(cols):
        both = jnp.concatenate([act[0], act[1]], axis=1)
        return jnp.dot(both, wd[:, cols], preferred_element_type=jnp.float32)

    def line_copy(downward, block, j, device):
        cols = pl.ds(j * chunk, chunk)
        return remote(
            onward.at[block, :, cols], from_line.at[downward, block, :, cols],
            line_send.at[block, j], line_recv.at[downward, block, j], device,
        )

    def pick(k):
        block = 0
        for zz in range(lines):
            others = sorted(
                (b for b in range(lines) if b != zz), key=lambda b: (-abs(b - zz), b)
            )
            for kk, b in enumerate(others):
                block = jnp.where((z == zz) & (k == kk), b, block)
        return block

    def cross_copy():
        return remote(x_out, x_in, cross_send, cross_recv, over_x)

    def visit(k, carry):
        block = pick(k)
        downward = jnp.where(block < z, 1, 0)

        @pl.when((k > 0) & ((z == 0) | (z == last)))
        def _():
            for e in range(half):
                distance, part = arrival(PIECES * (lines - 2) + (k - 1) * half + e, last)
                source = jnp.clip(jnp.where(z == 0, distance, last - distance), 0, last)
                tok_copy(source, part, up_send, above).wait_recv()

        activate(block)
        device = at(jnp.clip(jnp.where(downward == 1, z - 1, z + 1), 0, last), y, x, c)
        inner = jnp.where(downward == 1, z < last, z > 0)

        def one(j, carry):
            @pl.when(k == 0)
            def _():
                d_over(j).wait_recv()
                d_plane(j).start()
                d_mate(j, 0).start()
                d_plane(j).wait_recv()
                d_mate(j, 1).start()
                d_mate(j, 0).wait_recv()
                d_mate(j, 1).wait_recv()

            cols = pl.ds(pl.multiple_of(j * chunk, chunk), chunk)
            own = partial(cols)

            @pl.when(inner)
            def _():
                line_copy(downward, block, j, device).wait_recv()

            onward[block, :, cols] = (
                own + from_line[downward, block, :, cols].astype(jnp.float32)
            ).astype(jnp.bfloat16)
            line_copy(downward, block, j, device).start()
            return carry

        lax.fori_loop(0, CHUNKS, one, 0)

        @pl.when(k == 0)
        def _():
            for owner_x in range(TP // CORES):
                pair_copy(owner_x).wait_recv()
            x_out[...] = (keep[1 - x] + mate_in[1 - x].astype(jnp.float32)).astype(jnp.bfloat16)
            cross_copy().start()

        return carry

    lax.fori_loop(0, last, visit, 0)

    activate(z)

    def finish(j, carry):
        cols = pl.ds(pl.multiple_of(j * chunk, chunk), chunk)
        own = partial(cols)

        @pl.when(z > 0)
        def _():
            line_copy(0, z, j, above).wait_recv()

        @pl.when(z < last)
        def _():
            line_copy(1, z, j, above).wait_recv()

        routed_ref[:, cols] = (
            own + from_line[0, z, :, cols].astype(jnp.float32)
            + from_line[1, z, :, cols].astype(jnp.float32)
        ).astype(jnp.bfloat16)
        return carry

    cross_copy().wait_recv()
    attn_ref[...] = (
        keep[x] + mate_in[x].astype(jnp.float32) + x_in[...].astype(jnp.float32)
    ).astype(jnp.bfloat16)
    lax.fori_loop(0, CHUNKS, finish, 0)

    @pl.when(ahead)
    def _():
        halo.wait_send()

    cross_copy().wait_send()
    for owner_x in range(TP // CORES):
        pair_copy(owner_x).wait_send()
    for step in range(1, lines):
        other = lax.rem(z + step, lines)
        share_copy(z, other, at(other, y, x, c)).wait_send()

    def drain_gu(p, carry):
        gu_over(p).wait_send()
        gu_plane(p).wait_send()
        gu_mate(p, 0).wait_send()
        gu_mate(p, 1).wait_send()
        return carry

    lax.fori_loop(0, SLABS, drain_gu, 0)

    def drain_d(p, carry):
        d_over(p).wait_send()
        d_plane(p).wait_send()
        d_mate(p, 0).wait_send()
        d_mate(p, 1).wait_send()
        return carry

    lax.fori_loop(0, CHUNKS, drain_d, 0)

    def drain(line, carry):
        for part in range(PIECES):
            @pl.when((line <= z) & (z < last))
            def _():
                tok_copy(line, part, up_send, above).wait_send()

            @pl.when((line >= z) & (z > 0))
            def _():
                tok_copy(line, part, down_send, below).wait_send()

        @pl.when(line != z)
        def _():
            for j in range(CHUNKS):
                line_copy(0, line, j, above).wait_send()

        return carry

    lax.fori_loop(0, lines, drain, 0)


def fused_layer(normed, shares, gate_weight, up_weight, down_weight, queries, kv_rows, sinks, out_weight):
    lines = lax.axis_size("ep") // ROW
    tok_rows, width = normed.shape
    hidden = gate_weight.shape[1]
    attn_rows, attn_width = queries.shape
    quarter = (attn_rows // TP, out_weight.shape[1])
    block = (tok_rows, width)
    sem = pltpu.SemaphoreType.DMA
    pieces = SLABS + CHUNKS
    bf16, f32 = jnp.bfloat16, jnp.float32
    flops = 12 * lines * tok_rows * width * hidden
    return pl.pallas_call(
        functools.partial(fused_kernel, lines, width),
        out_shape=(jax.ShapeDtypeStruct(block, bf16), jax.ShapeDtypeStruct(quarter, bf16)),
        in_specs=[pl.BlockSpec(memory_space=pl.ANY)] * 9,
        out_specs=(pl.BlockSpec(memory_space=pltpu.VMEM), pl.BlockSpec(memory_space=pltpu.VMEM)),
        scratch_shapes=[
            pltpu.VMEM((lines,) + block, bf16),
            pltpu.VMEM((lines,) + shares.shape, f32),
            pltpu.VMEM((ROW, width, 2 * hidden), bf16),
            pltpu.VMEM((ROW * hidden, width), bf16),
            pltpu.VMEM((ROW, tok_rows, hidden), bf16),
            pltpu.VMEM((lines,) + block, bf16),
            pltpu.VMEM((2, lines) + block, bf16),
            pltpu.VMEM(queries.shape, bf16),
            pltpu.VMEM((attn_rows + WINDOW, kv_rows.shape[1]), bf16),
            pltpu.VMEM(sinks.shape, f32),
            pltpu.VMEM(out_weight.shape, bf16),
            pltpu.VMEM((TP // CORES,) + quarter, f32),
            pltpu.VMEM((TP // CORES,) + quarter, bf16),
            pltpu.VMEM((TP // CORES,) + quarter, bf16),
            pltpu.VMEM(quarter, bf16),
            pltpu.VMEM(quarter, bf16),
            sem((9,)),
            sem((lines,)),
            sem((lines,)),
            sem((2,)),
            sem((lines, PIECES)),
            sem((lines, PIECES)),
            sem((lines, PIECES)),
            sem((pieces,)),
            sem((pieces,)),
            sem((pieces,)),
            sem((pieces,)),
            sem((2, pieces)),
            sem((2, pieces)),
            sem((lines, CHUNKS)),
            sem((2, lines, CHUNKS)),
            sem((TP // CORES,)),
            sem((TP // CORES,)),
            sem,
            sem,
        ],
        compiler_params=pltpu.CompilerParams(
            collective_id=0, has_side_effects=True, vmem_limit_bytes=56 * 1024 * 1024
        ),
        cost_estimate=pl.CostEstimate(
            flops=flops, bytes_accessed=16 * tok_rows * width * lines, transcendentals=0
        ),
    )(normed, shares, gate_weight, up_weight, down_weight, queries, kv_rows, sinks, out_weight)


def fused_path(
    queries, head_keys, head_values, sink_logits, out_weight,
    moe_input, norm_gain, routes, route_weight, gate_weight, up_weight, down_weight,
):
    targets = lax.axis_size("ep")
    values32 = moe_input.astype(jnp.float32)
    scale = lax.rsqrt(jnp.mean(values32 * values32, axis=-1, keepdims=True) + EPSILON)
    normed = (values32 * scale * norm_gain).astype(jnp.bfloat16)
    experts = jnp.arange(targets, dtype=jnp.int32)
    named = routes[:, None, :] == experts[None, :, None]
    shares = jnp.sum(jnp.where(named, route_weight[:, None, :], 0.0), axis=2).T
    kv_rows = jnp.concatenate([head_keys, head_keys, head_values, head_values], axis=1)
    sinks = jnp.broadcast_to(sink_logits[:, None], (sink_logits.shape[0], 128))
    routed, attended = fused_layer(
        normed, shares, gate_weight[0], up_weight[0], down_weight[0], queries, kv_rows, sinks,
        out_weight,
    )
    return (attended, routed)


def fits(queries, head_keys, sink_logits, moe_input, routes):
    targets = lax.axis_size("ep")
    tok_rows = moe_input.shape[0]
    return (
        2 * routes.shape[1] * tok_rows // targets >= tok_rows
        and targets == 4 * ROW
        and lax.axis_size("tp") == TP
        and head_keys.shape[1] == HEAD_DIM
        and sink_logits.shape[0] == 4
        and queries.shape[0] == SLABS * WINDOW
    )


def on_device(
    queries,
    head_keys,
    head_values,
    sink_logits,
    out_weight,
    moe_input,
    norm_gain,
    routes,
    route_weight,
    gate_weight,
    up_weight,
    down_weight,
):
    if fits(queries, head_keys, sink_logits, moe_input, routes):
        return fused_path(
            queries, head_keys, head_values, sink_logits, out_weight, moe_input, norm_gain,
            routes, route_weight, gate_weight, up_weight, down_weight,
        )
    attention_out = attend(queries, head_keys, head_values, sink_logits, out_weight)
    routed_out = experts_part(
        moe_input, norm_gain, routes, route_weight, gate_weight, up_weight, down_weight
    )
    return (attention_out, routed_out)


def solution(mesh):
    placed = (
        P("ep", "tp"),
        P("ep", "tp"),
        P("ep", "tp"),
        P("tp"),
        P("tp", None),
        P(("ep", "tp"), None),
        P(),
        P(("ep", "tp"), None),
        P(("ep", "tp"), None),
        P("ep", None, None),
        P("ep", None, None),
        P("ep", None, None),
    )
    return jax.shard_map(
        on_device,
        mesh=mesh,
        in_specs=placed,
        out_specs=(P(("ep", "tp"), None), P(("ep", "tp"), None)),
        check_vma=False,
    )
```

```python
import functools

import jax
import jax.numpy as jnp
from jax import lax
from jax.experimental import pallas as pl
from jax.experimental.pallas import tpu as pltpu
from jax.sharding import PartitionSpec as P

HEAD_DIM = 64
WINDOW = 128
SEQS = 1


EPSILON = 1e-05
NEGATIVE = -1e30


def passed_along(value, axis, steps):
    count = lax.axis_size(axis)
    first, last = (max(0, -steps), min(count, count - steps))
    return lax.ppermute(value, axis, [(source, source + steps) for source in range(first, last)])


def clamped_unit(gate_pre, up_pre):
    gate_cut = jnp.minimum(gate_pre, 7.0)
    up_cut = jnp.clip(up_pre, -7.0, 7.0)
    return gate_cut * jax.nn.sigmoid(1.702 * gate_cut) * (up_cut + 1.0)


def attend(queries, head_keys, head_values, sink_logits, out_weight):
    tok_rows = queries.shape[0]
    local_heads = sink_logits.shape[0]
    local_kv = head_keys.shape[1] // HEAD_DIM
    per_group = local_heads // local_kv
    block_count = tok_rows // WINDOW
    key_width = local_kv * HEAD_DIM
    kv_rows = jnp.concatenate([head_keys, head_values], axis=1)
    earlier = passed_along(kv_rows[tok_rows - WINDOW :], "ep", 1)
    extended = jnp.concatenate([earlier, kv_rows], axis=0)
    banded = jnp.concatenate(
        [
            extended[:tok_rows].reshape(block_count, WINDOW, 2 * key_width),
            kv_rows.reshape(block_count, WINDOW, 2 * key_width),
        ],
        axis=1,
    )
    band_keys = banded[:, :, :key_width].reshape(block_count, 2 * WINDOW, local_kv, HEAD_DIM)
    band_values = banded[:, :, key_width:].reshape(block_count, 2 * WINDOW, local_kv, HEAD_DIM)
    blocked = queries.reshape(block_count, WINDOW, local_kv, per_group, HEAD_DIM)
    scores = jnp.einsum(
        "nqkgd,nskd->nkgqs", blocked, band_keys, preferred_element_type=jnp.float32
    ) * HEAD_DIM ** (-0.5)
    offset = lax.axis_index("ep") * tok_rows
    seq_len = tok_rows * lax.axis_size("ep") // SEQS
    query_pos = offset + jnp.arange(tok_rows, dtype=jnp.int32).reshape(block_count, WINDOW)
    key_pos = (
        offset
        - WINDOW
        + (jnp.arange(block_count, dtype=jnp.int32) * WINDOW)[:, None]
        + jnp.arange(2 * WINDOW, dtype=jnp.int32)[None, :]
    )
    distance = query_pos[:, :, None] - key_pos[:, None, :]
    starts = query_pos // seq_len * seq_len
    valid = (distance >= 0) & (distance < WINDOW) & (key_pos[:, None, :] >= starts[:, :, None])
    scores = jnp.where(valid[:, None, None], scores, NEGATIVE)
    sinks = sink_logits.reshape(local_kv, per_group, 1, 1)
    maxima = jnp.maximum(jnp.max(scores, axis=-1, keepdims=True), sinks)
    powers = jnp.exp(scores - maxima)
    weights = (powers / (jnp.sum(powers, axis=-1, keepdims=True) + jnp.exp(sinks - maxima))).astype(
        jnp.bfloat16
    )
    heads_out = jnp.einsum(
        "nkgqs,nskd->nqkgd", weights, band_values, preferred_element_type=jnp.float32
    )
    heads_out = heads_out.astype(jnp.bfloat16).reshape(tok_rows, local_heads * HEAD_DIM)
    summed = lax.psum_scatter(
        jnp.dot(heads_out, out_weight, preferred_element_type=jnp.float32),
        "tp",
        scatter_dimension=0,
        tiled=True,
    )
    return summed.astype(jnp.bfloat16)


def experts_part(moe_input, norm_gain, routes, route_weight, gate_weight, up_weight, down_weight):
    tok_rows, model_width = moe_input.shape
    choice_count = routes.shape[1]
    targets = lax.axis_size("ep")
    capacity = 2 * choice_count * tok_rows // targets
    values32 = moe_input.astype(jnp.float32)
    scale = lax.rsqrt(jnp.mean(values32 * values32, axis=-1, keepdims=True) + EPSILON)
    normed = (values32 * scale * norm_gain).astype(jnp.bfloat16)
    if capacity >= tok_rows:
        experts = jnp.arange(targets, dtype=jnp.int32)
        named = routes[:, :, None] == experts[None, None, :]
        shares = jnp.sum(jnp.where(named, route_weight[:, :, None], 0.0), axis=1)
        everyone = lax.all_gather(normed, "ep", axis=0, tiled=True)
        mine = lax.all_to_all(shares.T[:, None], "ep", split_axis=0, concat_axis=0, tiled=True)
        gate_pre = jnp.dot(everyone, gate_weight[0], preferred_element_type=jnp.float32)
        up_pre = jnp.dot(everyone, up_weight[0], preferred_element_type=jnp.float32)
        act = clamped_unit(gate_pre, up_pre).astype(jnp.bfloat16)
        result = jnp.dot(act, down_weight[0], preferred_element_type=jnp.float32)
        part = result.astype(jnp.bfloat16).astype(jnp.float32) * mine.reshape(-1, 1)
        return lax.psum_scatter(
            part.astype(jnp.bfloat16), "ep", scatter_dimension=0, tiled=True
        )
    flat_routes = routes.reshape(-1)
    onehot = (flat_routes[:, None] == jnp.arange(targets, dtype=jnp.int32)[None, :]).astype(
        jnp.int32
    )
    earlier_count = jnp.sum((jnp.cumsum(onehot, axis=0) - onehot) * onehot, axis=1)
    slot_index = flat_routes * capacity + earlier_count
    copies = jnp.repeat(normed, choice_count, axis=0)
    outgoing = jnp.zeros((targets * capacity, model_width), jnp.bfloat16).at[slot_index].set(copies)
    outgoing = outgoing.reshape(targets, capacity, model_width)
    arrived = lax.all_to_all(outgoing, "ep", split_axis=0, concat_axis=0, tiled=True)
    flat_rows = arrived.reshape(-1, model_width)
    gate_pre = jnp.dot(flat_rows, gate_weight[0], preferred_element_type=jnp.float32)
    up_pre = jnp.dot(flat_rows, up_weight[0], preferred_element_type=jnp.float32)
    act = clamped_unit(gate_pre, up_pre).astype(jnp.bfloat16)
    result = jnp.dot(act, down_weight[0], preferred_element_type=jnp.float32).astype(jnp.bfloat16)
    came_back = lax.all_to_all(
        result.reshape(arrived.shape), "ep", split_axis=0, concat_axis=0, tiled=True
    )
    picked = came_back.reshape(targets * capacity, model_width)[slot_index]
    weighted = (
        picked.astype(jnp.float32).reshape(tok_rows, choice_count, model_width)
        * route_weight[:, :, None]
    )
    return jnp.sum(weighted, axis=1).astype(jnp.bfloat16)


ROW = 2
CORES = 2
TP = 4
PIECES = 4
CHUNKS = 4
SLABS = 16
LAG = 4
NORM_ROWS = 16


def fused_kernel(
    lines, width,
    rows_hbm, gain_hbm, routes_hbm, route_weight_hbm, gate_hbm, up_hbm, down_hbm,
    q_hbm, keys_hbm, values_hbm, sinks_hbm, proj_hbm,
    routed_ref, attn_ref,
    raw, gain, routes, route_weight,
    gath, shares, wgu, wd, act, onward, from_line,
    qs, ext, sinks, wo, keep, mate_out, mate_in, x_out, x_in,
    local_sem, gu_sem, share_send, share_recv, halo_sem,
    up_send, down_send, tok_recv,
    y_send, y_recv, x_send, x_recv, m_send, m_recv,
    line_send, line_recv, pair_send, pair_recv, cross_send, cross_recv,
):
    ep, tp = lax.axis_index("ep"), lax.axis_index("tp")
    z, y, x, c = ep // ROW, ep % ROW, tp // CORES, tp % CORES
    tok_rows, model_width = routed_ref.shape
    hidden = gate_hbm.shape[1]
    attn_rows = q_hbm.shape[0]
    piece = tok_rows // PIECES
    chunk = model_width // CHUNKS
    last = lines - 1
    quarter = wgu.shape[1] // TP
    slab = quarter // SLABS

    def at(zz, yy, xx, cc):
        return {"ep": zz * ROW + yy, "tp": xx * CORES + cc}

    def remote(source, target, send, recv, device):
        return pltpu.make_async_remote_copy(
            src_ref=source, dst_ref=target, send_sem=send, recv_sem=recv,
            device_id=device, device_id_type=pl.DeviceIdType.MESH,
        )

    above = at(jnp.minimum(z + 1, last), y, x, c)
    below = at(jnp.maximum(z - 1, 0), y, x, c)
    over_y, over_x, mate = at(z, 1 - y, x, c), at(z, y, 1 - x, c), at(z, y, x, 1 - c)

    def gu_load(q, half):
        place = pl.ds(q * quarter, quarter)
        source = (gate_hbm, up_hbm)[half]
        return pltpu.make_async_copy(
            source.at[place], wgu.at[0, place, pl.ds(half * hidden, hidden)], gu_sem.at[half, q]
        )

    own = pl.ds(WINDOW, attn_rows)
    loads = [
        pltpu.make_async_copy(source, target, local_sem.at[i])
        for i, (source, target) in enumerate([
            (keys_hbm, ext.at[pl.ds(0, HEAD_DIM), own]),
            (values_hbm, ext.at[pl.ds(HEAD_DIM, HEAD_DIM), own]),
            (rows_hbm, raw),
            (gain_hbm, gain),
            (routes_hbm, routes),
            (route_weight_hbm, route_weight),
            (down_hbm, wd.at[pl.ds(0, hidden)]),
            (q_hbm, qs),
            (sinks_hbm, sinks),
            (proj_hbm, wo),
        ])
    ]
    gu_load(tp, 0).start()
    gu_load(tp, 1).start()
    for load in loads:
        load.start()
    for step in range(1, TP):
        gu_load(lax.rem(tp + step, TP), 0).start()
        gu_load(lax.rem(tp + step, TP), 1).start()

    ahead = ep + 1 < lines * ROW
    behind = ep > 0
    skew = jnp.where(y == 1, z < last, z > 0)
    skew_ep = jnp.where(y == 1, jnp.minimum(ep + 1, lines * ROW - 1), jnp.maximum(ep - 1, 0))
    barrier = pltpu.get_barrier_semaphore()

    def greet(device):
        pl.semaphore_signal(barrier, inc=1, device_id=device, device_id_type=pl.DeviceIdType.MESH)

    for step in range(1, lines):
        greet(at(lax.rem(z + step, lines), y, x, c))
    greet(over_y)
    greet(over_x)
    greet(mate)

    @pl.when(skew)
    def _():
        greet({"ep": skew_ep, "tp": tp})

    pl.semaphore_wait(barrier, last + 3 + jnp.where(skew, 1, 0))

    halo = remote(
        ext.at[:, pl.ds(attn_rows, WINDOW)], ext.at[:, pl.ds(0, WINDOW)], halo_sem.at[0],
        halo_sem.at[1], {"ep": jnp.minimum(ep + 1, lines * ROW - 1), "tp": tp},
    )

    def share_copy(slot, recv_slot, device):
        return remote(
            shares.at[slot], shares.at[slot], share_send.at[recv_slot], share_recv.at[slot], device
        )

    def tok_copy(block, part, sems, device):
        view = gath.at[block, pl.ds(part * piece, piece)]
        return remote(view, view, sems.at[block, part], tok_recv.at[block, part], device)

    def gu_view(expert, q, p):
        return wgu.at[expert, pl.ds(q * quarter + p * slab, slab)]

    def d_view(expert, q, p):
        return wd.at[
            pl.ds(expert * hidden + q * (hidden // TP), hidden // TP), pl.ds(p * chunk, chunk)
        ]

    def weight_copies(view, base):
        def over_link(p):
            return remote(
                view(0, tp, p), view(1, tp, p), y_send.at[base + p], y_recv.at[base + p], over_y
            )

        def to_plane(p):
            return remote(
                view(1, tp, p), view(1, tp, p), x_send.at[base + p], x_recv.at[base + p], over_x
            )

        def to_mate(p, second):
            q = jnp.where(second == 1, (1 - x) * CORES + c, tp) if second else tp
            return remote(
                view(1, q, p), view(1, q, p), m_send.at[second, base + p],
                m_recv.at[second, base + p], mate,
            )

        return over_link, to_plane, to_mate

    gu_over, gu_plane, gu_mate = weight_copies(gu_view, 0)
    d_over, d_plane, d_mate = weight_copies(d_view, SLABS)

    loads[0].wait()
    loads[1].wait()

    @pl.when(ahead)
    def _():
        halo.start()

    gu_load(tp, 0).wait()
    gu_load(tp, 1).wait()

    def launch_gu(p, carry):
        gu_over(p).start()
        return carry

    lax.fori_loop(0, SLABS, launch_gu, 0)
    for load in loads[2:6]:
        load.wait()

    def normalize(i, carry):
        place = pl.ds(i * NORM_ROWS, NORM_ROWS)
        values32 = raw[place].astype(jnp.float32)
        mean = jnp.sum(values32 * values32, axis=-1, keepdims=True) * (1.0 / model_width)
        scale = lax.rsqrt(mean + EPSILON)
        gath[z, place] = (values32 * scale * gain[...]).astype(jnp.bfloat16)
        return carry

    lax.fori_loop(0, tok_rows // NORM_ROWS, normalize, 0)
    expert = lax.broadcasted_iota(jnp.int32, shares.shape[1:], 0)
    share = jnp.zeros(shares.shape[1:], jnp.float32)
    for choice in range(routes.shape[0]):
        named = routes[choice : choice + 1, :] == expert
        share = share + jnp.where(named, route_weight[choice : choice + 1, :], 0.0)
    shares[z] = share

    def own_tokens(first, count, upward):
        for part in range(first, first + count):
            if upward:
                tok_copy(z, part, up_send, above).start()
            else:
                tok_copy(z, part, down_send, below).start()

    half = PIECES // 2

    @pl.when(z < last)
    def _():
        own_tokens(0, half, True)

    @pl.when(z == 0)
    def _():
        own_tokens(half, half, True)

    @pl.when(z > 0)
    def _():
        own_tokens(0, half, False)

    @pl.when(z == last)
    def _():
        own_tokens(half, half, False)

    for step in range(1, lines):
        other = lax.rem(z + step, lines)
        share_copy(z, other, at(other, y, x, c)).start()
    loads[6].wait()

    def launch_d(p, carry):
        d_over(p).start()
        return carry

    lax.fori_loop(0, CHUNKS, launch_d, 0)
    for load in loads[7:]:
        load.wait()

    def arrival(i, reach):
        s = i // half
        far = s < reach
        distance = jnp.where(far, s + 1, 2 * reach - s)
        part = jnp.where(far, 0, half) + i % half
        return distance, part

    def pump_tokens(i):
        for upward in (True, False):
            reach = z if upward else last - z
            distance, part = arrival(i, reach)
            block = jnp.clip(z - distance if upward else z + distance, 0, last)

            @pl.when(i < PIECES * reach)
            def _():
                tok_copy(block, part, up_send, above).wait_recv()

            @pl.when((i < PIECES * reach) & (reach < last))
            def _():
                if upward:
                    tok_copy(block, part, up_send, above).start()
                else:
                    tok_copy(block, part, down_send, below).start()

            @pl.when((i == PIECES * reach - 1) & (reach < last))
            def _():
                own_tokens(half, half, upward)

    per_group = sinks.shape[0]
    band = 2 * WINDOW
    quarter_rows = attn_ref.shape[0]
    blocks_each = quarter_rows // WINDOW

    def pair_copy(owner_x):
        return remote(
            mate_out.at[owner_x], mate_in.at[owner_x], pair_send.at[owner_x],
            pair_recv.at[owner_x], mate,
        )

    def attend_block(n):
        q_rows = qs[pl.ds(n * WINDOW, WINDOW)] * jnp.bfloat16(HEAD_DIM ** (-0.5))
        held = ext[:, pl.ds(pl.multiple_of(n * WINDOW, WINDOW), band)]
        keys = jnp.concatenate([held[:HEAD_DIM]] * per_group, axis=0)
        values = held[HEAD_DIM:]
        q_head = lax.broadcasted_iota(jnp.int32, q_rows.shape, 1) // HEAD_DIM
        stacked = jnp.concatenate(
            [jnp.where(q_head == h, q_rows, jnp.zeros_like(q_rows)) for h in range(per_group)],
            axis=0,
        )
        scores = jnp.dot(stacked, keys, preferred_element_type=jnp.float32)
        begins = lax.rem(ep * (qs.shape[0] // WINDOW) + n, lines * ROW * (qs.shape[0] // WINDOW) // SEQS) == 0
        row = lax.broadcasted_iota(jnp.int32, (WINDOW, band), 0)
        col = lax.broadcasted_iota(jnp.int32, (WINDOW, band), 1)
        valid = (col > row) & (col <= row + WINDOW) & (col >= jnp.where(begins, WINDOW, 0))
        weights = []
        for h in range(per_group):
            score = jnp.where(valid, scores[h * WINDOW : (h + 1) * WINDOW], NEGATIVE)
            sink = sinks[h]
            top = jnp.maximum(jnp.max(score, axis=1, keepdims=True), sink)
            powers = jnp.exp(score - top)
            total = jnp.sum(powers, axis=1, keepdims=True) + jnp.exp(sink - top)
            weights.append((powers * (1.0 / total)).astype(jnp.bfloat16))
        blank = jnp.zeros_like(values)
        spread = jnp.concatenate(
            [
                jnp.concatenate([values if g == h else blank for g in range(per_group)], axis=1)
                for h in range(per_group)
            ],
            axis=0,
        )
        heads = lax.dot_general(
            jnp.concatenate(weights, axis=1), spread, (((1,), (1,)), ((), ())),
            preferred_element_type=jnp.float32,
        ).astype(jnp.bfloat16)
        owner = n // blocks_each
        owner_x, owner_c = owner // CORES, owner % CORES
        place = pl.ds((n % blocks_each) * WINDOW, WINDOW)
        share = jnp.dot(heads, wo[...], preferred_element_type=jnp.float32)

        @pl.when(owner_c == c)
        def _():
            keep[owner_x, place] = share

        @pl.when(owner_c != c)
        def _():
            mate_out[owner_x, place] = share.astype(jnp.bfloat16)

    each = SLABS * WINDOW // attn_rows

    def slot(i, carry):
        gu_over(i).wait_recv()
        gu_plane(i).start()
        gu_mate(i, 0).start()

        @pl.when(i >= LAG)
        def _():
            gu_plane(i - LAG).wait_recv()
            gu_mate(i - LAG, 1).start()

        @pl.when(i % each == 0)
        def _():
            n = lax.rem(i // each + 1, attn_rows // WINDOW)

            @pl.when((n == 0) & behind)
            def _():
                halo.wait_recv()

            @pl.when((n == 0) & (ep == 0))
            def _():
                ext[:, pl.ds(0, WINDOW)] = jnp.zeros((ext.shape[0], WINDOW), ext.dtype)

            attend_block(n)

        @pl.when(i % each == each - 1)
        def _():
            pump_tokens(i // each)

        @pl.when((i % each == each - 1) & (i // each < lines))
        def _():
            block = jnp.minimum(i // each, last)

            @pl.when(z == 0)
            def _():
                from_line[0, block] = jnp.zeros(from_line.shape[2:], from_line.dtype)

            @pl.when(z == last)
            def _():
                from_line[1, block] = jnp.zeros(from_line.shape[2:], from_line.dtype)

        return carry

    lax.fori_loop(0, SLABS, slot, 0)
    for owner_x in range(TP // CORES):
        pair_copy(owner_x).start()

    def pass_down(j):
        d_over(j).wait_recv()
        d_plane(j).start()
        d_mate(j, 0).start()

    for p in range(SLABS - LAG, SLABS):
        if p == SLABS - LAG // 2:
            pass_down(0)
        gu_plane(p).wait_recv()
        gu_mate(p, 1).start()
    for step in range(1, lines):
        source = lax.rem(z + step, lines)
        share_copy(source, source, at(source, y, x, c)).wait_recv()
    for step in range(1, TP):
        gu_load(lax.rem(tp + step, TP), 0).wait()
        gu_load(lax.rem(tp + step, TP), 1).wait()

    square = (tok_rows, tok_rows)
    eye = lax.broadcasted_iota(jnp.int32, square, 0) == lax.broadcasted_iota(jnp.int32, square, 1)

    def activate(block, first, end):
        def one(expert, carry):
            pre = jnp.dot(gath[block], wgu[expert], preferred_element_type=jnp.float32)
            unit = clamped_unit(pre[:, :hidden], pre[:, hidden:])
            named = z * ROW + jnp.where(expert == 1, 1 - y, y)
            column = jnp.sum(
                jnp.where(eye, shares[block, pl.ds(named, 1), :], 0.0), axis=1, keepdims=True
            )
            act[expert] = (unit * column).astype(jnp.bfloat16)
            return carry

        lax.fori_loop(first, end, one, 0)

    def partial(cols):
        both = jnp.concatenate([act[0], act[1]], axis=1)
        return jnp.dot(both, wd[:, cols], preferred_element_type=jnp.float32)

    def line_copy(downward, block, j, device):
        cols = pl.ds(j * chunk, chunk)
        return remote(
            onward.at[block, :, cols], from_line.at[downward, block, :, cols],
            line_send.at[block, j], line_recv.at[downward, block, j], device,
        )

    def pick(k):
        block = 0
        for zz in range(lines):
            others = sorted(
                (b for b in range(lines) if b != zz),
                key=lambda b: (-abs(b - zz), min(b, last - b)),
            )
            for kk, b in enumerate(others):
                block = jnp.where((z == zz) & (k == kk), b, block)
        return block

    def cross_copy():
        return remote(x_out, x_in, cross_send, cross_recv, over_x)

    def visit(k, carry):
        block = pick(k)
        downward = jnp.where(block < z, 1, 0)

        @pl.when((k > 0) & ((z == 0) | (z == last)))
        def _():
            for e in range(half):
                distance, part = arrival(PIECES * (lines - 2) + (k - 1) * half + e, last)
                source = jnp.clip(jnp.where(z == 0, distance, last - distance), 0, last)
                tok_copy(source, part, up_send, above).wait_recv()

        activate(block, jnp.where(k == 0, 1, 0), ROW)
        device = at(jnp.clip(jnp.where(downward == 1, z - 1, z + 1), 0, last), y, x, c)
        inner = jnp.where(downward == 1, z < last, z > 0)

        def one(j, carry):
            @pl.when(k == 0)
            def _():
                @pl.when(j + 2 < CHUNKS)
                def _():
                    pass_down(jnp.minimum(j + 2, CHUNKS - 1))

                d_plane(j).wait_recv()
                d_mate(j, 1).start()
                d_mate(j, 0).wait_recv()
                d_mate(j, 1).wait_recv()

            cols = pl.ds(pl.multiple_of(j * chunk, chunk), chunk)
            own = partial(cols)

            @pl.when(inner)
            def _():
                line_copy(downward, block, j, device).wait_recv()

            onward[block, :, cols] = (
                own + from_line[downward, block, :, cols].astype(jnp.float32)
            ).astype(jnp.bfloat16)
            line_copy(downward, block, j, device).start()

            @pl.when((k == 0) & (j == CHUNKS - 3))
            def _():
                for owner_x in range(TP // CORES):
                    pair_copy(owner_x).wait_recv()
                x_out[...] = (
                    keep[1 - x] + mate_in[1 - x].astype(jnp.float32)
                ).astype(jnp.bfloat16)
                cross_copy().start()

            return carry

        lax.fori_loop(0, CHUNKS, one, 0)
        return carry

    pass_down(1)
    activate(pick(0), 0, 1)

    def gather_gu(p, carry):
        gu_mate(p, 0).wait_recv()
        gu_mate(p, 1).wait_recv()
        return carry

    lax.fori_loop(0, SLABS, gather_gu, 0)
    lax.fori_loop(0, last, visit, 0)
    activate(z, 0, ROW)

    def finish(j, carry):
        cols = pl.ds(pl.multiple_of(j * chunk, chunk), chunk)
        own = partial(cols)

        @pl.when(z > 0)
        def _():
            line_copy(0, z, j, above).wait_recv()

        @pl.when(z < last)
        def _():
            line_copy(1, z, j, above).wait_recv()

        routed_ref[:, cols] = (
            own + from_line[0, z, :, cols].astype(jnp.float32)
            + from_line[1, z, :, cols].astype(jnp.float32)
        ).astype(jnp.bfloat16)
        return carry

    cross_copy().wait_recv()
    attn_ref[...] = (
        keep[x] + mate_in[x].astype(jnp.float32) + x_in[...].astype(jnp.float32)
    ).astype(jnp.bfloat16)
    lax.fori_loop(0, CHUNKS, finish, 0)

    @pl.when(ahead)
    def _():
        halo.wait_send()

    cross_copy().wait_send()
    for owner_x in range(TP // CORES):
        pair_copy(owner_x).wait_send()
    for step in range(1, lines):
        other = lax.rem(z + step, lines)
        share_copy(z, other, at(other, y, x, c)).wait_send()

    def drain_gu(p, carry):
        gu_over(p).wait_send()
        gu_plane(p).wait_send()
        gu_mate(p, 0).wait_send()
        gu_mate(p, 1).wait_send()
        return carry

    lax.fori_loop(0, SLABS, drain_gu, 0)

    def drain_d(p, carry):
        d_over(p).wait_send()
        d_plane(p).wait_send()
        d_mate(p, 0).wait_send()
        d_mate(p, 1).wait_send()
        return carry

    lax.fori_loop(0, CHUNKS, drain_d, 0)

    def drain(line, carry):
        for part in range(PIECES):
            @pl.when((line <= z) & (z < last))
            def _():
                tok_copy(line, part, up_send, above).wait_send()

            @pl.when((line >= z) & (z > 0))
            def _():
                tok_copy(line, part, down_send, below).wait_send()

        @pl.when(line != z)
        def _():
            for j in range(CHUNKS):
                line_copy(0, line, j, above).wait_send()

        return carry

    lax.fori_loop(0, lines, drain, 0)


def fused_layer(*operands):
    moe_input, _, routes, _, gate_weight, _, _, queries, keys, _, sinks, out_weight = operands
    targets = lax.axis_size("ep")
    lines = targets // ROW
    tok_rows, width = moe_input.shape
    hidden = gate_weight.shape[1]
    attn_rows = queries.shape[0]
    quarter = (attn_rows // TP, out_weight.shape[1])
    block = (tok_rows, width)
    sem = pltpu.SemaphoreType.DMA
    pieces = SLABS + CHUNKS
    bf16, f32 = jnp.bfloat16, jnp.float32
    flops = 12 * lines * tok_rows * width * hidden
    return pl.pallas_call(
        functools.partial(fused_kernel, lines, width),
        out_shape=(pltpu.VMEM(block, bf16), pltpu.VMEM(quarter, bf16)),
        in_specs=[pl.BlockSpec(memory_space=pl.ANY)] * len(operands),
        out_specs=(pl.BlockSpec(memory_space=pltpu.VMEM), pl.BlockSpec(memory_space=pltpu.VMEM)),
        scratch_shapes=[
            pltpu.VMEM(block, bf16),
            pltpu.VMEM((1, width), f32),
            pltpu.VMEM(routes.shape, jnp.int32),
            pltpu.VMEM(routes.shape, f32),
            pltpu.VMEM((lines,) + block, bf16),
            pltpu.VMEM((lines, targets, tok_rows), f32),
            pltpu.VMEM((ROW, width, 2 * hidden), bf16),
            pltpu.VMEM((ROW * hidden, width), bf16),
            pltpu.VMEM((ROW, tok_rows, hidden), bf16),
            pltpu.VMEM((lines,) + block, bf16),
            pltpu.VMEM((2, lines) + block, bf16),
            pltpu.VMEM(queries.shape, bf16),
            pltpu.VMEM((2 * HEAD_DIM, WINDOW + attn_rows), bf16),
            pltpu.SMEM(sinks.shape, f32),
            pltpu.VMEM(out_weight.shape, bf16),
            pltpu.VMEM((TP // CORES,) + quarter, f32),
            pltpu.VMEM((TP // CORES,) + quarter, bf16),
            pltpu.VMEM((TP // CORES,) + quarter, bf16),
            pltpu.VMEM(quarter, bf16),
            pltpu.VMEM(quarter, bf16),
            sem((10,)),
            sem((2, TP)),
            sem((lines,)),
            sem((lines,)),
            sem((2,)),
            sem((lines, PIECES)),
            sem((lines, PIECES)),
            sem((lines, PIECES)),
            sem((pieces,)),
            sem((pieces,)),
            sem((pieces,)),
            sem((pieces,)),
            sem((2, pieces)),
            sem((2, pieces)),
            sem((lines, CHUNKS)),
            sem((2, lines, CHUNKS)),
            sem((TP // CORES,)),
            sem((TP // CORES,)),
            sem,
            sem,
        ],
        compiler_params=pltpu.CompilerParams(
            collective_id=0, has_side_effects=True, vmem_limit_bytes=56 * 1024 * 1024
        ),
        cost_estimate=pl.CostEstimate(
            flops=flops, bytes_accessed=16 * tok_rows * width * lines, transcendentals=0
        ),
    )(*operands)


def fused_path(
    queries, head_keys, head_values, sink_logits, out_weight,
    moe_input, norm_gain, routes, route_weight, gate_weight, up_weight, down_weight,
):
    routed, attended = fused_layer(
        moe_input, norm_gain.reshape(1, -1), routes.T, route_weight.T,
        gate_weight[0], up_weight[0], down_weight[0],
        queries, head_keys.T, head_values.T, sink_logits, out_weight,
    )
    return (attended, routed)


def fits(queries, head_keys, sink_logits, moe_input, routes):
    targets = lax.axis_size("ep")
    tok_rows = moe_input.shape[0]
    return (
        2 * routes.shape[1] * tok_rows // targets >= tok_rows
        and targets == 4 * ROW
        and lax.axis_size("tp") == TP
        and head_keys.shape[1] == HEAD_DIM
        and sink_logits.shape[0] == 4
        and (SLABS * WINDOW) % queries.shape[0] == 0
        and queries.shape[0] >= 4 * ROW * WINDOW
    )


def on_device(
    queries,
    head_keys,
    head_values,
    sink_logits,
    out_weight,
    moe_input,
    norm_gain,
    routes,
    route_weight,
    gate_weight,
    up_weight,
    down_weight,
):
    if fits(queries, head_keys, sink_logits, moe_input, routes):
        return fused_path(
            queries, head_keys, head_values, sink_logits, out_weight, moe_input, norm_gain,
            routes, route_weight, gate_weight, up_weight, down_weight,
        )
    attention_out = attend(queries, head_keys, head_values, sink_logits, out_weight)
    routed_out = experts_part(
        moe_input, norm_gain, routes, route_weight, gate_weight, up_weight, down_weight
    )
    return (attention_out, routed_out)


def solution(mesh):
    placed = (
        P("ep", "tp"),
        P("ep", "tp"),
        P("ep", "tp"),
        P("tp"),
        P("tp", None),
        P(("ep", "tp"), None),
        P(),
        P(("ep", "tp"), None),
        P(("ep", "tp"), None),
        P("ep", None, None),
        P("ep", None, None),
        P("ep", None, None),
    )
    return jax.shard_map(
        on_device,
        mesh=mesh,
        in_specs=placed,
        out_specs=(P(("ep", "tp"), None), P(("ep", "tp"), None)),
        check_vma=False,
    )
```

```python
import functools

import jax
import jax.numpy as jnp
from jax import lax
from jax.experimental import pallas as pl
from jax.experimental.pallas import tpu as pltpu
from jax.sharding import PartitionSpec as P

HEAD_DIM = 64
WINDOW = 128
SEQS = 1


EPSILON = 1e-05
NEGATIVE = -1e30


def passed_along(value, axis, steps):
    count = lax.axis_size(axis)
    first, last = (max(0, -steps), min(count, count - steps))
    return lax.ppermute(value, axis, [(source, source + steps) for source in range(first, last)])


def clamped_unit(gate_pre, up_pre):
    gate_cut = jnp.minimum(gate_pre, 7.0)
    up_cut = jnp.clip(up_pre, -7.0, 7.0)
    return gate_cut * jax.nn.sigmoid(1.702 * gate_cut) * (up_cut + 1.0)


def attend(queries, head_keys, head_values, sink_logits, out_weight):
    tok_rows = queries.shape[0]
    local_heads = sink_logits.shape[0]
    local_kv = head_keys.shape[1] // HEAD_DIM
    per_group = local_heads // local_kv
    block_count = tok_rows // WINDOW
    key_width = local_kv * HEAD_DIM
    kv_rows = jnp.concatenate([head_keys, head_values], axis=1)
    earlier = passed_along(kv_rows[tok_rows - WINDOW :], "ep", 1)
    extended = jnp.concatenate([earlier, kv_rows], axis=0)
    banded = jnp.concatenate(
        [
            extended[:tok_rows].reshape(block_count, WINDOW, 2 * key_width),
            kv_rows.reshape(block_count, WINDOW, 2 * key_width),
        ],
        axis=1,
    )
    band_keys = banded[:, :, :key_width].reshape(block_count, 2 * WINDOW, local_kv, HEAD_DIM)
    band_values = banded[:, :, key_width:].reshape(block_count, 2 * WINDOW, local_kv, HEAD_DIM)
    blocked = queries.reshape(block_count, WINDOW, local_kv, per_group, HEAD_DIM)
    scores = jnp.einsum(
        "nqkgd,nskd->nkgqs", blocked, band_keys, preferred_element_type=jnp.float32
    ) * HEAD_DIM ** (-0.5)
    offset = lax.axis_index("ep") * tok_rows
    seq_len = tok_rows * lax.axis_size("ep") // SEQS
    query_pos = offset + jnp.arange(tok_rows, dtype=jnp.int32).reshape(block_count, WINDOW)
    key_pos = (
        offset
        - WINDOW
        + (jnp.arange(block_count, dtype=jnp.int32) * WINDOW)[:, None]
        + jnp.arange(2 * WINDOW, dtype=jnp.int32)[None, :]
    )
    distance = query_pos[:, :, None] - key_pos[:, None, :]
    starts = query_pos // seq_len * seq_len
    valid = (distance >= 0) & (distance < WINDOW) & (key_pos[:, None, :] >= starts[:, :, None])
    scores = jnp.where(valid[:, None, None], scores, NEGATIVE)
    sinks = sink_logits.reshape(local_kv, per_group, 1, 1)
    maxima = jnp.maximum(jnp.max(scores, axis=-1, keepdims=True), sinks)
    powers = jnp.exp(scores - maxima)
    weights = (powers / (jnp.sum(powers, axis=-1, keepdims=True) + jnp.exp(sinks - maxima))).astype(
        jnp.bfloat16
    )
    heads_out = jnp.einsum(
        "nkgqs,nskd->nqkgd", weights, band_values, preferred_element_type=jnp.float32
    )
    heads_out = heads_out.astype(jnp.bfloat16).reshape(tok_rows, local_heads * HEAD_DIM)
    summed = lax.psum_scatter(
        jnp.dot(heads_out, out_weight, preferred_element_type=jnp.float32),
        "tp",
        scatter_dimension=0,
        tiled=True,
    )
    return summed.astype(jnp.bfloat16)


def experts_part(moe_input, norm_gain, routes, route_weight, gate_weight, up_weight, down_weight):
    tok_rows, model_width = moe_input.shape
    choice_count = routes.shape[1]
    targets = lax.axis_size("ep")
    capacity = 2 * choice_count * tok_rows // targets
    values32 = moe_input.astype(jnp.float32)
    scale = lax.rsqrt(jnp.mean(values32 * values32, axis=-1, keepdims=True) + EPSILON)
    normed = (values32 * scale * norm_gain).astype(jnp.bfloat16)
    if capacity >= tok_rows:
        experts = jnp.arange(targets, dtype=jnp.int32)
        named = routes[:, :, None] == experts[None, None, :]
        shares = jnp.sum(jnp.where(named, route_weight[:, :, None], 0.0), axis=1)
        everyone = lax.all_gather(normed, "ep", axis=0, tiled=True)
        mine = lax.all_to_all(shares.T[:, None], "ep", split_axis=0, concat_axis=0, tiled=True)
        gate_pre = jnp.dot(everyone, gate_weight[0], preferred_element_type=jnp.float32)
        up_pre = jnp.dot(everyone, up_weight[0], preferred_element_type=jnp.float32)
        act = clamped_unit(gate_pre, up_pre).astype(jnp.bfloat16)
        result = jnp.dot(act, down_weight[0], preferred_element_type=jnp.float32)
        part = result.astype(jnp.bfloat16).astype(jnp.float32) * mine.reshape(-1, 1)
        return lax.psum_scatter(
            part.astype(jnp.bfloat16), "ep", scatter_dimension=0, tiled=True
        )
    flat_routes = routes.reshape(-1)
    onehot = (flat_routes[:, None] == jnp.arange(targets, dtype=jnp.int32)[None, :]).astype(
        jnp.int32
    )
    earlier_count = jnp.sum((jnp.cumsum(onehot, axis=0) - onehot) * onehot, axis=1)
    slot_index = flat_routes * capacity + earlier_count
    copies = jnp.repeat(normed, choice_count, axis=0)
    outgoing = jnp.zeros((targets * capacity, model_width), jnp.bfloat16).at[slot_index].set(copies)
    outgoing = outgoing.reshape(targets, capacity, model_width)
    arrived = lax.all_to_all(outgoing, "ep", split_axis=0, concat_axis=0, tiled=True)
    flat_rows = arrived.reshape(-1, model_width)
    gate_pre = jnp.dot(flat_rows, gate_weight[0], preferred_element_type=jnp.float32)
    up_pre = jnp.dot(flat_rows, up_weight[0], preferred_element_type=jnp.float32)
    act = clamped_unit(gate_pre, up_pre).astype(jnp.bfloat16)
    result = jnp.dot(act, down_weight[0], preferred_element_type=jnp.float32).astype(jnp.bfloat16)
    came_back = lax.all_to_all(
        result.reshape(arrived.shape), "ep", split_axis=0, concat_axis=0, tiled=True
    )
    picked = came_back.reshape(targets * capacity, model_width)[slot_index]
    weighted = (
        picked.astype(jnp.float32).reshape(tok_rows, choice_count, model_width)
        * route_weight[:, :, None]
    )
    return jnp.sum(weighted, axis=1).astype(jnp.bfloat16)


ROW = 2
CORES = 2
TP = 4
PIECES = 4
CHUNKS = 8
SLABS = 16
LAG = 4
AHEAD = 3
NORM_ROWS = 16


def fused_kernel(
    lines, width,
    rows_hbm, gain_hbm, routes_hbm, route_weight_hbm, gate_hbm, up_hbm, down_hbm,
    q_hbm, keys_hbm, values_hbm, sinks_hbm, proj_hbm,
    routed_ref, attn_ref,
    raw, gain, routes, route_weight,
    gath, shares, wgu, wd, act, onward, from_line,
    qs, ext, sinks, wo, keep, mate_out, mate_in, x_out, x_in,
    local_sem, gu_sem, share_sem, halo_sem,
    up_send, down_send, tok_recv,
    y_send, y_recv, x_send, x_recv, m_send, gm_recv, m_recv,
    line_send, line_recv, pair_sem, cross_send, cross_recv,
):
    ep, tp = lax.axis_index("ep"), lax.axis_index("tp")
    z, y, x, c = ep // ROW, ep % ROW, tp // CORES, tp % CORES
    tok_rows, model_width = routed_ref.shape
    hidden = gate_hbm.shape[1]
    attn_rows = q_hbm.shape[0]
    piece = tok_rows // PIECES
    chunk = model_width // CHUNKS
    last = lines - 1
    quarter = wgu.shape[1] // TP
    slab = quarter // SLABS

    def at(zz, yy, xx, cc):
        return {"ep": zz * ROW + yy, "tp": xx * CORES + cc}

    def remote(source, target, send, recv, device):
        return pltpu.make_async_remote_copy(
            src_ref=source, dst_ref=target, send_sem=send, recv_sem=recv,
            device_id=device, device_id_type=pl.DeviceIdType.MESH,
        )

    above = at(jnp.minimum(z + 1, last), y, x, c)
    below = at(jnp.maximum(z - 1, 0), y, x, c)
    over_y, over_x, mate = at(z, 1 - y, x, c), at(z, y, 1 - x, c), at(z, y, x, 1 - c)

    def gu_load(q, half):
        place = pl.ds(q * quarter, quarter)
        source = (gate_hbm, up_hbm)[half]
        return pltpu.make_async_copy(
            source.at[place], wgu.at[0, place, pl.ds(half * hidden, hidden)],
            gu_sem.at[jnp.where(q == tp, 0, 1)],
        )

    def loaded(target, semaphore):
        pltpu.make_async_copy(target, target, semaphore).wait()

    own = pl.ds(WINDOW, attn_rows)
    loads = [
        pltpu.make_async_copy(source, target, local_sem.at[max(i - 1, 0)])
        for i, (source, target) in enumerate([
            (keys_hbm, ext.at[pl.ds(0, HEAD_DIM), own]),
            (values_hbm, ext.at[pl.ds(HEAD_DIM, HEAD_DIM), own]),
            (rows_hbm, raw),
            (gain_hbm, gain),
            (routes_hbm, routes),
            (route_weight_hbm, route_weight),
            (down_hbm, wd.at[pl.ds(0, hidden)]),
            (q_hbm, qs),
            (sinks_hbm, sinks),
            (proj_hbm, wo),
        ])
    ]
    gu_load(tp, 0).start()
    gu_load(tp, 1).start()
    for load in loads:
        load.start()
    for step in range(1, TP):
        gu_load(lax.rem(tp + step, TP), 0).start()
        gu_load(lax.rem(tp + step, TP), 1).start()

    ahead = ep + 1 < lines * ROW
    behind = ep > 0
    skew = jnp.where(y == 1, z < last, z > 0)
    skew_ep = jnp.where(y == 1, jnp.minimum(ep + 1, lines * ROW - 1), jnp.maximum(ep - 1, 0))
    barrier = pltpu.get_barrier_semaphore()

    def greet(device):
        pl.semaphore_signal(barrier, inc=1, device_id=device, device_id_type=pl.DeviceIdType.MESH)

    for step in range(1, lines):
        greet(at(lax.rem(z + step, lines), y, x, c))
    greet(over_y)
    greet(over_x)
    greet(mate)

    @pl.when(skew)
    def _():
        greet({"ep": skew_ep, "tp": tp})

    pl.semaphore_wait(barrier, last + 3 + jnp.where(skew, 1, 0))

    halo = remote(
        ext.at[:, pl.ds(attn_rows, WINDOW)], ext.at[:, pl.ds(0, WINDOW)], halo_sem.at[0],
        halo_sem.at[1], {"ep": jnp.minimum(ep + 1, lines * ROW - 1), "tp": tp},
    )

    def share_copy(slot, device):
        return remote(
            shares.at[slot], shares.at[slot], share_sem.at[0], share_sem.at[1], device
        )

    def all_of(view, send, recv):
        return remote(view, view, send, recv, mate)

    def shares_done():
        return all_of(shares.at[pl.ds(0, last)], share_sem.at[0], share_sem.at[1])

    def tok_copy(block, part, sems, device):
        view = gath.at[block, pl.ds(part * piece, piece)]
        return remote(view, view, sems.at[block], tok_recv.at[block, part], device)

    def gu_view(expert, q, p):
        return wgu.at[expert, pl.ds(q * quarter + p * slab, slab)]

    def d_view(expert, q, p):
        return wd.at[
            pl.ds(expert * hidden + q * (hidden // TP), hidden // TP), pl.ds(p * chunk, chunk)
        ]

    def weight_copies(view, kind, base, mate_recv):
        def over_link(p):
            return remote(
                view(0, tp, p), view(1, tp, p), y_send.at[kind], y_recv.at[base + p], over_y
            )

        def to_plane(p):
            return remote(
                view(1, tp, p), view(1, tp, p), x_send.at[kind], x_recv.at[base + p], over_x
            )

        def to_mate(p, second):
            q = (1 - x) * CORES + c if second else tp
            return remote(
                view(1, q, p), view(1, q, p), m_send.at[kind, second], mate_recv(second, p), mate
            )

        return over_link, to_plane, to_mate

    gu_over, gu_plane, gu_mate = weight_copies(gu_view, 0, 0, lambda second, p: gm_recv.at[second])
    d_over, d_plane, d_mate = weight_copies(
        d_view, 1, SLABS, lambda second, p: m_recv.at[second, p]
    )
    gu_whole = wgu.at[1, pl.ds(0, quarter)]
    d_whole = wd.at[pl.ds(0, hidden // TP)]

    loaded(ext.at[:, own], local_sem.at[0])

    @pl.when(ahead)
    def _():
        halo.start()

    loaded(wgu.at[0, pl.ds(0, quarter)], gu_sem.at[0])

    def launch_gu(p, carry):
        gu_over(p).start()
        return carry

    lax.fori_loop(0, SLABS, launch_gu, 0)
    for load in loads[2:6]:
        load.wait()

    def normalize(i, carry):
        place = pl.ds(i * NORM_ROWS, NORM_ROWS)
        values32 = raw[place].astype(jnp.float32)
        mean = jnp.sum(values32 * values32, axis=-1, keepdims=True) * (1.0 / model_width)
        scale = lax.rsqrt(mean + EPSILON)
        gath[z, place] = (values32 * scale * gain[...]).astype(jnp.bfloat16)
        return carry

    lax.fori_loop(0, tok_rows // NORM_ROWS, normalize, 0)
    expert = lax.broadcasted_iota(jnp.int32, shares.shape[1:], 0)
    share = jnp.zeros(shares.shape[1:], jnp.float32)
    for choice in range(routes.shape[0]):
        named = routes[choice : choice + 1, :] == expert
        share = share + jnp.where(named, route_weight[choice : choice + 1, :], 0.0)
    shares[z] = share

    def own_tokens(first, count, upward):
        for part in range(first, first + count):
            if upward:
                tok_copy(z, part, up_send, above).start()
            else:
                tok_copy(z, part, down_send, below).start()

    half = PIECES // 2

    @pl.when(z < last)
    def _():
        own_tokens(0, half, True)

    @pl.when(z == 0)
    def _():
        own_tokens(half, half, True)

    @pl.when(z > 0)
    def _():
        own_tokens(0, half, False)

    @pl.when(z == last)
    def _():
        own_tokens(half, half, False)

    for step in range(1, lines):
        other = lax.rem(z + step, lines)
        share_copy(z, at(other, y, x, c)).start()
    loads[6].wait()

    def launch_d(p, carry):
        d_over(p).start()
        return carry

    lax.fori_loop(0, CHUNKS, launch_d, 0)
    for load in loads[7:]:
        load.wait()

    def arrival(i, reach):
        s = i // half
        far = s < reach
        distance = jnp.where(far, s + 1, 2 * reach - s)
        part = jnp.where(far, 0, half) + i % half
        return distance, part

    def pump_tokens(i):
        for upward in (True, False):
            reach = z if upward else last - z
            distance, part = arrival(i, reach)
            block = jnp.clip(z - distance if upward else z + distance, 0, last)

            @pl.when(i < PIECES * reach)
            def _():
                tok_copy(block, part, up_send, above).wait_recv()

            @pl.when((i < PIECES * reach) & (reach < last))
            def _():
                if upward:
                    tok_copy(block, part, up_send, above).start()
                else:
                    tok_copy(block, part, down_send, below).start()

            @pl.when((i == PIECES * reach - 1) & (reach < last))
            def _():
                own_tokens(half, half, upward)

    per_group = sinks.shape[0]
    band = 2 * WINDOW
    quarter_rows = attn_ref.shape[0]
    blocks_each = quarter_rows // WINDOW

    def pair_copy(owner_x):
        return remote(
            mate_out.at[owner_x], mate_in.at[owner_x], pair_sem.at[0], pair_sem.at[1], mate
        )

    def attend_block(n):
        q_rows = qs[pl.ds(n * WINDOW, WINDOW)] * jnp.bfloat16(HEAD_DIM ** (-0.5))
        held = ext[:, pl.ds(pl.multiple_of(n * WINDOW, WINDOW), band)]
        keys = jnp.concatenate([held[:HEAD_DIM]] * per_group, axis=0)
        values = held[HEAD_DIM:]
        q_head = lax.broadcasted_iota(jnp.int32, q_rows.shape, 1) // HEAD_DIM
        stacked = jnp.concatenate(
            [jnp.where(q_head == h, q_rows, jnp.zeros_like(q_rows)) for h in range(per_group)],
            axis=0,
        )
        scores = jnp.dot(stacked, keys, preferred_element_type=jnp.float32)
        begins = lax.rem(ep * (qs.shape[0] // WINDOW) + n, lines * ROW * (qs.shape[0] // WINDOW) // SEQS) == 0
        row = lax.broadcasted_iota(jnp.int32, (WINDOW, band), 0)
        col = lax.broadcasted_iota(jnp.int32, (WINDOW, band), 1)
        valid = (col > row) & (col <= row + WINDOW) & (col >= jnp.where(begins, WINDOW, 0))
        weights = []
        for h in range(per_group):
            score = jnp.where(valid, scores[h * WINDOW : (h + 1) * WINDOW], NEGATIVE)
            sink = sinks[h]
            top = jnp.maximum(jnp.max(score, axis=1, keepdims=True), sink)
            powers = jnp.exp(score - top)
            total = jnp.sum(powers, axis=1, keepdims=True) + jnp.exp(sink - top)
            weights.append((powers * (1.0 / total)).astype(jnp.bfloat16))
        blank = jnp.zeros_like(values)
        spread = jnp.concatenate(
            [
                jnp.concatenate([values if g == h else blank for g in range(per_group)], axis=1)
                for h in range(per_group)
            ],
            axis=0,
        )
        heads = lax.dot_general(
            jnp.concatenate(weights, axis=1), spread, (((1,), (1,)), ((), ())),
            preferred_element_type=jnp.float32,
        ).astype(jnp.bfloat16)
        owner = n // blocks_each
        owner_x, owner_c = owner // CORES, owner % CORES
        place = pl.ds((n % blocks_each) * WINDOW, WINDOW)
        share = jnp.dot(heads, wo[...], preferred_element_type=jnp.float32)

        @pl.when(owner_c == c)
        def _():
            keep[owner_x, place] = share

        @pl.when(owner_c != c)
        def _():
            mate_out[owner_x, place] = share.astype(jnp.bfloat16)

    each = SLABS * WINDOW // attn_rows

    def slot(i, carry):
        gu_over(i).wait_recv()
        gu_plane(i).start()
        gu_mate(i, 0).start()

        @pl.when(i >= LAG)
        def _():
            gu_plane(i - LAG).wait_recv()
            gu_mate(i - LAG, 1).start()

        @pl.when(i % each == 0)
        def _():
            n = lax.rem(i // each + 1, attn_rows // WINDOW)

            @pl.when((n == 0) & behind)
            def _():
                halo.wait_recv()

            @pl.when((n == 0) & (ep == 0))
            def _():
                ext[:, pl.ds(0, WINDOW)] = jnp.zeros((ext.shape[0], WINDOW), ext.dtype)

            attend_block(n)

        @pl.when(i % each == each - 1)
        def _():
            pump_tokens(i // each)

        @pl.when((i % each == each - 1) & (i // each < lines))
        def _():
            block = jnp.minimum(i // each, last)

            @pl.when(z == 0)
            def _():
                from_line[0, block] = jnp.zeros(from_line.shape[2:], from_line.dtype)

            @pl.when(z == last)
            def _():
                from_line[1, block] = jnp.zeros(from_line.shape[2:], from_line.dtype)

        return carry

    lax.fori_loop(0, SLABS, slot, 0)
    for owner_x in range(TP // CORES):
        pair_copy(owner_x).start()

    def pass_down(j):
        d_over(j).wait_recv()
        d_plane(j).start()
        d_mate(j, 0).start()

    def late(p, carry):
        gu_plane(p).wait_recv()
        gu_mate(p, 1).start()
        return carry

    shares_done().wait_recv()
    loaded(wgu.at[0, pl.ds(quarter, (TP - 1) * quarter)], gu_sem.at[1])

    square = (tok_rows, tok_rows)
    eye = lax.broadcasted_iota(jnp.int32, square, 0) == lax.broadcasted_iota(jnp.int32, square, 1)

    def activate(block, first, end):
        def one(expert, carry):
            pre = jnp.dot(gath[block], wgu[expert], preferred_element_type=jnp.float32)
            unit = clamped_unit(pre[:, :hidden], pre[:, hidden:])
            named = z * ROW + jnp.where(expert == 1, 1 - y, y)
            column = jnp.sum(
                jnp.where(eye, shares[block, pl.ds(named, 1), :], 0.0), axis=1, keepdims=True
            )
            act[expert] = (unit * column).astype(jnp.bfloat16)
            return carry

        lax.fori_loop(first, end, one, 0)

    def partial(cols):
        both = jnp.concatenate([act[0], act[1]], axis=1)
        return jnp.dot(both, wd[:, cols], preferred_element_type=jnp.float32)

    def line_copy(downward, block, j, device, holder):
        cols = pl.ds(j * chunk, chunk)
        row = jnp.where(downward == 1, lines - holder + block, block - holder)
        return remote(
            onward.at[block, :, cols], from_line.at[downward, block, :, cols],
            line_send.at[block], line_recv.at[row, j], device,
        )

    def pick(k):
        block = 0
        for zz in range(lines):
            others = sorted(
                (b for b in range(lines) if b != zz),
                key=lambda b: (-abs(b - zz), min(b, last - b)),
            )
            for kk, b in enumerate(others):
                block = jnp.where((z == zz) & (k == kk), b, block)
        return block

    def cross_copy():
        return remote(x_out, x_in, cross_send, cross_recv, over_x)

    edge = (z == 0) | (z == last)

    def send_cross():
        all_of(mate_in, pair_sem.at[0], pair_sem.at[1]).wait_recv()
        x_out[...] = (keep[1 - x] + mate_in[1 - x].astype(jnp.float32)).astype(jnp.bfloat16)
        cross_copy().start()

    def visit(k, carry):
        block = pick(k)
        downward = jnp.where(block < z, 1, 0)

        @pl.when((k > 0) & edge)
        def _():
            for e in range(half):
                distance, part = arrival(PIECES * (lines - 2) + (k - 1) * half + e, last)
                source = jnp.clip(jnp.where(z == 0, distance, last - distance), 0, last)
                tok_copy(source, part, up_send, above).wait_recv()

        activate(block, jnp.where(k == 0, ROW, 0), ROW)
        onto = jnp.clip(jnp.where(downward == 1, z - 1, z + 1), 0, last)
        device = at(onto, y, x, c)
        inner = jnp.where(downward == 1, z < last, z > 0)

        def one(j, carry):
            @pl.when(k == 0)
            def _():
                d_mate(j, 0).wait_recv()
                d_mate(j, 1).wait_recv()

            cols = pl.ds(pl.multiple_of(j * chunk, chunk), chunk)
            own = partial(cols)

            @pl.when(inner)
            def _():
                line_copy(downward, block, j, device, z).wait_recv()

            onward[block, :, cols] = (
                own + from_line[downward, block, :, cols].astype(jnp.float32)
            ).astype(jnp.bfloat16)
            line_copy(downward, block, j, device, onto).start()

            @pl.when((k == 0) & edge & (j + AHEAD < CHUNKS))
            def _():
                pass_down(jnp.minimum(j + AHEAD, CHUNKS - 1))

            @pl.when((k == 0) & (j + 1 < CHUNKS))
            def _():
                take_plane(jnp.minimum(j + 1, CHUNKS - 1))

            @pl.when((k == 0) & (j == CHUNKS - AHEAD - 1) & edge)
            def _():
                send_cross()

            return carry

        lax.fori_loop(0, CHUNKS, one, 0)
        return carry

    def take_plane(j):
        d_plane(j).wait_recv()
        d_mate(j, 1).start()

    activate(pick(0), 0, 1)
    pass_down(0)
    lax.fori_loop(SLABS - LAG, SLABS, late, 0)
    for p in range(1, AHEAD - 1):
        pass_down(p)
    for second in range(2):
        all_of(gu_whole, gm_recv.at[second], gm_recv.at[second]).wait_recv()
    activate(pick(0), 1, ROW)
    take_plane(0)
    pass_down(AHEAD - 1)

    @pl.when(jnp.logical_not(edge))
    def _():
        for p in range(AHEAD, CHUNKS):
            pass_down(p)
        send_cross()

    lax.fori_loop(0, last, visit, 0)
    activate(z, 0, ROW)

    def finish(j, carry):
        cols = pl.ds(pl.multiple_of(j * chunk, chunk), chunk)
        own = partial(cols)

        @pl.when(z > 0)
        def _():
            line_copy(0, z, j, above, z).wait_recv()

        @pl.when(z < last)
        def _():
            line_copy(1, z, j, above, z).wait_recv()

        routed_ref[:, cols] = (
            own + from_line[0, z, :, cols].astype(jnp.float32)
            + from_line[1, z, :, cols].astype(jnp.float32)
        ).astype(jnp.bfloat16)
        return carry

    keep[x] = keep[x] + mate_in[x].astype(jnp.float32)
    lax.fori_loop(0, CHUNKS, finish, 0)
    cross_copy().wait_recv()
    attn_ref[...] = (keep[x] + x_in[...].astype(jnp.float32)).astype(jnp.bfloat16)

    @pl.when(ahead)
    def _():
        halo.wait_send()

    cross_copy().wait_send()
    all_of(mate_out, pair_sem.at[0], pair_sem.at[1]).wait_send()
    shares_done().wait_send()

    for kind, whole in enumerate((gu_whole, d_whole)):
        all_of(whole, y_send.at[kind], y_send.at[kind]).wait_send()
        all_of(whole, x_send.at[kind], x_send.at[kind]).wait_send()
        for second in range(2):
            all_of(whole, m_send.at[kind, second], m_send.at[kind, second]).wait_send()

    def drain(line, carry):
        @pl.when((line <= z) & (z < last))
        def _():
            all_of(gath.at[line], up_send.at[line], up_send.at[line]).wait_send()

        @pl.when((line >= z) & (z > 0))
        def _():
            all_of(gath.at[line], down_send.at[line], down_send.at[line]).wait_send()

        @pl.when(line != z)
        def _():
            all_of(onward.at[line], line_send.at[line], line_send.at[line]).wait_send()

        return carry

    lax.fori_loop(0, lines, drain, 0)


def fused_layer(*operands):
    moe_input, _, routes, _, gate_weight, _, _, queries, keys, _, sinks, out_weight = operands
    targets = lax.axis_size("ep")
    lines = targets // ROW
    tok_rows, width = moe_input.shape
    hidden = gate_weight.shape[1]
    attn_rows = queries.shape[0]
    quarter = (attn_rows // TP, out_weight.shape[1])
    block = (tok_rows, width)
    sem = pltpu.SemaphoreType.DMA
    pieces = SLABS + CHUNKS
    bf16, f32 = jnp.bfloat16, jnp.float32
    flops = 12 * lines * tok_rows * width * hidden
    return pl.pallas_call(
        functools.partial(fused_kernel, lines, width),
        out_shape=(pltpu.VMEM(block, bf16), pltpu.VMEM(quarter, bf16)),
        in_specs=[pl.BlockSpec(memory_space=pl.ANY)] * len(operands),
        out_specs=(pl.BlockSpec(memory_space=pltpu.VMEM), pl.BlockSpec(memory_space=pltpu.VMEM)),
        scratch_shapes=[
            pltpu.VMEM(block, bf16),
            pltpu.VMEM((1, width), f32),
            pltpu.VMEM(routes.shape, jnp.int32),
            pltpu.VMEM(routes.shape, f32),
            pltpu.VMEM((lines,) + block, bf16),
            pltpu.VMEM((lines, targets, tok_rows), f32),
            pltpu.VMEM((ROW, width, 2 * hidden), bf16),
            pltpu.VMEM((ROW * hidden, width), bf16),
            pltpu.VMEM((ROW, tok_rows, hidden), bf16),
            pltpu.VMEM((lines,) + block, bf16),
            pltpu.VMEM((2, lines) + block, bf16),
            pltpu.VMEM(queries.shape, bf16),
            pltpu.VMEM((2 * HEAD_DIM, WINDOW + attn_rows), bf16),
            pltpu.SMEM(sinks.shape, f32),
            pltpu.VMEM(out_weight.shape, bf16),
            pltpu.VMEM((TP // CORES,) + quarter, f32),
            pltpu.VMEM((TP // CORES,) + quarter, bf16),
            pltpu.VMEM((TP // CORES,) + quarter, bf16),
            pltpu.VMEM(quarter, bf16),
            pltpu.VMEM(quarter, bf16),
            sem((9,)),
            sem((2,)),
            sem((2,)),
            sem((2,)),
            sem((lines,)),
            sem((lines,)),
            sem((lines, PIECES)),
            sem((2,)),
            sem((pieces,)),
            sem((2,)),
            sem((pieces,)),
            sem((2, 2)),
            sem((2,)),
            sem((2, CHUNKS)),
            sem((lines,)),
            sem((lines + 1, CHUNKS)),
            sem((2,)),
            sem,
            sem,
        ],
        compiler_params=pltpu.CompilerParams(
            collective_id=0, has_side_effects=True, vmem_limit_bytes=56 * 1024 * 1024
        ),
        cost_estimate=pl.CostEstimate(
            flops=flops, bytes_accessed=16 * tok_rows * width * lines, transcendentals=0
        ),
    )(*operands)


def fused_path(
    queries, head_keys, head_values, sink_logits, out_weight,
    moe_input, norm_gain, routes, route_weight, gate_weight, up_weight, down_weight,
):
    routed, attended = fused_layer(
        moe_input, norm_gain.reshape(1, -1), routes.T, route_weight.T,
        gate_weight[0], up_weight[0], down_weight[0],
        queries, head_keys.T, head_values.T, sink_logits, out_weight,
    )
    return (attended, routed)


def fits(queries, head_keys, sink_logits, moe_input, routes):
    targets = lax.axis_size("ep")
    tok_rows = moe_input.shape[0]
    return (
        2 * routes.shape[1] * tok_rows // targets >= tok_rows
        and targets == 4 * ROW
        and lax.axis_size("tp") == TP
        and head_keys.shape[1] == HEAD_DIM
        and sink_logits.shape[0] == 4
        and (SLABS * WINDOW) % queries.shape[0] == 0
        and queries.shape[0] >= 4 * ROW * WINDOW
    )


def on_device(
    queries,
    head_keys,
    head_values,
    sink_logits,
    out_weight,
    moe_input,
    norm_gain,
    routes,
    route_weight,
    gate_weight,
    up_weight,
    down_weight,
):
    if fits(queries, head_keys, sink_logits, moe_input, routes):
        return fused_path(
            queries, head_keys, head_values, sink_logits, out_weight, moe_input, norm_gain,
            routes, route_weight, gate_weight, up_weight, down_weight,
        )
    attention_out = attend(queries, head_keys, head_values, sink_logits, out_weight)
    routed_out = experts_part(
        moe_input, norm_gain, routes, route_weight, gate_weight, up_weight, down_weight
    )
    return (attention_out, routed_out)


def solution(mesh):
    placed = (
        P("ep", "tp"),
        P("ep", "tp"),
        P("ep", "tp"),
        P("tp"),
        P("tp", None),
        P(("ep", "tp"), None),
        P(),
        P(("ep", "tp"), None),
        P(("ep", "tp"), None),
        P("ep", None, None),
        P("ep", None, None),
        P("ep", None, None),
    )
    return jax.shard_map(
        on_device,
        mesh=mesh,
        in_specs=placed,
        out_specs=(P(("ep", "tp"), None), P(("ep", "tp"), None)),
        check_vma=False,
    )
```

```python
import functools

import jax
import jax.numpy as jnp
from jax import lax
from jax.experimental import pallas as pl
from jax.experimental.pallas import tpu as pltpu
from jax.sharding import PartitionSpec as P

HEAD_DIM = 64
WINDOW = 128
SEQS = 1


EPSILON = 1e-05
NEGATIVE = -1e30


def passed_along(value, axis, steps):
    count = lax.axis_size(axis)
    first, last = (max(0, -steps), min(count, count - steps))
    return lax.ppermute(value, axis, [(source, source + steps) for source in range(first, last)])


def clamped_unit(gate_pre, up_pre):
    gate_cut = jnp.minimum(gate_pre, 7.0)
    up_cut = jnp.clip(up_pre, -7.0, 7.0)
    return gate_cut * jax.nn.sigmoid(1.702 * gate_cut) * (up_cut + 1.0)


def attend(queries, head_keys, head_values, sink_logits, out_weight):
    tok_rows = queries.shape[0]
    local_heads = sink_logits.shape[0]
    local_kv = head_keys.shape[1] // HEAD_DIM
    per_group = local_heads // local_kv
    block_count = tok_rows // WINDOW
    key_width = local_kv * HEAD_DIM
    kv_rows = jnp.concatenate([head_keys, head_values], axis=1)
    earlier = passed_along(kv_rows[tok_rows - WINDOW :], "ep", 1)
    extended = jnp.concatenate([earlier, kv_rows], axis=0)
    banded = jnp.concatenate(
        [
            extended[:tok_rows].reshape(block_count, WINDOW, 2 * key_width),
            kv_rows.reshape(block_count, WINDOW, 2 * key_width),
        ],
        axis=1,
    )
    band_keys = banded[:, :, :key_width].reshape(block_count, 2 * WINDOW, local_kv, HEAD_DIM)
    band_values = banded[:, :, key_width:].reshape(block_count, 2 * WINDOW, local_kv, HEAD_DIM)
    blocked = queries.reshape(block_count, WINDOW, local_kv, per_group, HEAD_DIM)
    scores = jnp.einsum(
        "nqkgd,nskd->nkgqs", blocked, band_keys, preferred_element_type=jnp.float32
    ) * HEAD_DIM ** (-0.5)
    offset = lax.axis_index("ep") * tok_rows
    seq_len = tok_rows * lax.axis_size("ep") // SEQS
    query_pos = offset + jnp.arange(tok_rows, dtype=jnp.int32).reshape(block_count, WINDOW)
    key_pos = (
        offset
        - WINDOW
        + (jnp.arange(block_count, dtype=jnp.int32) * WINDOW)[:, None]
        + jnp.arange(2 * WINDOW, dtype=jnp.int32)[None, :]
    )
    distance = query_pos[:, :, None] - key_pos[:, None, :]
    starts = query_pos // seq_len * seq_len
    valid = (distance >= 0) & (distance < WINDOW) & (key_pos[:, None, :] >= starts[:, :, None])
    scores = jnp.where(valid[:, None, None], scores, NEGATIVE)
    sinks = sink_logits.reshape(local_kv, per_group, 1, 1)
    maxima = jnp.maximum(jnp.max(scores, axis=-1, keepdims=True), sinks)
    powers = jnp.exp(scores - maxima)
    weights = (powers / (jnp.sum(powers, axis=-1, keepdims=True) + jnp.exp(sinks - maxima))).astype(
        jnp.bfloat16
    )
    heads_out = jnp.einsum(
        "nkgqs,nskd->nqkgd", weights, band_values, preferred_element_type=jnp.float32
    )
    heads_out = heads_out.astype(jnp.bfloat16).reshape(tok_rows, local_heads * HEAD_DIM)
    summed = lax.psum_scatter(
        jnp.dot(heads_out, out_weight, preferred_element_type=jnp.float32),
        "tp",
        scatter_dimension=0,
        tiled=True,
    )
    return summed.astype(jnp.bfloat16)


def experts_part(moe_input, norm_gain, routes, route_weight, gate_weight, up_weight, down_weight):
    tok_rows, model_width = moe_input.shape
    choice_count = routes.shape[1]
    targets = lax.axis_size("ep")
    capacity = 2 * choice_count * tok_rows // targets
    values32 = moe_input.astype(jnp.float32)
    scale = lax.rsqrt(jnp.mean(values32 * values32, axis=-1, keepdims=True) + EPSILON)
    normed = (values32 * scale * norm_gain).astype(jnp.bfloat16)
    if capacity >= tok_rows:
        experts = jnp.arange(targets, dtype=jnp.int32)
        named = routes[:, :, None] == experts[None, None, :]
        shares = jnp.sum(jnp.where(named, route_weight[:, :, None], 0.0), axis=1)
        everyone = lax.all_gather(normed, "ep", axis=0, tiled=True)
        mine = lax.all_to_all(shares.T[:, None], "ep", split_axis=0, concat_axis=0, tiled=True)
        gate_pre = jnp.dot(everyone, gate_weight[0], preferred_element_type=jnp.float32)
        up_pre = jnp.dot(everyone, up_weight[0], preferred_element_type=jnp.float32)
        act = clamped_unit(gate_pre, up_pre).astype(jnp.bfloat16)
        result = jnp.dot(act, down_weight[0], preferred_element_type=jnp.float32)
        part = result.astype(jnp.bfloat16).astype(jnp.float32) * mine.reshape(-1, 1)
        return lax.psum_scatter(
            part.astype(jnp.bfloat16), "ep", scatter_dimension=0, tiled=True
        )
    flat_routes = routes.reshape(-1)
    onehot = (flat_routes[:, None] == jnp.arange(targets, dtype=jnp.int32)[None, :]).astype(
        jnp.int32
    )
    earlier_count = jnp.sum((jnp.cumsum(onehot, axis=0) - onehot) * onehot, axis=1)
    slot_index = flat_routes * capacity + earlier_count
    copies = jnp.repeat(normed, choice_count, axis=0)
    outgoing = jnp.zeros((targets * capacity, model_width), jnp.bfloat16).at[slot_index].set(copies)
    outgoing = outgoing.reshape(targets, capacity, model_width)
    arrived = lax.all_to_all(outgoing, "ep", split_axis=0, concat_axis=0, tiled=True)
    flat_rows = arrived.reshape(-1, model_width)
    gate_pre = jnp.dot(flat_rows, gate_weight[0], preferred_element_type=jnp.float32)
    up_pre = jnp.dot(flat_rows, up_weight[0], preferred_element_type=jnp.float32)
    act = clamped_unit(gate_pre, up_pre).astype(jnp.bfloat16)
    result = jnp.dot(act, down_weight[0], preferred_element_type=jnp.float32).astype(jnp.bfloat16)
    came_back = lax.all_to_all(
        result.reshape(arrived.shape), "ep", split_axis=0, concat_axis=0, tiled=True
    )
    picked = came_back.reshape(targets * capacity, model_width)[slot_index]
    weighted = (
        picked.astype(jnp.float32).reshape(tok_rows, choice_count, model_width)
        * route_weight[:, :, None]
    )
    return jnp.sum(weighted, axis=1).astype(jnp.bfloat16)


ROW = 2
CORES = 2
TP = 4
PIECES = 4
CHUNKS = 8
SLABS = 16
LAG = 3
AHEAD = 4
NORM_ROWS = 16


def fused_kernel(
    lines, width,
    rows_hbm, gain_hbm, routes_hbm, route_weight_hbm, gate_hbm, up_hbm, down_hbm,
    q_hbm, keys_hbm, values_hbm, sinks_hbm, proj_hbm,
    routed_ref, attn_ref,
    raw, gain, routes, route_weight,
    gath, shares, wgu, wd, act, onward, from_line,
    qs, ext, sinks, wo, keep, mate_out, mate_in, x_out, x_in,
    local_sem, gu_sem, share_sem, halo_sem,
    up_send, down_send, tok_recv,
    y_send, y_recv, x_send, x_recv, m_send, gm_recv, m_recv,
    line_send, line_recv, pair_sem, cross_send, cross_recv,
):
    ep, tp = lax.axis_index("ep"), lax.axis_index("tp")
    z, y, x, c = ep // ROW, ep % ROW, tp // CORES, tp % CORES
    tok_rows, model_width = routed_ref.shape
    hidden = gate_hbm.shape[1]
    attn_rows = q_hbm.shape[0]
    piece = tok_rows // PIECES
    chunk = model_width // CHUNKS
    last = lines - 1
    quarter = wgu.shape[1] // TP
    slab = quarter // SLABS

    def at(zz, yy, xx, cc):
        return {"ep": zz * ROW + yy, "tp": xx * CORES + cc}

    def remote(source, target, send, recv, device):
        return pltpu.make_async_remote_copy(
            src_ref=source, dst_ref=target, send_sem=send, recv_sem=recv,
            device_id=device, device_id_type=pl.DeviceIdType.MESH,
        )

    above = at(jnp.minimum(z + 1, last), y, x, c)
    below = at(jnp.maximum(z - 1, 0), y, x, c)
    over_y, over_x, mate = at(z, 1 - y, x, c), at(z, y, 1 - x, c), at(z, y, x, 1 - c)

    def gu_load(q, half):
        place = pl.ds(q * quarter, quarter)
        source = (gate_hbm, up_hbm)[half]
        return pltpu.make_async_copy(
            source.at[place], wgu.at[0, place, pl.ds(half * hidden, hidden)],
            gu_sem.at[jnp.where(q == tp, 0, 1)],
        )

    def loaded(target, semaphore):
        pltpu.make_async_copy(target, target, semaphore).wait()

    own = pl.ds(WINDOW, attn_rows)
    loads = [
        pltpu.make_async_copy(source, target, local_sem.at[max(i - 1, 0)])
        for i, (source, target) in enumerate([
            (keys_hbm, ext.at[pl.ds(0, HEAD_DIM), own]),
            (values_hbm, ext.at[pl.ds(HEAD_DIM, HEAD_DIM), own]),
            (rows_hbm, raw),
            (gain_hbm, gain),
            (routes_hbm, routes),
            (route_weight_hbm, route_weight),
            (down_hbm, wd.at[pl.ds(0, hidden)]),
            (q_hbm, qs),
            (sinks_hbm, sinks),
            (proj_hbm, wo),
        ])
    ]
    gu_load(tp, 0).start()
    gu_load(tp, 1).start()
    for load in loads:
        load.start()
    for step in range(1, TP):
        gu_load(lax.rem(tp + step, TP), 0).start()
        gu_load(lax.rem(tp + step, TP), 1).start()

    ahead = ep + 1 < lines * ROW
    behind = ep > 0
    skew = jnp.where(y == 1, z < last, z > 0)
    skew_ep = jnp.where(y == 1, jnp.minimum(ep + 1, lines * ROW - 1), jnp.maximum(ep - 1, 0))
    barrier = pltpu.get_barrier_semaphore()

    def greet(device):
        pl.semaphore_signal(barrier, inc=1, device_id=device, device_id_type=pl.DeviceIdType.MESH)

    for step in range(1, lines):
        greet(at(lax.rem(z + step, lines), y, x, c))
    greet(over_y)
    greet(over_x)
    greet(mate)

    @pl.when(skew)
    def _():
        greet({"ep": skew_ep, "tp": tp})

    pl.semaphore_wait(barrier, last + 3 + jnp.where(skew, 1, 0))

    halo = remote(
        ext.at[:, pl.ds(attn_rows, WINDOW)], ext.at[:, pl.ds(0, WINDOW)], halo_sem.at[0],
        halo_sem.at[1], {"ep": jnp.minimum(ep + 1, lines * ROW - 1), "tp": tp},
    )

    def share_copy(slot, device):
        return remote(
            shares.at[slot], shares.at[slot], share_sem.at[0], share_sem.at[1], device
        )

    def all_of(view, send, recv):
        return remote(view, view, send, recv, mate)

    def shares_done():
        return all_of(shares.at[pl.ds(0, last)], share_sem.at[0], share_sem.at[1])

    def tok_copy(block, part, sems, device):
        view = gath.at[block, pl.ds(part * piece, piece)]
        return remote(view, view, sems.at[block], tok_recv.at[block, part], device)

    def gu_view(expert, q, p):
        return wgu.at[expert, pl.ds(q * quarter + p * slab, slab)]

    def d_view(expert, q, p):
        return wd.at[
            pl.ds(expert * hidden + q * (hidden // TP), hidden // TP), pl.ds(p * chunk, chunk)
        ]

    def weight_copies(view, kind, base, mate_recv):
        def over_link(p):
            return remote(
                view(0, tp, p), view(1, tp, p), y_send.at[kind], y_recv.at[base + p], over_y
            )

        def to_plane(p):
            return remote(
                view(1, tp, p), view(1, tp, p), x_send.at[kind], x_recv.at[base + p], over_x
            )

        def to_mate(p, second):
            q = (1 - x) * CORES + c if second else tp
            return remote(
                view(1, q, p), view(1, q, p), m_send.at[kind, second], mate_recv(second, p), mate
            )

        return over_link, to_plane, to_mate

    gu_over, gu_plane, gu_mate = weight_copies(gu_view, 0, 0, lambda second, p: gm_recv.at[second])
    d_over, d_plane, d_mate = weight_copies(
        d_view, 1, SLABS, lambda second, p: m_recv.at[second, p]
    )
    gu_whole = wgu.at[1, pl.ds(0, quarter)]
    d_whole = wd.at[pl.ds(0, hidden // TP)]

    loaded(ext.at[:, own], local_sem.at[0])

    @pl.when(ahead)
    def _():
        halo.start()

    loaded(wgu.at[0, pl.ds(0, quarter)], gu_sem.at[0])

    def launch_gu(p, carry):
        gu_over(p).start()
        return carry

    lax.fori_loop(0, SLABS, launch_gu, 0)
    for load in loads[2:6]:
        load.wait()

    def normalize(i, carry):
        place = pl.ds(i * NORM_ROWS, NORM_ROWS)
        values32 = raw[place].astype(jnp.float32)
        mean = jnp.sum(values32 * values32, axis=-1, keepdims=True) * (1.0 / model_width)
        scale = lax.rsqrt(mean + EPSILON)
        gath[z, place] = (values32 * scale * gain[...]).astype(jnp.bfloat16)
        return carry

    lax.fori_loop(0, tok_rows // NORM_ROWS, normalize, 0)
    expert = lax.broadcasted_iota(jnp.int32, shares.shape[1:], 0)
    share = jnp.zeros(shares.shape[1:], jnp.float32)
    for choice in range(routes.shape[0]):
        named = routes[choice : choice + 1, :] == expert
        share = share + jnp.where(named, route_weight[choice : choice + 1, :], 0.0)
    shares[z] = share

    def own_tokens(first, count, upward):
        for part in range(first, first + count):
            if upward:
                tok_copy(z, part, up_send, above).start()
            else:
                tok_copy(z, part, down_send, below).start()

    half = PIECES // 2

    @pl.when(z < last)
    def _():
        own_tokens(0, half, True)

    @pl.when(z == 0)
    def _():
        own_tokens(half, half, True)

    @pl.when(z > 0)
    def _():
        own_tokens(0, half, False)

    @pl.when(z == last)
    def _():
        own_tokens(half, half, False)

    for step in range(1, lines):
        other = lax.rem(z + step, lines)
        share_copy(z, at(other, y, x, c)).start()
    loads[6].wait()

    def launch_d(p, carry):
        d_over(p).start()
        return carry

    lax.fori_loop(0, CHUNKS, launch_d, 0)
    for load in loads[7:]:
        load.wait()

    def arrival(i, reach):
        s = i // half
        far = s < reach
        distance = jnp.where(far, s + 1, 2 * reach - s)
        part = jnp.where(far, 0, half) + i % half
        return distance, part

    def pump_tokens(i):
        for upward in (True, False):
            reach = z if upward else last - z
            distance, part = arrival(i, reach)
            block = jnp.clip(z - distance if upward else z + distance, 0, last)

            @pl.when(i < PIECES * reach)
            def _():
                tok_copy(block, part, up_send, above).wait_recv()

            @pl.when((i < PIECES * reach) & (reach < last))
            def _():
                if upward:
                    tok_copy(block, part, up_send, above).start()
                else:
                    tok_copy(block, part, down_send, below).start()

            @pl.when((i == PIECES * reach - 1) & (reach < last))
            def _():
                own_tokens(half, half, upward)

    per_group = sinks.shape[0]
    band = 2 * WINDOW
    quarter_rows = attn_ref.shape[0]
    blocks_each = quarter_rows // WINDOW

    def pair_copy(owner_x):
        return remote(
            mate_out.at[owner_x], mate_in.at[owner_x], pair_sem.at[0], pair_sem.at[1], mate
        )

    def attend_block(n):
        q_rows = qs[pl.ds(n * WINDOW, WINDOW)] * jnp.bfloat16(HEAD_DIM ** (-0.5))
        held = ext[:, pl.ds(pl.multiple_of(n * WINDOW, WINDOW), band)]
        keys = jnp.concatenate([held[:HEAD_DIM]] * per_group, axis=0)
        values = held[HEAD_DIM:]
        q_head = lax.broadcasted_iota(jnp.int32, q_rows.shape, 1) // HEAD_DIM
        stacked = jnp.concatenate(
            [jnp.where(q_head == h, q_rows, jnp.zeros_like(q_rows)) for h in range(per_group)],
            axis=0,
        )
        scores = jnp.dot(stacked, keys, preferred_element_type=jnp.float32)
        begins = lax.rem(ep * (qs.shape[0] // WINDOW) + n, lines * ROW * (qs.shape[0] // WINDOW) // SEQS) == 0
        row = lax.broadcasted_iota(jnp.int32, (WINDOW, band), 0)
        col = lax.broadcasted_iota(jnp.int32, (WINDOW, band), 1)
        valid = (col > row) & (col <= row + WINDOW) & (col >= jnp.where(begins, WINDOW, 0))
        weights = []
        for h in range(per_group):
            score = jnp.where(valid, scores[h * WINDOW : (h + 1) * WINDOW], NEGATIVE)
            sink = sinks[h]
            top = jnp.maximum(jnp.max(score, axis=1, keepdims=True), sink)
            powers = jnp.exp(score - top)
            total = jnp.sum(powers, axis=1, keepdims=True) + jnp.exp(sink - top)
            weights.append((powers * (1.0 / total)).astype(jnp.bfloat16))
        blank = jnp.zeros_like(values)
        spread = jnp.concatenate(
            [
                jnp.concatenate([values if g == h else blank for g in range(per_group)], axis=1)
                for h in range(per_group)
            ],
            axis=0,
        )
        heads = lax.dot_general(
            jnp.concatenate(weights, axis=1), spread, (((1,), (1,)), ((), ())),
            preferred_element_type=jnp.float32,
        ).astype(jnp.bfloat16)
        owner = n // blocks_each
        owner_x, owner_c = owner // CORES, owner % CORES
        place = pl.ds((n % blocks_each) * WINDOW, WINDOW)
        share = jnp.dot(heads, wo[...], preferred_element_type=jnp.float32)

        @pl.when(owner_c == c)
        def _():
            keep[owner_x, place] = share

        @pl.when(owner_c != c)
        def _():
            mate_out[owner_x, place] = share.astype(jnp.bfloat16)

    each = SLABS * WINDOW // attn_rows

    def slot(i, carry):
        gu_over(i).wait_recv()
        gu_plane(i).start()
        gu_mate(i, 0).start()

        @pl.when(i >= LAG)
        def _():
            gu_plane(i - LAG).wait_recv()
            gu_mate(i - LAG, 1).start()

        @pl.when(i % each == 0)
        def _():
            n = lax.rem(i // each + 1, attn_rows // WINDOW)

            @pl.when((n == 0) & behind)
            def _():
                halo.wait_recv()

            @pl.when((n == 0) & (ep == 0))
            def _():
                ext[:, pl.ds(0, WINDOW)] = jnp.zeros((ext.shape[0], WINDOW), ext.dtype)

            attend_block(n)

        @pl.when(i % each == each - 1)
        def _():
            pump_tokens(i // each)

        @pl.when((i % each == each - 1) & (i // each < lines))
        def _():
            block = jnp.minimum(i // each, last)

            @pl.when(z == 0)
            def _():
                from_line[0, block] = jnp.zeros(from_line.shape[2:], from_line.dtype)

            @pl.when(z == last)
            def _():
                from_line[1, block] = jnp.zeros(from_line.shape[2:], from_line.dtype)

        return carry

    lax.fori_loop(0, SLABS, slot, 0)
    for owner_x in range(TP // CORES):
        pair_copy(owner_x).start()

    def pass_down(j):
        d_over(j).wait_recv()
        d_plane(j).start()
        d_mate(j, 0).start()

    def late(p, carry):
        gu_plane(p).wait_recv()
        gu_mate(p, 1).start()
        return carry

    shares_done().wait_recv()
    loaded(wgu.at[0, pl.ds(quarter, (TP - 1) * quarter)], gu_sem.at[1])

    square = (tok_rows, tok_rows)
    eye = lax.broadcasted_iota(jnp.int32, square, 0) == lax.broadcasted_iota(jnp.int32, square, 1)

    def activate(block, first, end):
        def one(expert, carry):
            pre = jnp.dot(gath[block], wgu[expert], preferred_element_type=jnp.float32)
            unit = clamped_unit(pre[:, :hidden], pre[:, hidden:])
            named = z * ROW + jnp.where(expert == 1, 1 - y, y)
            column = jnp.sum(
                jnp.where(eye, shares[block, pl.ds(named, 1), :], 0.0), axis=1, keepdims=True
            )
            act[expert] = (unit * column).astype(jnp.bfloat16)
            return carry

        lax.fori_loop(first, end, one, 0)

    def partial(cols):
        both = jnp.concatenate([act[0], act[1]], axis=1)
        return jnp.dot(both, wd[:, cols], preferred_element_type=jnp.float32)

    def line_copy(downward, block, j, device, holder):
        cols = pl.ds(j * chunk, chunk)
        row = jnp.where(downward == 1, lines - holder + block, block - holder)
        return remote(
            onward.at[block, :, cols], from_line.at[downward, block, :, cols],
            line_send.at[block], line_recv.at[row, j], device,
        )

    def pick(k):
        block = 0
        for zz in range(lines):
            others = sorted(
                (b for b in range(lines) if b != zz),
                key=lambda b: (-abs(b - zz), min(b, last - b)),
            )
            for kk, b in enumerate(others):
                block = jnp.where((z == zz) & (k == kk), b, block)
        return block

    def cross_copy():
        return remote(x_out, x_in, cross_send, cross_recv, over_x)

    edge = (z == 0) | (z == last)

    def send_cross():
        all_of(mate_in, pair_sem.at[0], pair_sem.at[1]).wait_recv()
        x_out[...] = (keep[1 - x] + mate_in[1 - x].astype(jnp.float32)).astype(jnp.bfloat16)
        cross_copy().start()

    def visit(k, carry):
        block = pick(k)
        downward = jnp.where(block < z, 1, 0)

        @pl.when((k > 0) & edge)
        def _():
            for e in range(half):
                distance, part = arrival(PIECES * (lines - 2) + (k - 1) * half + e, last)
                source = jnp.clip(jnp.where(z == 0, distance, last - distance), 0, last)
                tok_copy(source, part, up_send, above).wait_recv()

        activate(block, jnp.where(k == 0, ROW, 0), ROW)
        onto = jnp.clip(jnp.where(downward == 1, z - 1, z + 1), 0, last)
        device = at(onto, y, x, c)
        inner = jnp.where(downward == 1, z < last, z > 0)

        def one(j, carry):
            @pl.when(k == 0)
            def _():
                d_mate(j, 0).wait_recv()
                d_mate(j, 1).wait_recv()

            cols = pl.ds(pl.multiple_of(j * chunk, chunk), chunk)
            own = partial(cols)

            @pl.when(inner)
            def _():
                line_copy(downward, block, j, device, z).wait_recv()

            onward[block, :, cols] = (
                own + from_line[downward, block, :, cols].astype(jnp.float32)
            ).astype(jnp.bfloat16)
            line_copy(downward, block, j, device, onto).start()

            @pl.when((k == 0) & edge & (j + AHEAD < CHUNKS))
            def _():
                pass_down(jnp.minimum(j + AHEAD, CHUNKS - 1))

            @pl.when((k == 0) & (j + 1 < CHUNKS))
            def _():
                take_plane(jnp.minimum(j + 1, CHUNKS - 1))

            @pl.when((k == 0) & (j == CHUNKS - AHEAD - 1) & edge)
            def _():
                send_cross()

            return carry

        lax.fori_loop(0, CHUNKS, one, 0)
        return carry

    def take_plane(j):
        d_plane(j).wait_recv()
        d_mate(j, 1).start()

    activate(pick(0), 0, 1)
    pass_down(0)
    lax.fori_loop(SLABS - LAG, SLABS, late, 0)
    for p in range(1, AHEAD - 1):
        pass_down(p)
    for second in range(2):
        all_of(gu_whole, gm_recv.at[second], gm_recv.at[second]).wait_recv()
    activate(pick(0), 1, ROW)
    take_plane(0)
    pass_down(AHEAD - 1)

    @pl.when(jnp.logical_not(edge))
    def _():
        for p in range(AHEAD, CHUNKS):
            pass_down(p)
        send_cross()

    lax.fori_loop(0, last, visit, 0)
    activate(z, 0, ROW)

    def finish(j, carry):
        cols = pl.ds(pl.multiple_of(j * chunk, chunk), chunk)
        own = partial(cols)

        @pl.when(z > 0)
        def _():
            line_copy(0, z, j, above, z).wait_recv()

        @pl.when(z < last)
        def _():
            line_copy(1, z, j, above, z).wait_recv()

        routed_ref[:, cols] = (
            own + from_line[0, z, :, cols].astype(jnp.float32)
            + from_line[1, z, :, cols].astype(jnp.float32)
        ).astype(jnp.bfloat16)
        return carry

    keep[x] = keep[x] + mate_in[x].astype(jnp.float32)
    lax.fori_loop(0, CHUNKS - 1, finish, 0)
    cross_copy().wait_recv()
    attn_ref[...] = (keep[x] + x_in[...].astype(jnp.float32)).astype(jnp.bfloat16)
    finish(CHUNKS - 1, 0)

    @pl.when(ahead)
    def _():
        halo.wait_send()

    cross_copy().wait_send()
    all_of(mate_out, pair_sem.at[0], pair_sem.at[1]).wait_send()
    shares_done().wait_send()

    for kind, whole in enumerate((gu_whole, d_whole)):
        all_of(whole, y_send.at[kind], y_send.at[kind]).wait_send()
        all_of(whole, x_send.at[kind], x_send.at[kind]).wait_send()
        for second in range(2):
            all_of(whole, m_send.at[kind, second], m_send.at[kind, second]).wait_send()

    def drain(line, carry):
        @pl.when((line <= z) & (z < last))
        def _():
            all_of(gath.at[line], up_send.at[line], up_send.at[line]).wait_send()

        @pl.when((line >= z) & (z > 0))
        def _():
            all_of(gath.at[line], down_send.at[line], down_send.at[line]).wait_send()

        @pl.when(line != z)
        def _():
            all_of(onward.at[line], line_send.at[line], line_send.at[line]).wait_send()

        return carry

    lax.fori_loop(0, lines, drain, 0)


def fused_layer(*operands):
    moe_input, _, routes, _, gate_weight, _, _, queries, keys, _, sinks, out_weight = operands
    targets = lax.axis_size("ep")
    lines = targets // ROW
    tok_rows, width = moe_input.shape
    hidden = gate_weight.shape[1]
    attn_rows = queries.shape[0]
    quarter = (attn_rows // TP, out_weight.shape[1])
    block = (tok_rows, width)
    sem = pltpu.SemaphoreType.DMA
    pieces = SLABS + CHUNKS
    bf16, f32 = jnp.bfloat16, jnp.float32
    flops = 12 * lines * tok_rows * width * hidden
    return pl.pallas_call(
        functools.partial(fused_kernel, lines, width),
        out_shape=(pltpu.VMEM(block, bf16), pltpu.VMEM(quarter, bf16)),
        in_specs=[pl.BlockSpec(memory_space=pl.ANY)] * len(operands),
        out_specs=(pl.BlockSpec(memory_space=pltpu.VMEM), pl.BlockSpec(memory_space=pltpu.VMEM)),
        scratch_shapes=[
            pltpu.VMEM(block, bf16),
            pltpu.VMEM((1, width), f32),
            pltpu.VMEM(routes.shape, jnp.int32),
            pltpu.VMEM(routes.shape, f32),
            pltpu.VMEM((lines,) + block, bf16),
            pltpu.VMEM((lines, targets, tok_rows), f32),
            pltpu.VMEM((ROW, width, 2 * hidden), bf16),
            pltpu.VMEM((ROW * hidden, width), bf16),
            pltpu.VMEM((ROW, tok_rows, hidden), bf16),
            pltpu.VMEM((lines,) + block, bf16),
            pltpu.VMEM((2, lines) + block, bf16),
            pltpu.VMEM(queries.shape, bf16),
            pltpu.VMEM((2 * HEAD_DIM, WINDOW + attn_rows), bf16),
            pltpu.SMEM(sinks.shape, f32),
            pltpu.VMEM(out_weight.shape, bf16),
            pltpu.VMEM((TP // CORES,) + quarter, f32),
            pltpu.VMEM((TP // CORES,) + quarter, bf16),
            pltpu.VMEM((TP // CORES,) + quarter, bf16),
            pltpu.VMEM(quarter, bf16),
            pltpu.VMEM(quarter, bf16),
            sem((9,)),
            sem((2,)),
            sem((2,)),
            sem((2,)),
            sem((lines,)),
            sem((lines,)),
            sem((lines, PIECES)),
            sem((2,)),
            sem((pieces,)),
            sem((2,)),
            sem((pieces,)),
            sem((2, 2)),
            sem((2,)),
            sem((2, CHUNKS)),
            sem((lines,)),
            sem((lines + 1, CHUNKS)),
            sem((2,)),
            sem,
            sem,
        ],
        compiler_params=pltpu.CompilerParams(
            collective_id=0, has_side_effects=True, vmem_limit_bytes=56 * 1024 * 1024
        ),
        cost_estimate=pl.CostEstimate(
            flops=flops, bytes_accessed=16 * tok_rows * width * lines, transcendentals=0
        ),
    )(*operands)


def fused_path(
    queries, head_keys, head_values, sink_logits, out_weight,
    moe_input, norm_gain, routes, route_weight, gate_weight, up_weight, down_weight,
):
    routed, attended = fused_layer(
        moe_input, norm_gain.reshape(1, -1), routes.T, route_weight.T,
        gate_weight[0], up_weight[0], down_weight[0],
        queries, head_keys.T, head_values.T, sink_logits, out_weight,
    )
    return (attended, routed)


def fits(queries, head_keys, sink_logits, moe_input, routes):
    targets = lax.axis_size("ep")
    tok_rows = moe_input.shape[0]
    return (
        2 * routes.shape[1] * tok_rows // targets >= tok_rows
        and targets == 4 * ROW
        and lax.axis_size("tp") == TP
        and head_keys.shape[1] == HEAD_DIM
        and sink_logits.shape[0] == 4
        and (SLABS * WINDOW) % queries.shape[0] == 0
        and queries.shape[0] >= 4 * ROW * WINDOW
    )


def on_device(
    queries,
    head_keys,
    head_values,
    sink_logits,
    out_weight,
    moe_input,
    norm_gain,
    routes,
    route_weight,
    gate_weight,
    up_weight,
    down_weight,
):
    if fits(queries, head_keys, sink_logits, moe_input, routes):
        return fused_path(
            queries, head_keys, head_values, sink_logits, out_weight, moe_input, norm_gain,
            routes, route_weight, gate_weight, up_weight, down_weight,
        )
    attention_out = attend(queries, head_keys, head_values, sink_logits, out_weight)
    routed_out = experts_part(
        moe_input, norm_gain, routes, route_weight, gate_weight, up_weight, down_weight
    )
    return (attention_out, routed_out)


def solution(mesh):
    placed = (
        P("ep", "tp"),
        P("ep", "tp"),
        P("ep", "tp"),
        P("tp"),
        P("tp", None),
        P(("ep", "tp"), None),
        P(),
        P(("ep", "tp"), None),
        P(("ep", "tp"), None),
        P("ep", None, None),
        P("ep", None, None),
        P("ep", None, None),
    )
    return jax.shard_map(
        on_device,
        mesh=mesh,
        in_specs=placed,
        out_specs=(P(("ep", "tp"), None), P(("ep", "tp"), None)),
        check_vma=False,
    )
```

```python
import functools

import jax
import jax.numpy as jnp
from jax import lax
from jax.experimental import pallas as pl
from jax.experimental.pallas import tpu as pltpu
from jax.sharding import PartitionSpec as P

HEAD_DIM = 64
WINDOW = 128
SEQS = 1


EPSILON = 1e-05
NEGATIVE = -1e30


def passed_along(value, axis, steps):
    count = lax.axis_size(axis)
    first, last = (max(0, -steps), min(count, count - steps))
    return lax.ppermute(value, axis, [(source, source + steps) for source in range(first, last)])


def clamped_unit(gate_pre, up_pre):
    gate_cut = jnp.minimum(gate_pre, 7.0)
    up_cut = jnp.clip(up_pre, -7.0, 7.0)
    return gate_cut * jax.nn.sigmoid(1.702 * gate_cut) * (up_cut + 1.0)


def attend(queries, head_keys, head_values, sink_logits, out_weight):
    tok_rows = queries.shape[0]
    local_heads = sink_logits.shape[0]
    local_kv = head_keys.shape[1] // HEAD_DIM
    per_group = local_heads // local_kv
    block_count = tok_rows // WINDOW
    key_width = local_kv * HEAD_DIM
    kv_rows = jnp.concatenate([head_keys, head_values], axis=1)
    earlier = passed_along(kv_rows[tok_rows - WINDOW :], "ep", 1)
    extended = jnp.concatenate([earlier, kv_rows], axis=0)
    banded = jnp.concatenate(
        [
            extended[:tok_rows].reshape(block_count, WINDOW, 2 * key_width),
            kv_rows.reshape(block_count, WINDOW, 2 * key_width),
        ],
        axis=1,
    )
    band_keys = banded[:, :, :key_width].reshape(block_count, 2 * WINDOW, local_kv, HEAD_DIM)
    band_values = banded[:, :, key_width:].reshape(block_count, 2 * WINDOW, local_kv, HEAD_DIM)
    blocked = queries.reshape(block_count, WINDOW, local_kv, per_group, HEAD_DIM)
    scores = jnp.einsum(
        "nqkgd,nskd->nkgqs", blocked, band_keys, preferred_element_type=jnp.float32
    ) * HEAD_DIM ** (-0.5)
    offset = lax.axis_index("ep") * tok_rows
    seq_len = tok_rows * lax.axis_size("ep") // SEQS
    query_pos = offset + jnp.arange(tok_rows, dtype=jnp.int32).reshape(block_count, WINDOW)
    key_pos = (
        offset
        - WINDOW
        + (jnp.arange(block_count, dtype=jnp.int32) * WINDOW)[:, None]
        + jnp.arange(2 * WINDOW, dtype=jnp.int32)[None, :]
    )
    distance = query_pos[:, :, None] - key_pos[:, None, :]
    starts = query_pos // seq_len * seq_len
    valid = (distance >= 0) & (distance < WINDOW) & (key_pos[:, None, :] >= starts[:, :, None])
    scores = jnp.where(valid[:, None, None], scores, NEGATIVE)
    sinks = sink_logits.reshape(local_kv, per_group, 1, 1)
    maxima = jnp.maximum(jnp.max(scores, axis=-1, keepdims=True), sinks)
    powers = jnp.exp(scores - maxima)
    weights = (powers / (jnp.sum(powers, axis=-1, keepdims=True) + jnp.exp(sinks - maxima))).astype(
        jnp.bfloat16
    )
    heads_out = jnp.einsum(
        "nkgqs,nskd->nqkgd", weights, band_values, preferred_element_type=jnp.float32
    )
    heads_out = heads_out.astype(jnp.bfloat16).reshape(tok_rows, local_heads * HEAD_DIM)
    summed = lax.psum_scatter(
        jnp.dot(heads_out, out_weight, preferred_element_type=jnp.float32),
        "tp",
        scatter_dimension=0,
        tiled=True,
    )
    return summed.astype(jnp.bfloat16)


def experts_part(moe_input, norm_gain, routes, route_weight, gate_weight, up_weight, down_weight):
    tok_rows, model_width = moe_input.shape
    choice_count = routes.shape[1]
    targets = lax.axis_size("ep")
    capacity = 2 * choice_count * tok_rows // targets
    values32 = moe_input.astype(jnp.float32)
    scale = lax.rsqrt(jnp.mean(values32 * values32, axis=-1, keepdims=True) + EPSILON)
    normed = (values32 * scale * norm_gain).astype(jnp.bfloat16)
    if capacity >= tok_rows:
        experts = jnp.arange(targets, dtype=jnp.int32)
        named = routes[:, :, None] == experts[None, None, :]
        shares = jnp.sum(jnp.where(named, route_weight[:, :, None], 0.0), axis=1)
        everyone = lax.all_gather(normed, "ep", axis=0, tiled=True)
        mine = lax.all_to_all(shares.T[:, None], "ep", split_axis=0, concat_axis=0, tiled=True)
        gate_pre = jnp.dot(everyone, gate_weight[0], preferred_element_type=jnp.float32)
        up_pre = jnp.dot(everyone, up_weight[0], preferred_element_type=jnp.float32)
        act = clamped_unit(gate_pre, up_pre).astype(jnp.bfloat16)
        result = jnp.dot(act, down_weight[0], preferred_element_type=jnp.float32)
        part = result.astype(jnp.bfloat16).astype(jnp.float32) * mine.reshape(-1, 1)
        return lax.psum_scatter(
            part.astype(jnp.bfloat16), "ep", scatter_dimension=0, tiled=True
        )
    flat_routes = routes.reshape(-1)
    onehot = (flat_routes[:, None] == jnp.arange(targets, dtype=jnp.int32)[None, :]).astype(
        jnp.int32
    )
    earlier_count = jnp.sum((jnp.cumsum(onehot, axis=0) - onehot) * onehot, axis=1)
    slot_index = flat_routes * capacity + earlier_count
    copies = jnp.repeat(normed, choice_count, axis=0)
    outgoing = jnp.zeros((targets * capacity, model_width), jnp.bfloat16).at[slot_index].set(copies)
    outgoing = outgoing.reshape(targets, capacity, model_width)
    arrived = lax.all_to_all(outgoing, "ep", split_axis=0, concat_axis=0, tiled=True)
    flat_rows = arrived.reshape(-1, model_width)
    gate_pre = jnp.dot(flat_rows, gate_weight[0], preferred_element_type=jnp.float32)
    up_pre = jnp.dot(flat_rows, up_weight[0], preferred_element_type=jnp.float32)
    act = clamped_unit(gate_pre, up_pre).astype(jnp.bfloat16)
    result = jnp.dot(act, down_weight[0], preferred_element_type=jnp.float32).astype(jnp.bfloat16)
    came_back = lax.all_to_all(
        result.reshape(arrived.shape), "ep", split_axis=0, concat_axis=0, tiled=True
    )
    picked = came_back.reshape(targets * capacity, model_width)[slot_index]
    weighted = (
        picked.astype(jnp.float32).reshape(tok_rows, choice_count, model_width)
        * route_weight[:, :, None]
    )
    return jnp.sum(weighted, axis=1).astype(jnp.bfloat16)


ROW = 2
CORES = 2
TP = 4
PIECES = 4
CHUNKS = 8
SLABS = 16
LAG = 3
AHEAD = 4
NORM_ROWS = 16


def fused_kernel(
    lines, width,
    rows_hbm, gain_hbm, routes_hbm, route_weight_hbm, gate_hbm, up_hbm, down_hbm,
    q_hbm, keys_hbm, values_hbm, sinks_hbm, proj_hbm,
    routed_ref, attn_ref,
    raw, gain, routes, route_weight,
    gath, shares, wgu, wd, act, onward, from_line,
    qs, ext, sinks, wo, keep, mate_out, mate_in, x_out, x_in,
    local_sem, gu_sem, share_up, share_down, share_recv, halo_sem,
    up_send, down_send, tok_recv,
    y_send, y_recv, x_send, x_recv, m_send, gm_recv, m_recv,
    line_send, line_recv, pair_sem, cross_send, cross_recv,
):
    ep, tp = lax.axis_index("ep"), lax.axis_index("tp")
    z, y, x, c = ep // ROW, ep % ROW, tp // CORES, tp % CORES
    tok_rows, model_width = routed_ref.shape
    hidden = gate_hbm.shape[1]
    attn_rows = q_hbm.shape[0]
    piece = tok_rows // PIECES
    chunk = model_width // CHUNKS
    last = lines - 1
    quarter = wgu.shape[1] // TP
    slab = quarter // SLABS

    def at(zz, yy, xx, cc):
        return {"ep": zz * ROW + yy, "tp": xx * CORES + cc}

    def remote(source, target, send, recv, device):
        return pltpu.make_async_remote_copy(
            src_ref=source, dst_ref=target, send_sem=send, recv_sem=recv,
            device_id=device, device_id_type=pl.DeviceIdType.MESH,
        )

    above = at(jnp.minimum(z + 1, last), y, x, c)
    below = at(jnp.maximum(z - 1, 0), y, x, c)
    over_y, over_x, mate = at(z, 1 - y, x, c), at(z, y, 1 - x, c), at(z, y, x, 1 - c)

    def gu_load(q, half):
        place = pl.ds(q * quarter, quarter)
        source = (gate_hbm, up_hbm)[half]
        return pltpu.make_async_copy(
            source.at[place], wgu.at[0, place, pl.ds(half * hidden, hidden)],
            gu_sem.at[jnp.where(q == tp, 0, 1)],
        )

    def loaded(target, semaphore):
        pltpu.make_async_copy(target, target, semaphore).wait()

    own = pl.ds(WINDOW, attn_rows)
    loads = [
        pltpu.make_async_copy(source, target, local_sem.at[max(i - 1, 0)])
        for i, (source, target) in enumerate([
            (keys_hbm, ext.at[pl.ds(0, HEAD_DIM), own]),
            (values_hbm, ext.at[pl.ds(HEAD_DIM, HEAD_DIM), own]),
            (rows_hbm, raw),
            (gain_hbm, gain),
            (routes_hbm, routes),
            (route_weight_hbm, route_weight),
            (down_hbm, wd.at[pl.ds(0, hidden)]),
            (q_hbm, qs),
            (sinks_hbm, sinks),
            (proj_hbm, wo),
        ])
    ]
    gu_load(tp, 0).start()
    gu_load(tp, 1).start()
    for load in loads:
        load.start()
    for step in range(1, TP):
        gu_load(lax.rem(tp + step, TP), 0).start()
        gu_load(lax.rem(tp + step, TP), 1).start()

    ahead = ep + 1 < lines * ROW
    behind = ep > 0
    skew = jnp.where(y == 1, z < last, z > 0)
    skew_ep = jnp.where(y == 1, jnp.minimum(ep + 1, lines * ROW - 1), jnp.maximum(ep - 1, 0))
    barrier = pltpu.get_barrier_semaphore()

    def greet(device):
        pl.semaphore_signal(barrier, inc=1, device_id=device, device_id_type=pl.DeviceIdType.MESH)

    @pl.when(z < last)
    def _():
        greet(above)

    @pl.when(z > 0)
    def _():
        greet(below)

    greet(over_y)
    greet(over_x)
    greet(mate)

    @pl.when(skew)
    def _():
        greet({"ep": skew_ep, "tp": tp})

    beside = jnp.where(z < last, 1, 0) + jnp.where(z > 0, 1, 0)
    pl.semaphore_wait(barrier, beside + 3 + jnp.where(skew, 1, 0))

    halo = remote(
        ext.at[:, pl.ds(attn_rows, WINDOW)], ext.at[:, pl.ds(0, WINDOW)], halo_sem.at[0],
        halo_sem.at[1], {"ep": jnp.minimum(ep + 1, lines * ROW - 1), "tp": tp},
    )

    def share_copy(block, upward, device):
        sems = share_up if upward else share_down
        return remote(
            shares.at[block], shares.at[block], sems.at[block], share_recv.at[block], device
        )

    def all_of(view, send, recv):
        return remote(view, view, send, recv, mate)

    def tok_copy(block, part, sems, device):
        view = gath.at[block, pl.ds(part * piece, piece)]
        return remote(view, view, sems.at[block], tok_recv.at[block, part], device)

    def gu_view(expert, q, p):
        return wgu.at[expert, pl.ds(q * quarter + p * slab, slab)]

    def d_view(expert, q, p):
        return wd.at[
            pl.ds(expert * hidden + q * (hidden // TP), hidden // TP), pl.ds(p * chunk, chunk)
        ]

    def weight_copies(view, kind, base, mate_recv):
        def over_link(p):
            return remote(
                view(0, tp, p), view(1, tp, p), y_send.at[kind], y_recv.at[base + p], over_y
            )

        def to_plane(p):
            return remote(
                view(1, tp, p), view(1, tp, p), x_send.at[kind], x_recv.at[base + p], over_x
            )

        def to_mate(p, second):
            q = (1 - x) * CORES + c if second else tp
            return remote(
                view(1, q, p), view(1, q, p), m_send.at[kind, second], mate_recv(second, p), mate
            )

        return over_link, to_plane, to_mate

    gu_over, gu_plane, gu_mate = weight_copies(gu_view, 0, 0, lambda second, p: gm_recv.at[second])
    d_over, d_plane, d_mate = weight_copies(
        d_view, 1, SLABS, lambda second, p: m_recv.at[second, p]
    )
    gu_whole = wgu.at[1, pl.ds(0, quarter)]
    d_whole = wd.at[pl.ds(0, hidden // TP)]

    loaded(ext.at[:, own], local_sem.at[0])

    @pl.when(ahead)
    def _():
        halo.start()

    loaded(wgu.at[0, pl.ds(0, quarter)], gu_sem.at[0])

    def launch_gu(p, carry):
        gu_over(p).start()
        return carry

    lax.fori_loop(0, SLABS, launch_gu, 0)
    for load in loads[2:6]:
        load.wait()

    def normalize(i, carry):
        place = pl.ds(i * NORM_ROWS, NORM_ROWS)
        values32 = raw[place].astype(jnp.float32)
        mean = jnp.sum(values32 * values32, axis=-1, keepdims=True) * (1.0 / model_width)
        scale = lax.rsqrt(mean + EPSILON)
        gath[z, place] = (values32 * scale * gain[...]).astype(jnp.bfloat16)
        return carry

    lax.fori_loop(0, tok_rows // NORM_ROWS, normalize, 0)
    expert = lax.broadcasted_iota(jnp.int32, shares.shape[1:], 0)
    share = jnp.zeros(shares.shape[1:], jnp.float32)
    for choice in range(routes.shape[0]):
        named = routes[choice : choice + 1, :] == expert
        share = share + jnp.where(named, route_weight[choice : choice + 1, :], 0.0)
    shares[z] = share

    def own_tokens(first, count, upward):
        if first == 0:
            share_copy(z, upward, above if upward else below).start()
        for part in range(first, first + count):
            if upward:
                tok_copy(z, part, up_send, above).start()
            else:
                tok_copy(z, part, down_send, below).start()

    half = PIECES // 2

    @pl.when(z < last)
    def _():
        own_tokens(0, half, True)

    @pl.when(z == 0)
    def _():
        own_tokens(half, half, True)

    @pl.when(z > 0)
    def _():
        own_tokens(0, half, False)

    @pl.when(z == last)
    def _():
        own_tokens(half, half, False)

    loads[6].wait()

    def launch_d(p, carry):
        d_over(p).start()
        return carry

    lax.fori_loop(0, CHUNKS, launch_d, 0)
    for load in loads[7:]:
        load.wait()

    def arrival(i, reach):
        s = i // half
        far = s < reach
        distance = jnp.where(far, s + 1, 2 * reach - s)
        part = jnp.where(far, 0, half) + i % half
        return distance, part

    def pump_tokens(i):
        for upward in (True, False):
            reach = z if upward else last - z
            distance, part = arrival(i, reach)
            block = jnp.clip(z - distance if upward else z + distance, 0, last)

            @pl.when(i < PIECES * reach)
            def _():
                tok_copy(block, part, up_send, above).wait_recv()

            @pl.when((i < PIECES * reach) & (part == 0))
            def _():
                share_copy(block, upward, above).wait_recv()

            @pl.when((i < PIECES * reach) & (part == 0) & (reach < last))
            def _():
                share_copy(block, upward, above if upward else below).start()

            @pl.when((i < PIECES * reach) & (reach < last))
            def _():
                if upward:
                    tok_copy(block, part, up_send, above).start()
                else:
                    tok_copy(block, part, down_send, below).start()

            @pl.when((i == PIECES * reach - 1) & (reach < last))
            def _():
                own_tokens(half, half, upward)

    per_group = sinks.shape[0]
    band = 2 * WINDOW
    quarter_rows = attn_ref.shape[0]
    blocks_each = quarter_rows // WINDOW

    def pair_copy(owner_x):
        return remote(
            mate_out.at[owner_x], mate_in.at[owner_x], pair_sem.at[0], pair_sem.at[1], mate
        )

    def attend_block(n):
        q_rows = qs[pl.ds(n * WINDOW, WINDOW)] * jnp.bfloat16(HEAD_DIM ** (-0.5))
        held = ext[:, pl.ds(pl.multiple_of(n * WINDOW, WINDOW), band)]
        keys = jnp.concatenate([held[:HEAD_DIM]] * per_group, axis=0)
        values = held[HEAD_DIM:]
        q_head = lax.broadcasted_iota(jnp.int32, q_rows.shape, 1) // HEAD_DIM
        stacked = jnp.concatenate(
            [jnp.where(q_head == h, q_rows, jnp.zeros_like(q_rows)) for h in range(per_group)],
            axis=0,
        )
        scores = jnp.dot(stacked, keys, preferred_element_type=jnp.float32)
        begins = lax.rem(ep * (qs.shape[0] // WINDOW) + n, lines * ROW * (qs.shape[0] // WINDOW) // SEQS) == 0
        row = lax.broadcasted_iota(jnp.int32, (WINDOW, band), 0)
        col = lax.broadcasted_iota(jnp.int32, (WINDOW, band), 1)
        valid = (col > row) & (col <= row + WINDOW) & (col >= jnp.where(begins, WINDOW, 0))
        weights = []
        for h in range(per_group):
            score = jnp.where(valid, scores[h * WINDOW : (h + 1) * WINDOW], NEGATIVE)
            sink = sinks[h]
            top = jnp.maximum(jnp.max(score, axis=1, keepdims=True), sink)
            powers = jnp.exp(score - top)
            total = jnp.sum(powers, axis=1, keepdims=True) + jnp.exp(sink - top)
            weights.append((powers * (1.0 / total)).astype(jnp.bfloat16))
        blank = jnp.zeros_like(values)
        spread = jnp.concatenate(
            [
                jnp.concatenate([values if g == h else blank for g in range(per_group)], axis=1)
                for h in range(per_group)
            ],
            axis=0,
        )
        heads = lax.dot_general(
            jnp.concatenate(weights, axis=1), spread, (((1,), (1,)), ((), ())),
            preferred_element_type=jnp.float32,
        ).astype(jnp.bfloat16)
        owner = n // blocks_each
        owner_x, owner_c = owner // CORES, owner % CORES
        place = pl.ds((n % blocks_each) * WINDOW, WINDOW)
        share = jnp.dot(heads, wo[...], preferred_element_type=jnp.float32)

        @pl.when(owner_c == c)
        def _():
            keep[owner_x, place] = share

        @pl.when(owner_c != c)
        def _():
            mate_out[owner_x, place] = share.astype(jnp.bfloat16)

    each = SLABS * WINDOW // attn_rows

    def slot(i, carry):
        gu_over(i).wait_recv()
        gu_plane(i).start()
        gu_mate(i, 0).start()

        @pl.when(i >= LAG)
        def _():
            gu_plane(i - LAG).wait_recv()
            gu_mate(i - LAG, 1).start()

        @pl.when(i % each == 0)
        def _():
            n = lax.rem(i // each + 1, attn_rows // WINDOW)

            @pl.when((n == 0) & behind)
            def _():
                halo.wait_recv()

            @pl.when((n == 0) & (ep == 0))
            def _():
                ext[:, pl.ds(0, WINDOW)] = jnp.zeros((ext.shape[0], WINDOW), ext.dtype)

            attend_block(n)

        @pl.when(i % each == each - 1)
        def _():
            pump_tokens(i // each)

        @pl.when((i % each == each - 1) & (i // each < lines))
        def _():
            block = jnp.minimum(i // each, last)

            @pl.when(z == 0)
            def _():
                from_line[0, block] = jnp.zeros(from_line.shape[2:], from_line.dtype)

            @pl.when(z == last)
            def _():
                from_line[1, block] = jnp.zeros(from_line.shape[2:], from_line.dtype)

        return carry

    lax.fori_loop(0, SLABS, slot, 0)
    for owner_x in range(TP // CORES):
        pair_copy(owner_x).start()

    def pass_down(j):
        d_over(j).wait_recv()
        d_plane(j).start()
        d_mate(j, 0).start()

    def late(p, carry):
        gu_plane(p).wait_recv()
        gu_mate(p, 1).start()
        return carry

    loaded(wgu.at[0, pl.ds(quarter, (TP - 1) * quarter)], gu_sem.at[1])

    square = (tok_rows, tok_rows)
    eye = lax.broadcasted_iota(jnp.int32, square, 0) == lax.broadcasted_iota(jnp.int32, square, 1)

    def activate(block, first, end):
        def one(expert, carry):
            pre = jnp.dot(gath[block], wgu[expert], preferred_element_type=jnp.float32)
            unit = clamped_unit(pre[:, :hidden], pre[:, hidden:])
            named = z * ROW + jnp.where(expert == 1, 1 - y, y)
            column = jnp.sum(
                jnp.where(eye, shares[block, pl.ds(named, 1), :], 0.0), axis=1, keepdims=True
            )
            act[expert] = (unit * column).astype(jnp.bfloat16)
            return carry

        lax.fori_loop(first, end, one, 0)

    def partial(cols):
        both = jnp.concatenate([act[0], act[1]], axis=1)
        return jnp.dot(both, wd[:, cols], preferred_element_type=jnp.float32)

    def line_copy(downward, block, j, device, holder):
        cols = pl.ds(j * chunk, chunk)
        row = jnp.where(downward == 1, lines - holder + block, block - holder)
        return remote(
            onward.at[block, :, cols], from_line.at[downward, block, :, cols],
            line_send.at[block], line_recv.at[row, j], device,
        )

    def pick(k):
        block = 0
        for zz in range(lines):
            others = sorted(
                (b for b in range(lines) if b != zz),
                key=lambda b: (-abs(b - zz), min(b, last - b)),
            )
            for kk, b in enumerate(others):
                block = jnp.where((z == zz) & (k == kk), b, block)
        return block

    def cross_copy():
        return remote(x_out, x_in, cross_send, cross_recv, over_x)

    edge = (z == 0) | (z == last)

    def send_cross():
        all_of(mate_in, pair_sem.at[0], pair_sem.at[1]).wait_recv()
        x_out[...] = (keep[1 - x] + mate_in[1 - x].astype(jnp.float32)).astype(jnp.bfloat16)
        cross_copy().start()

    def visit(k, carry):
        block = pick(k)
        downward = jnp.where(block < z, 1, 0)

        @pl.when((k > 0) & edge)
        def _():
            for e in range(half):
                distance, part = arrival(PIECES * (lines - 2) + (k - 1) * half + e, last)
                source = jnp.clip(jnp.where(z == 0, distance, last - distance), 0, last)
                tok_copy(source, part, up_send, above).wait_recv()

        activate(block, jnp.where(k == 0, ROW, 0), ROW)
        onto = jnp.clip(jnp.where(downward == 1, z - 1, z + 1), 0, last)
        device = at(onto, y, x, c)
        inner = jnp.where(downward == 1, z < last, z > 0)

        def one(j, carry):
            @pl.when(k == 0)
            def _():
                d_mate(j, 0).wait_recv()
                d_mate(j, 1).wait_recv()

            cols = pl.ds(pl.multiple_of(j * chunk, chunk), chunk)
            own = partial(cols)

            @pl.when(inner)
            def _():
                line_copy(downward, block, j, device, z).wait_recv()

            onward[block, :, cols] = (
                own + from_line[downward, block, :, cols].astype(jnp.float32)
            ).astype(jnp.bfloat16)
            line_copy(downward, block, j, device, onto).start()

            @pl.when((k == 0) & edge & (j + AHEAD < CHUNKS))
            def _():
                pass_down(jnp.minimum(j + AHEAD, CHUNKS - 1))

            @pl.when((k == 0) & (j + 1 < CHUNKS))
            def _():
                take_plane(jnp.minimum(j + 1, CHUNKS - 1))

            @pl.when((k == 0) & (j == CHUNKS - AHEAD - 1) & edge)
            def _():
                send_cross()

            return carry

        lax.fori_loop(0, CHUNKS, one, 0)
        return carry

    def take_plane(j):
        d_plane(j).wait_recv()
        d_mate(j, 1).start()

    activate(pick(0), 0, 1)
    pass_down(0)
    lax.fori_loop(SLABS - LAG, SLABS, late, 0)
    for p in range(1, AHEAD - 1):
        pass_down(p)
    for second in range(2):
        all_of(gu_whole, gm_recv.at[second], gm_recv.at[second]).wait_recv()
    activate(pick(0), 1, ROW)
    take_plane(0)
    pass_down(AHEAD - 1)

    @pl.when(jnp.logical_not(edge))
    def _():
        for p in range(AHEAD, CHUNKS):
            pass_down(p)
        send_cross()

    lax.fori_loop(0, last, visit, 0)
    activate(z, 0, ROW)

    def finish(j, carry):
        cols = pl.ds(pl.multiple_of(j * chunk, chunk), chunk)
        own = partial(cols)

        @pl.when(z > 0)
        def _():
            line_copy(0, z, j, above, z).wait_recv()

        @pl.when(z < last)
        def _():
            line_copy(1, z, j, above, z).wait_recv()

        routed_ref[:, cols] = (
            own + from_line[0, z, :, cols].astype(jnp.float32)
            + from_line[1, z, :, cols].astype(jnp.float32)
        ).astype(jnp.bfloat16)
        return carry

    keep[x] = keep[x] + mate_in[x].astype(jnp.float32)
    lax.fori_loop(0, CHUNKS - 1, finish, 0)
    cross_copy().wait_recv()
    attn_ref[...] = (keep[x] + x_in[...].astype(jnp.float32)).astype(jnp.bfloat16)
    finish(CHUNKS - 1, 0)

    @pl.when(ahead)
    def _():
        halo.wait_send()

    cross_copy().wait_send()
    all_of(mate_out, pair_sem.at[0], pair_sem.at[1]).wait_send()

    for kind, whole in enumerate((gu_whole, d_whole)):
        all_of(whole, y_send.at[kind], y_send.at[kind]).wait_send()
        all_of(whole, x_send.at[kind], x_send.at[kind]).wait_send()
        for second in range(2):
            all_of(whole, m_send.at[kind, second], m_send.at[kind, second]).wait_send()

    def drain(line, carry):
        @pl.when((line <= z) & (z < last))
        def _():
            all_of(gath.at[line], up_send.at[line], up_send.at[line]).wait_send()
            share_copy(line, True, above).wait_send()

        @pl.when((line >= z) & (z > 0))
        def _():
            all_of(gath.at[line], down_send.at[line], down_send.at[line]).wait_send()
            share_copy(line, False, below).wait_send()

        @pl.when(line != z)
        def _():
            all_of(onward.at[line], line_send.at[line], line_send.at[line]).wait_send()

        return carry

    lax.fori_loop(0, lines, drain, 0)


def fused_layer(*operands):
    moe_input, _, routes, _, gate_weight, _, _, queries, keys, _, sinks, out_weight = operands
    targets = lax.axis_size("ep")
    lines = targets // ROW
    tok_rows, width = moe_input.shape
    hidden = gate_weight.shape[1]
    attn_rows = queries.shape[0]
    quarter = (attn_rows // TP, out_weight.shape[1])
    block = (tok_rows, width)
    sem = pltpu.SemaphoreType.DMA
    pieces = SLABS + CHUNKS
    bf16, f32 = jnp.bfloat16, jnp.float32
    flops = 12 * lines * tok_rows * width * hidden
    return pl.pallas_call(
        functools.partial(fused_kernel, lines, width),
        out_shape=(pltpu.VMEM(block, bf16), pltpu.VMEM(quarter, bf16)),
        in_specs=[pl.BlockSpec(memory_space=pl.ANY)] * len(operands),
        out_specs=(pl.BlockSpec(memory_space=pltpu.VMEM), pl.BlockSpec(memory_space=pltpu.VMEM)),
        scratch_shapes=[
            pltpu.VMEM(block, bf16),
            pltpu.VMEM((1, width), f32),
            pltpu.VMEM(routes.shape, jnp.int32),
            pltpu.VMEM(routes.shape, f32),
            pltpu.VMEM((lines,) + block, bf16),
            pltpu.VMEM((lines, targets, tok_rows), f32),
            pltpu.VMEM((ROW, width, 2 * hidden), bf16),
            pltpu.VMEM((ROW * hidden, width), bf16),
            pltpu.VMEM((ROW, tok_rows, hidden), bf16),
            pltpu.VMEM((lines,) + block, bf16),
            pltpu.VMEM((2, lines) + block, bf16),
            pltpu.VMEM(queries.shape, bf16),
            pltpu.VMEM((2 * HEAD_DIM, WINDOW + attn_rows), bf16),
            pltpu.SMEM(sinks.shape, f32),
            pltpu.VMEM(out_weight.shape, bf16),
            pltpu.VMEM((TP // CORES,) + quarter, f32),
            pltpu.VMEM((TP // CORES,) + quarter, bf16),
            pltpu.VMEM((TP // CORES,) + quarter, bf16),
            pltpu.VMEM(quarter, bf16),
            pltpu.VMEM(quarter, bf16),
            sem((9,)),
            sem((2,)),
            sem((lines,)),
            sem((lines,)),
            sem((lines,)),
            sem((2,)),
            sem((lines,)),
            sem((lines,)),
            sem((lines, PIECES)),
            sem((2,)),
            sem((pieces,)),
            sem((2,)),
            sem((pieces,)),
            sem((2, 2)),
            sem((2,)),
            sem((2, CHUNKS)),
            sem((lines,)),
            sem((lines + 1, CHUNKS)),
            sem((2,)),
            sem,
            sem,
        ],
        compiler_params=pltpu.CompilerParams(
            collective_id=0, has_side_effects=True, vmem_limit_bytes=56 * 1024 * 1024
        ),
        cost_estimate=pl.CostEstimate(
            flops=flops, bytes_accessed=16 * tok_rows * width * lines, transcendentals=0
        ),
    )(*operands)


def fused_path(
    queries, head_keys, head_values, sink_logits, out_weight,
    moe_input, norm_gain, routes, route_weight, gate_weight, up_weight, down_weight,
):
    routed, attended = fused_layer(
        moe_input, norm_gain.reshape(1, -1), routes.T, route_weight.T,
        gate_weight[0], up_weight[0], down_weight[0],
        queries, head_keys.T, head_values.T, sink_logits, out_weight,
    )
    return (attended, routed)


def fits(queries, head_keys, sink_logits, moe_input, routes):
    targets = lax.axis_size("ep")
    tok_rows = moe_input.shape[0]
    return (
        2 * routes.shape[1] * tok_rows // targets >= tok_rows
        and targets == 4 * ROW
        and lax.axis_size("tp") == TP
        and head_keys.shape[1] == HEAD_DIM
        and sink_logits.shape[0] == 4
        and (SLABS * WINDOW) % queries.shape[0] == 0
        and queries.shape[0] >= 4 * ROW * WINDOW
    )


def on_device(
    queries,
    head_keys,
    head_values,
    sink_logits,
    out_weight,
    moe_input,
    norm_gain,
    routes,
    route_weight,
    gate_weight,
    up_weight,
    down_weight,
):
    if fits(queries, head_keys, sink_logits, moe_input, routes):
        return fused_path(
            queries, head_keys, head_values, sink_logits, out_weight, moe_input, norm_gain,
            routes, route_weight, gate_weight, up_weight, down_weight,
        )
    attention_out = attend(queries, head_keys, head_values, sink_logits, out_weight)
    routed_out = experts_part(
        moe_input, norm_gain, routes, route_weight, gate_weight, up_weight, down_weight
    )
    return (attention_out, routed_out)


def solution(mesh):
    placed = (
        P("ep", "tp"),
        P("ep", "tp"),
        P("ep", "tp"),
        P("tp"),
        P("tp", None),
        P(("ep", "tp"), None),
        P(),
        P(("ep", "tp"), None),
        P(("ep", "tp"), None),
        P("ep", None, None),
        P("ep", None, None),
        P("ep", None, None),
    )
    return jax.shard_map(
        on_device,
        mesh=mesh,
        in_specs=placed,
        out_specs=(P(("ep", "tp"), None), P(("ep", "tp"), None)),
        check_vma=False,
    )
```

```python
import functools

import jax
import jax.numpy as jnp
from jax import lax
from jax.experimental import pallas as pl
from jax.experimental.pallas import tpu as pltpu
from jax.sharding import PartitionSpec as P

HEAD_DIM = 64
WINDOW = 128
SEQS = 1


EPSILON = 1e-05
NEGATIVE = -1e30


def passed_along(value, axis, steps):
    count = lax.axis_size(axis)
    first, last = (max(0, -steps), min(count, count - steps))
    return lax.ppermute(value, axis, [(source, source + steps) for source in range(first, last)])


def clamped_unit(gate_pre, up_pre):
    gate_cut = jnp.minimum(gate_pre, 7.0)
    up_cut = jnp.clip(up_pre, -7.0, 7.0)
    return gate_cut * jax.nn.sigmoid(1.702 * gate_cut) * (up_cut + 1.0)


def attend(queries, head_keys, head_values, sink_logits, out_weight):
    tok_rows = queries.shape[0]
    local_heads = sink_logits.shape[0]
    local_kv = head_keys.shape[1] // HEAD_DIM
    per_group = local_heads // local_kv
    block_count = tok_rows // WINDOW
    key_width = local_kv * HEAD_DIM
    kv_rows = jnp.concatenate([head_keys, head_values], axis=1)
    earlier = passed_along(kv_rows[tok_rows - WINDOW :], "ep", 1)
    extended = jnp.concatenate([earlier, kv_rows], axis=0)
    banded = jnp.concatenate(
        [
            extended[:tok_rows].reshape(block_count, WINDOW, 2 * key_width),
            kv_rows.reshape(block_count, WINDOW, 2 * key_width),
        ],
        axis=1,
    )
    band_keys = banded[:, :, :key_width].reshape(block_count, 2 * WINDOW, local_kv, HEAD_DIM)
    band_values = banded[:, :, key_width:].reshape(block_count, 2 * WINDOW, local_kv, HEAD_DIM)
    blocked = queries.reshape(block_count, WINDOW, local_kv, per_group, HEAD_DIM)
    scores = jnp.einsum(
        "nqkgd,nskd->nkgqs", blocked, band_keys, preferred_element_type=jnp.float32
    ) * HEAD_DIM ** (-0.5)
    offset = lax.axis_index("ep") * tok_rows
    seq_len = tok_rows * lax.axis_size("ep") // SEQS
    query_pos = offset + jnp.arange(tok_rows, dtype=jnp.int32).reshape(block_count, WINDOW)
    key_pos = (
        offset
        - WINDOW
        + (jnp.arange(block_count, dtype=jnp.int32) * WINDOW)[:, None]
        + jnp.arange(2 * WINDOW, dtype=jnp.int32)[None, :]
    )
    distance = query_pos[:, :, None] - key_pos[:, None, :]
    starts = query_pos // seq_len * seq_len
    valid = (distance >= 0) & (distance < WINDOW) & (key_pos[:, None, :] >= starts[:, :, None])
    scores = jnp.where(valid[:, None, None], scores, NEGATIVE)
    sinks = sink_logits.reshape(local_kv, per_group, 1, 1)
    maxima = jnp.maximum(jnp.max(scores, axis=-1, keepdims=True), sinks)
    powers = jnp.exp(scores - maxima)
    weights = (powers / (jnp.sum(powers, axis=-1, keepdims=True) + jnp.exp(sinks - maxima))).astype(
        jnp.bfloat16
    )
    heads_out = jnp.einsum(
        "nkgqs,nskd->nqkgd", weights, band_values, preferred_element_type=jnp.float32
    )
    heads_out = heads_out.astype(jnp.bfloat16).reshape(tok_rows, local_heads * HEAD_DIM)
    summed = lax.psum_scatter(
        jnp.dot(heads_out, out_weight, preferred_element_type=jnp.float32),
        "tp",
        scatter_dimension=0,
        tiled=True,
    )
    return summed.astype(jnp.bfloat16)


def experts_part(moe_input, norm_gain, routes, route_weight, gate_weight, up_weight, down_weight):
    tok_rows, model_width = moe_input.shape
    choice_count = routes.shape[1]
    targets = lax.axis_size("ep")
    capacity = 2 * choice_count * tok_rows // targets
    values32 = moe_input.astype(jnp.float32)
    scale = lax.rsqrt(jnp.mean(values32 * values32, axis=-1, keepdims=True) + EPSILON)
    normed = (values32 * scale * norm_gain).astype(jnp.bfloat16)
    if capacity >= tok_rows:
        experts = jnp.arange(targets, dtype=jnp.int32)
        named = routes[:, :, None] == experts[None, None, :]
        shares = jnp.sum(jnp.where(named, route_weight[:, :, None], 0.0), axis=1)
        everyone = lax.all_gather(normed, "ep", axis=0, tiled=True)
        mine = lax.all_to_all(shares.T[:, None], "ep", split_axis=0, concat_axis=0, tiled=True)
        gate_pre = jnp.dot(everyone, gate_weight[0], preferred_element_type=jnp.float32)
        up_pre = jnp.dot(everyone, up_weight[0], preferred_element_type=jnp.float32)
        act = clamped_unit(gate_pre, up_pre).astype(jnp.bfloat16)
        result = jnp.dot(act, down_weight[0], preferred_element_type=jnp.float32)
        part = result.astype(jnp.bfloat16).astype(jnp.float32) * mine.reshape(-1, 1)
        return lax.psum_scatter(
            part.astype(jnp.bfloat16), "ep", scatter_dimension=0, tiled=True
        )
    flat_routes = routes.reshape(-1)
    onehot = (flat_routes[:, None] == jnp.arange(targets, dtype=jnp.int32)[None, :]).astype(
        jnp.int32
    )
    earlier_count = jnp.sum((jnp.cumsum(onehot, axis=0) - onehot) * onehot, axis=1)
    slot_index = flat_routes * capacity + earlier_count
    copies = jnp.repeat(normed, choice_count, axis=0)
    outgoing = jnp.zeros((targets * capacity, model_width), jnp.bfloat16).at[slot_index].set(copies)
    outgoing = outgoing.reshape(targets, capacity, model_width)
    arrived = lax.all_to_all(outgoing, "ep", split_axis=0, concat_axis=0, tiled=True)
    flat_rows = arrived.reshape(-1, model_width)
    gate_pre = jnp.dot(flat_rows, gate_weight[0], preferred_element_type=jnp.float32)
    up_pre = jnp.dot(flat_rows, up_weight[0], preferred_element_type=jnp.float32)
    act = clamped_unit(gate_pre, up_pre).astype(jnp.bfloat16)
    result = jnp.dot(act, down_weight[0], preferred_element_type=jnp.float32).astype(jnp.bfloat16)
    came_back = lax.all_to_all(
        result.reshape(arrived.shape), "ep", split_axis=0, concat_axis=0, tiled=True
    )
    picked = came_back.reshape(targets * capacity, model_width)[slot_index]
    weighted = (
        picked.astype(jnp.float32).reshape(tok_rows, choice_count, model_width)
        * route_weight[:, :, None]
    )
    return jnp.sum(weighted, axis=1).astype(jnp.bfloat16)


ROW = 2
CORES = 2
TP = 4
PIECES = 4
CHUNKS = 8
SLABS = 16
LAG = 3
GROUP = 4
AHEAD = 4
NORM_ROWS = 16


def fused_kernel(
    lines, width,
    rows_hbm, gain_hbm, routes_hbm, route_weight_hbm, gate_hbm, up_hbm, down_hbm,
    q_hbm, keys_hbm, values_hbm, sinks_hbm, proj_hbm,
    routed_ref, attn_ref,
    raw, gain, routes, route_weight,
    gath, shares, wgu, wd, act, onward, from_line,
    qs, ext, sinks, wo, keep, mate_out, mate_in, x_out, x_in,
    local_sem, gu_sem, share_up, share_down, share_recv, halo_sem,
    up_send, down_send, tok_recv,
    y_send, y_recv, x_send, x_recv, m_send, gm_recv, m_recv,
    line_send, line_recv, pair_sem, cross_send, cross_recv,
):
    ep, tp = lax.axis_index("ep"), lax.axis_index("tp")
    z, y, x, c = ep // ROW, ep % ROW, tp // CORES, tp % CORES
    tok_rows, model_width = routed_ref.shape
    hidden = gate_hbm.shape[1]
    attn_rows = q_hbm.shape[0]
    piece = tok_rows // PIECES
    chunk = model_width // CHUNKS
    last = lines - 1
    quarter = wgu.shape[1] // TP
    slab = quarter // SLABS

    def at(zz, yy, xx, cc):
        return {"ep": zz * ROW + yy, "tp": xx * CORES + cc}

    def remote(source, target, send, recv, device):
        return pltpu.make_async_remote_copy(
            src_ref=source, dst_ref=target, send_sem=send, recv_sem=recv,
            device_id=device, device_id_type=pl.DeviceIdType.MESH,
        )

    above = at(jnp.minimum(z + 1, last), y, x, c)
    below = at(jnp.maximum(z - 1, 0), y, x, c)
    over_y, over_x, mate = at(z, 1 - y, x, c), at(z, y, 1 - x, c), at(z, y, x, 1 - c)

    def gu_load(q, half):
        place = pl.ds(q * quarter, quarter)
        source = (gate_hbm, up_hbm)[half]
        return pltpu.make_async_copy(
            source.at[place], wgu.at[0, place, pl.ds(half * hidden, hidden)],
            gu_sem.at[jnp.where(q == tp, 0, 1)],
        )

    def loaded(target, semaphore):
        pltpu.make_async_copy(target, target, semaphore).wait()

    own = pl.ds(WINDOW, attn_rows)
    loads = [
        pltpu.make_async_copy(source, target, local_sem.at[max(i - 1, 0)])
        for i, (source, target) in enumerate([
            (keys_hbm, ext.at[pl.ds(0, HEAD_DIM), own]),
            (values_hbm, ext.at[pl.ds(HEAD_DIM, HEAD_DIM), own]),
            (rows_hbm, raw),
            (gain_hbm, gain),
            (routes_hbm, routes),
            (route_weight_hbm, route_weight),
            (down_hbm, wd.at[pl.ds(0, hidden)]),
            (q_hbm, qs),
            (sinks_hbm, sinks),
            (proj_hbm, wo),
        ])
    ]
    gu_load(tp, 0).start()
    gu_load(tp, 1).start()
    for load in loads:
        load.start()
    for step in range(1, TP):
        gu_load(lax.rem(tp + step, TP), 0).start()
        gu_load(lax.rem(tp + step, TP), 1).start()

    ahead = ep + 1 < lines * ROW
    behind = ep > 0
    skew = jnp.where(y == 1, z < last, z > 0)
    skew_ep = jnp.where(y == 1, jnp.minimum(ep + 1, lines * ROW - 1), jnp.maximum(ep - 1, 0))
    barrier = pltpu.get_barrier_semaphore()

    def greet(device):
        pl.semaphore_signal(barrier, inc=1, device_id=device, device_id_type=pl.DeviceIdType.MESH)

    @pl.when(z < last)
    def _():
        greet(above)

    @pl.when(z > 0)
    def _():
        greet(below)

    greet(over_y)
    greet(over_x)
    greet(mate)

    @pl.when(skew)
    def _():
        greet({"ep": skew_ep, "tp": tp})

    beside = jnp.where(z < last, 1, 0) + jnp.where(z > 0, 1, 0)
    pl.semaphore_wait(barrier, beside + 3 + jnp.where(skew, 1, 0))

    halo = remote(
        ext.at[:, pl.ds(attn_rows, WINDOW)], ext.at[:, pl.ds(0, WINDOW)], halo_sem.at[0],
        halo_sem.at[1], {"ep": jnp.minimum(ep + 1, lines * ROW - 1), "tp": tp},
    )

    def share_copy(block, upward, device):
        sems = share_up if upward else share_down
        return remote(
            shares.at[block], shares.at[block], sems.at[block], share_recv.at[block], device
        )

    def all_of(view, send, recv):
        return remote(view, view, send, recv, mate)

    def tok_copy(block, part, sems, device):
        view = gath.at[block, pl.ds(part * piece, piece)]
        return remote(view, view, sems.at[block], tok_recv.at[block, part], device)

    def gu_view(expert, q, p):
        return wgu.at[expert, pl.ds(q * quarter + p * slab, slab)]

    def d_view(expert, q, p):
        return wd.at[
            pl.ds(expert * hidden + q * (hidden // TP), hidden // TP), pl.ds(p * chunk, chunk)
        ]

    def weight_copies(view, kind, base, plane_recv, mate_recv):
        def over_link(p):
            return remote(
                view(0, tp, p), view(1, tp, p), y_send.at[kind], y_recv.at[base + p], over_y
            )

        def to_plane(p):
            return remote(
                view(1, tp, p), view(1, tp, p), x_send.at[kind], plane_recv(p), over_x
            )

        def to_mate(p, second):
            q = (1 - x) * CORES + c if second else tp
            return remote(
                view(1, q, p), view(1, q, p), m_send.at[kind, second], mate_recv(second, p), mate
            )

        return over_link, to_plane, to_mate

    gu_over, gu_plane, gu_mate = weight_copies(
        gu_view, 0, 0, lambda p: x_recv.at[p // GROUP], lambda second, p: gm_recv.at[second]
    )
    d_over, d_plane, d_mate = weight_copies(
        d_view, 1, SLABS, lambda p: x_recv.at[SLABS // GROUP + p], lambda second, p: m_recv.at[p]
    )
    gu_whole = wgu.at[1, pl.ds(0, quarter)]
    d_whole = wd.at[pl.ds(0, hidden // TP)]

    loaded(ext.at[:, own], local_sem.at[0])

    @pl.when(ahead)
    def _():
        halo.start()

    loaded(wgu.at[0, pl.ds(0, quarter)], gu_sem.at[0])

    def launch_gu(p, carry):
        gu_over(p).start()
        return carry

    lax.fori_loop(0, SLABS, launch_gu, 0)
    for load in loads[2:6]:
        load.wait()

    def normalize(i, carry):
        place = pl.ds(i * NORM_ROWS, NORM_ROWS)
        values32 = raw[place].astype(jnp.float32)
        mean = jnp.sum(values32 * values32, axis=-1, keepdims=True) * (1.0 / model_width)
        scale = lax.rsqrt(mean + EPSILON)
        gath[z, place] = (values32 * scale * gain[...]).astype(jnp.bfloat16)
        return carry

    lax.fori_loop(0, tok_rows // NORM_ROWS, normalize, 0)
    expert = lax.broadcasted_iota(jnp.int32, shares.shape[1:], 0)
    share = jnp.zeros(shares.shape[1:], jnp.float32)
    for choice in range(routes.shape[0]):
        named = routes[choice : choice + 1, :] == expert
        share = share + jnp.where(named, route_weight[choice : choice + 1, :], 0.0)
    shares[z] = share

    def own_tokens(first, count, upward):
        if first == 0:
            share_copy(z, upward, above if upward else below).start()
        for part in range(first, first + count):
            if upward:
                tok_copy(z, part, up_send, above).start()
            else:
                tok_copy(z, part, down_send, below).start()

    half = PIECES // 2

    @pl.when(z < last)
    def _():
        own_tokens(0, half, True)

    @pl.when(z == 0)
    def _():
        own_tokens(half, half, True)

    @pl.when(z > 0)
    def _():
        own_tokens(0, half, False)

    @pl.when(z == last)
    def _():
        own_tokens(half, half, False)

    loads[6].wait()

    def launch_d(p, carry):
        d_over(p).start()
        return carry

    lax.fori_loop(0, CHUNKS, launch_d, 0)
    for load in loads[7:]:
        load.wait()

    def arrival(i, reach):
        s = i // half
        far = s < reach
        distance = jnp.where(far, s + 1, 2 * reach - s)
        part = jnp.where(far, 0, half) + i % half
        return distance, part

    def pump_tokens(i):
        for upward in (True, False):
            reach = z if upward else last - z
            distance, part = arrival(i, reach)
            block = jnp.clip(z - distance if upward else z + distance, 0, last)

            @pl.when(i < PIECES * reach)
            def _():
                tok_copy(block, part, up_send, above).wait_recv()

            @pl.when((i < PIECES * reach) & (part == 0))
            def _():
                share_copy(block, upward, above).wait_recv()

            @pl.when((i < PIECES * reach) & (part == 0) & (reach < last))
            def _():
                share_copy(block, upward, above if upward else below).start()

            @pl.when((i < PIECES * reach) & (reach < last))
            def _():
                if upward:
                    tok_copy(block, part, up_send, above).start()
                else:
                    tok_copy(block, part, down_send, below).start()

            @pl.when((i == PIECES * reach - 1) & (reach < last))
            def _():
                own_tokens(half, half, upward)

    per_group = sinks.shape[0]
    band = 2 * WINDOW
    quarter_rows = attn_ref.shape[0]
    blocks_each = quarter_rows // WINDOW

    def pair_copy(owner_x):
        return remote(
            mate_out.at[owner_x], mate_in.at[owner_x], pair_sem.at[0], pair_sem.at[1], mate
        )

    def attend_block(n):
        q_rows = qs[pl.ds(n * WINDOW, WINDOW)] * jnp.bfloat16(HEAD_DIM ** (-0.5))
        held = ext[:, pl.ds(pl.multiple_of(n * WINDOW, WINDOW), band)]
        keys = jnp.concatenate([held[:HEAD_DIM]] * per_group, axis=0)
        values = held[HEAD_DIM:]
        q_head = lax.broadcasted_iota(jnp.int32, q_rows.shape, 1) // HEAD_DIM
        stacked = jnp.concatenate(
            [jnp.where(q_head == h, q_rows, jnp.zeros_like(q_rows)) for h in range(per_group)],
            axis=0,
        )
        scores = jnp.dot(stacked, keys, preferred_element_type=jnp.float32)
        begins = lax.rem(ep * (qs.shape[0] // WINDOW) + n, lines * ROW * (qs.shape[0] // WINDOW) // SEQS) == 0
        row = lax.broadcasted_iota(jnp.int32, (WINDOW, band), 0)
        col = lax.broadcasted_iota(jnp.int32, (WINDOW, band), 1)
        valid = (col > row) & (col <= row + WINDOW) & (col >= jnp.where(begins, WINDOW, 0))
        weights = []
        for h in range(per_group):
            score = jnp.where(valid, scores[h * WINDOW : (h + 1) * WINDOW], NEGATIVE)
            sink = sinks[h]
            top = jnp.maximum(jnp.max(score, axis=1, keepdims=True), sink)
            powers = jnp.exp(score - top)
            total = jnp.sum(powers, axis=1, keepdims=True) + jnp.exp(sink - top)
            weights.append((powers * (1.0 / total)).astype(jnp.bfloat16))
        blank = jnp.zeros_like(values)
        spread = jnp.concatenate(
            [
                jnp.concatenate([values if g == h else blank for g in range(per_group)], axis=1)
                for h in range(per_group)
            ],
            axis=0,
        )
        heads = lax.dot_general(
            jnp.concatenate(weights, axis=1), spread, (((1,), (1,)), ((), ())),
            preferred_element_type=jnp.float32,
        ).astype(jnp.bfloat16)
        owner = n // blocks_each
        owner_x, owner_c = owner // CORES, owner % CORES
        place = pl.ds((n % blocks_each) * WINDOW, WINDOW)
        share = jnp.dot(heads, wo[...], preferred_element_type=jnp.float32)

        @pl.when(owner_c == c)
        def _():
            keep[owner_x, place] = share

        @pl.when(owner_c != c)
        def _():
            mate_out[owner_x, place] = share.astype(jnp.bfloat16)

    each = SLABS * WINDOW // attn_rows

    def take_group(g):
        q = (1 - x) * CORES + c
        rows = wgu.at[1, pl.ds(q * quarter + g * (GROUP * slab), GROUP * slab)]
        all_of(rows, x_recv.at[g], x_recv.at[g]).wait_recv()
        remote(rows, rows, m_send.at[0, 1], gm_recv.at[1], mate).start()

    def slot(i, carry):
        gu_over(i).wait_recv()
        gu_plane(i).start()
        gu_mate(i, 0).start()

        @pl.when((i >= LAG + GROUP - 1) & ((i - LAG) % GROUP == GROUP - 1))
        def _():
            take_group((i - LAG) // GROUP)

        @pl.when(i % each == 0)
        def _():
            n = lax.rem(i // each + 1, attn_rows // WINDOW)

            @pl.when((n == 0) & behind)
            def _():
                halo.wait_recv()

            @pl.when((n == 0) & (ep == 0))
            def _():
                ext[:, pl.ds(0, WINDOW)] = jnp.zeros((ext.shape[0], WINDOW), ext.dtype)

            attend_block(n)

        @pl.when(i % each == each - 1)
        def _():
            pump_tokens(i // each)

        @pl.when((i % each == each - 1) & (i // each < lines))
        def _():
            block = jnp.minimum(i // each, last)

            @pl.when(z == 0)
            def _():
                from_line[0, block] = jnp.zeros(from_line.shape[2:], from_line.dtype)

            @pl.when(z == last)
            def _():
                from_line[1, block] = jnp.zeros(from_line.shape[2:], from_line.dtype)

        return carry

    lax.fori_loop(0, SLABS, slot, 0)
    for owner_x in range(TP // CORES):
        pair_copy(owner_x).start()

    def pass_down(j):
        d_over(j).wait_recv()
        d_plane(j).start()
        d_mate(j, 0).start()

    def late(g, carry):
        take_group(g)
        return carry

    loaded(wgu.at[0, pl.ds(quarter, (TP - 1) * quarter)], gu_sem.at[1])

    square = (tok_rows, tok_rows)
    eye = lax.broadcasted_iota(jnp.int32, square, 0) == lax.broadcasted_iota(jnp.int32, square, 1)

    def activate(block, first, end):
        def one(expert, carry):
            pre = jnp.dot(gath[block], wgu[expert], preferred_element_type=jnp.float32)
            unit = clamped_unit(pre[:, :hidden], pre[:, hidden:])
            named = z * ROW + jnp.where(expert == 1, 1 - y, y)
            column = jnp.sum(
                jnp.where(eye, shares[block, pl.ds(named, 1), :], 0.0), axis=1, keepdims=True
            )
            act[expert] = (unit * column).astype(jnp.bfloat16)
            return carry

        lax.fori_loop(first, end, one, 0)

    def partial(cols):
        both = jnp.concatenate([act[0], act[1]], axis=1)
        return jnp.dot(both, wd[:, cols], preferred_element_type=jnp.float32)

    def line_copy(downward, block, j, device, holder):
        cols = pl.ds(j * chunk, chunk)
        row = jnp.where(downward == 1, lines - holder + block, block - holder)
        return remote(
            onward.at[block, :, cols], from_line.at[downward, block, :, cols],
            line_send.at[block], line_recv.at[row, j], device,
        )

    def pick(k):
        block = 0
        for zz in range(lines):
            others = sorted(
                (b for b in range(lines) if b != zz),
                key=lambda b: (-abs(b - zz), min(b, last - b)),
            )
            for kk, b in enumerate(others):
                block = jnp.where((z == zz) & (k == kk), b, block)
        return block

    def cross_copy():
        return remote(x_out, x_in, cross_send, cross_recv, over_x)

    edge = (z == 0) | (z == last)

    def send_cross():
        all_of(mate_in, pair_sem.at[0], pair_sem.at[1]).wait_recv()
        x_out[...] = (keep[1 - x] + mate_in[1 - x].astype(jnp.float32)).astype(jnp.bfloat16)
        cross_copy().start()

    def visit(k, carry):
        block = pick(k)
        downward = jnp.where(block < z, 1, 0)

        @pl.when((k > 0) & edge)
        def _():
            for e in range(half):
                distance, part = arrival(PIECES * (lines - 2) + (k - 1) * half + e, last)
                source = jnp.clip(jnp.where(z == 0, distance, last - distance), 0, last)
                tok_copy(source, part, up_send, above).wait_recv()

        activate(block, jnp.where(k == 0, ROW, 0), ROW)
        onto = jnp.clip(jnp.where(downward == 1, z - 1, z + 1), 0, last)
        device = at(onto, y, x, c)
        inner = jnp.where(downward == 1, z < last, z > 0)

        def one(j, carry):
            @pl.when(k == 0)
            def _():
                both = wd.at[pl.ds(0, 2 * (hidden // TP)), pl.ds(0, chunk)]
                all_of(both, m_recv.at[j], m_recv.at[j]).wait_recv()

            cols = pl.ds(pl.multiple_of(j * chunk, chunk), chunk)
            own = partial(cols)

            @pl.when(inner)
            def _():
                line_copy(downward, block, j, device, z).wait_recv()

            onward[block, :, cols] = (
                own + from_line[downward, block, :, cols].astype(jnp.float32)
            ).astype(jnp.bfloat16)
            line_copy(downward, block, j, device, onto).start()

            @pl.when((k == 0) & edge & (j + AHEAD < CHUNKS))
            def _():
                pass_down(jnp.minimum(j + AHEAD, CHUNKS - 1))

            @pl.when((k == 0) & (j + 1 < CHUNKS))
            def _():
                take_plane(jnp.minimum(j + 1, CHUNKS - 1))

            @pl.when((k == 0) & (j == CHUNKS - AHEAD - 1) & edge)
            def _():
                send_cross()

            return carry

        lax.fori_loop(0, CHUNKS, one, 0)
        return carry

    def take_plane(j):
        d_plane(j).wait_recv()
        d_mate(j, 1).start()

    activate(pick(0), 0, 1)
    pass_down(0)
    lax.fori_loop((SLABS - LAG) // GROUP, SLABS // GROUP, late, 0)
    for p in range(1, AHEAD - 1):
        pass_down(p)
    for second in range(2):
        all_of(gu_whole, gm_recv.at[second], gm_recv.at[second]).wait_recv()
    activate(pick(0), 1, ROW)
    take_plane(0)
    pass_down(AHEAD - 1)

    @pl.when(jnp.logical_not(edge))
    def _():
        for p in range(AHEAD, CHUNKS):
            pass_down(p)
        send_cross()

    lax.fori_loop(0, last, visit, 0)
    activate(z, 0, ROW)

    def finish(j, carry):
        cols = pl.ds(pl.multiple_of(j * chunk, chunk), chunk)
        own = partial(cols)

        @pl.when(z > 0)
        def _():
            line_copy(0, z, j, above, z).wait_recv()

        @pl.when(z < last)
        def _():
            line_copy(1, z, j, above, z).wait_recv()

        routed_ref[:, cols] = (
            own + from_line[0, z, :, cols].astype(jnp.float32)
            + from_line[1, z, :, cols].astype(jnp.float32)
        ).astype(jnp.bfloat16)
        return carry

    keep[x] = keep[x] + mate_in[x].astype(jnp.float32)
    lax.fori_loop(0, CHUNKS - 1, finish, 0)
    cross_copy().wait_recv()
    attn_ref[...] = (keep[x] + x_in[...].astype(jnp.float32)).astype(jnp.bfloat16)
    finish(CHUNKS - 1, 0)

    @pl.when(ahead)
    def _():
        halo.wait_send()

    cross_copy().wait_send()
    all_of(mate_out, pair_sem.at[0], pair_sem.at[1]).wait_send()

    for kind, whole in enumerate((gu_whole, d_whole)):
        all_of(whole, y_send.at[kind], y_send.at[kind]).wait_send()
        all_of(whole, x_send.at[kind], x_send.at[kind]).wait_send()
        for second in range(2):
            all_of(whole, m_send.at[kind, second], m_send.at[kind, second]).wait_send()

    def drain(line, carry):
        @pl.when((line <= z) & (z < last))
        def _():
            all_of(gath.at[line], up_send.at[line], up_send.at[line]).wait_send()
            share_copy(line, True, above).wait_send()

        @pl.when((line >= z) & (z > 0))
        def _():
            all_of(gath.at[line], down_send.at[line], down_send.at[line]).wait_send()
            share_copy(line, False, below).wait_send()

        @pl.when(line != z)
        def _():
            all_of(onward.at[line], line_send.at[line], line_send.at[line]).wait_send()

        return carry

    lax.fori_loop(0, lines, drain, 0)


def fused_layer(*operands):
    moe_input, _, routes, _, gate_weight, _, _, queries, keys, _, sinks, out_weight = operands
    targets = lax.axis_size("ep")
    lines = targets // ROW
    tok_rows, width = moe_input.shape
    hidden = gate_weight.shape[1]
    attn_rows = queries.shape[0]
    quarter = (attn_rows // TP, out_weight.shape[1])
    block = (tok_rows, width)
    sem = pltpu.SemaphoreType.DMA
    pieces = SLABS + CHUNKS
    bf16, f32 = jnp.bfloat16, jnp.float32
    flops = 12 * lines * tok_rows * width * hidden
    return pl.pallas_call(
        functools.partial(fused_kernel, lines, width),
        out_shape=(pltpu.VMEM(block, bf16), pltpu.VMEM(quarter, bf16)),
        in_specs=[pl.BlockSpec(memory_space=pl.ANY)] * len(operands),
        out_specs=(pl.BlockSpec(memory_space=pltpu.VMEM), pl.BlockSpec(memory_space=pltpu.VMEM)),
        scratch_shapes=[
            pltpu.VMEM(block, bf16),
            pltpu.VMEM((1, width), f32),
            pltpu.VMEM(routes.shape, jnp.int32),
            pltpu.VMEM(routes.shape, f32),
            pltpu.VMEM((lines,) + block, bf16),
            pltpu.VMEM((lines, targets, tok_rows), f32),
            pltpu.VMEM((ROW, width, 2 * hidden), bf16),
            pltpu.VMEM((ROW * hidden, width), bf16),
            pltpu.VMEM((ROW, tok_rows, hidden), bf16),
            pltpu.VMEM((lines,) + block, bf16),
            pltpu.VMEM((2, lines) + block, bf16),
            pltpu.VMEM(queries.shape, bf16),
            pltpu.VMEM((2 * HEAD_DIM, WINDOW + attn_rows), bf16),
            pltpu.SMEM(sinks.shape, f32),
            pltpu.VMEM(out_weight.shape, bf16),
            pltpu.VMEM((TP // CORES,) + quarter, f32),
            pltpu.VMEM((TP // CORES,) + quarter, bf16),
            pltpu.VMEM((TP // CORES,) + quarter, bf16),
            pltpu.VMEM(quarter, bf16),
            pltpu.VMEM(quarter, bf16),
            sem((9,)),
            sem((2,)),
            sem((lines,)),
            sem((lines,)),
            sem((lines,)),
            sem((2,)),
            sem((lines,)),
            sem((lines,)),
            sem((lines, PIECES)),
            sem((2,)),
            sem((pieces,)),
            sem((2,)),
            sem((SLABS // GROUP + CHUNKS,)),
            sem((2, 2)),
            sem((2,)),
            sem((CHUNKS,)),
            sem((lines,)),
            sem((lines + 1, CHUNKS)),
            sem((2,)),
            sem,
            sem,
        ],
        compiler_params=pltpu.CompilerParams(
            collective_id=0, has_side_effects=True, vmem_limit_bytes=56 * 1024 * 1024
        ),
        cost_estimate=pl.CostEstimate(
            flops=flops, bytes_accessed=16 * tok_rows * width * lines, transcendentals=0
        ),
    )(*operands)


def fused_path(
    queries, head_keys, head_values, sink_logits, out_weight,
    moe_input, norm_gain, routes, route_weight, gate_weight, up_weight, down_weight,
):
    routed, attended = fused_layer(
        moe_input, norm_gain.reshape(1, -1), routes.T, route_weight.T,
        gate_weight[0], up_weight[0], down_weight[0],
        queries, head_keys.T, head_values.T, sink_logits, out_weight,
    )
    return (attended, routed)


def fits(queries, head_keys, sink_logits, moe_input, routes):
    targets = lax.axis_size("ep")
    tok_rows = moe_input.shape[0]
    return (
        2 * routes.shape[1] * tok_rows // targets >= tok_rows
        and targets == 4 * ROW
        and lax.axis_size("tp") == TP
        and head_keys.shape[1] == HEAD_DIM
        and sink_logits.shape[0] == 4
        and (SLABS * WINDOW) % queries.shape[0] == 0
        and queries.shape[0] >= 4 * ROW * WINDOW
    )


def on_device(
    queries,
    head_keys,
    head_values,
    sink_logits,
    out_weight,
    moe_input,
    norm_gain,
    routes,
    route_weight,
    gate_weight,
    up_weight,
    down_weight,
):
    if fits(queries, head_keys, sink_logits, moe_input, routes):
        return fused_path(
            queries, head_keys, head_values, sink_logits, out_weight, moe_input, norm_gain,
            routes, route_weight, gate_weight, up_weight, down_weight,
        )
    attention_out = attend(queries, head_keys, head_values, sink_logits, out_weight)
    routed_out = experts_part(
        moe_input, norm_gain, routes, route_weight, gate_weight, up_weight, down_weight
    )
    return (attention_out, routed_out)


def solution(mesh):
    placed = (
        P("ep", "tp"),
        P("ep", "tp"),
        P("ep", "tp"),
        P("tp"),
        P("tp", None),
        P(("ep", "tp"), None),
        P(),
        P(("ep", "tp"), None),
        P(("ep", "tp"), None),
        P("ep", None, None),
        P("ep", None, None),
        P("ep", None, None),
    )
    return jax.shard_map(
        on_device,
        mesh=mesh,
        in_specs=placed,
        out_specs=(P(("ep", "tp"), None), P(("ep", "tp"), None)),
        check_vma=False,
    )
```
